256 devices in a mesh: ep: 64 (over z, x, core), tp: 4 (over y).
Axes of the slice: x: 4, y: 4, z: 8, core: 2. Of those that a mesh axis runs over, the one named last changes fastest.
Arguments:
- tokens: bfloat16 [1024, 2048], P('ep'), may hold values from -6 to 6
- attn_gain: bfloat16 [2048], replicated, may hold values from 0.099609375 to 1.8984375
- query_weight: bfloat16 [2048, 1024], P('ep', 'tp'), may hold values from -0.125 to 0.125
- key_weight: bfloat16 [2048, 512], P('ep', 'tp'), may hold values from -0.125 to 0.125
- value_weight: bfloat16 [2048, 512], P('ep', 'tp'), may hold values from -0.125 to 0.125
- out_weight: bfloat16 [2048, 1024], P('ep', 'tp'), may hold values from -0.1875 to 0.1875
- head_gain: bfloat16 [1024], P('tp'), may hold values from 0.099609375 to 1.8984375
- past_keys: bfloat16 [1024, 1024, 4, 128], P('ep', None, 'tp'), may hold values from -6 to 6
- past_values: bfloat16 [1024, 1024, 4, 128], P('ep', None, 'tp'), may hold values from -50 to 50
- break_offset: float32 [1024, 8, 1024], P('ep', 'tp'), may hold values from -12.5 to 1
- cache_lengths: int32 [1024], P('ep'), may hold values from 1 to 1024, 524288 in all
- ffn_gain: bfloat16 [2048], replicated, may hold values from 0.099609375 to 1.8984375
- router_weight: bfloat16 [2048, 64], replicated, may hold values from -0.25 to 0.25
- expert_routes: int32 [1024, 6], P('ep'), may hold values from 0 to 63, all different within a row; in each aligned block of 16 rows (0 to 15, 16 to 31, ...) at most 3 rows name the same one
- expert_gate: bfloat16 [64, 2048, 512], P('ep', None, 'tp'), may hold values from -0.125 to 0.125
- expert_up: bfloat16 [64, 2048, 512], P('ep', None, 'tp'), may hold values from -0.125 to 0.125
- expert_down: bfloat16 [64, 512, 2048], P('ep', 'tp'), may hold values from -0.25 to 0.25
- shared_gate: bfloat16 [2048, 512], P(None, 'tp'), may hold values from -0.125 to 0.125
- shared_up: bfloat16 [2048, 512], P(None, 'tp'), may hold values from -0.125 to 0.125
- shared_down: bfloat16 [512, 2048], P('tp'), may hold values from -0.25 to 0.25
Outputs:
- mixed: bfloat16 [1024, 2048], P('ep', 'tp')
- fresh_keys: bfloat16 [1024, 512], P('ep', 'tp')
- fresh_values: bfloat16 [1024, 512], P('ep', 'tp')
The draws below stay inside these ranges and needn't reach their ends.
Inputs may be any that keep to these rules, and one draw needn't show every extreme that they name: `cache_lengths`: the lengths add up to half of 1048576, and some sequence has length 1024. `expert_routes`: each row names 6 different experts. Among the rows of one device no expert is named more than 3 times, and 3 is reached in some device's rows.
All inputs are finite; a program needn't handle non-finite values. No bound on the sum of `cache_lengths` on one device may be relied on, other than what follows from the above.
Results may differ from the reference program's by a relative error of at most 0.0095.
Values may be sent and summed in bfloat16 or wider, within the bound.
A program may use at most 64 MiB of HBM per device.

```python
import math
import jax
import jax.numpy as jnp
import numpy as np
from jax import lax

D = 2048
HQ = 8
KV = 4
HD = 128
EFF = 512
SFF = 512
TOP_K = 6
SEQ_DEV = 16
CACHE_POSITIONS = 1024
BATCH_SEQUENCES = 1024
EXPERTS = 64
CAP = 3
N_EP = 64
N_TP = 4


def draw_break_offset(key, part):
    fast_share = 0.5
    quick_heads = jax.random.uniform(jax.random.fold_in(key, 101), (BATCH_SEQUENCES, HQ, 1)) < fast_share
    baseline_level = jnp.where(quick_heads, math.log(0.08), math.log(0.5 / CACHE_POSITIONS))
    slowdown_factor = jax.random.uniform(jax.random.fold_in(key, 102), (BATCH_SEQUENCES, HQ, 1), minval=0.0, maxval=math.log(3.0))
    jitter_amount = 0.7 * jnp.clip(jax.random.normal(jax.random.fold_in(key, 103), (BATCH_SEQUENCES, HQ, CACHE_POSITIONS)), -5.0, 5.0)
    spike_events = jax.random.uniform(jax.random.fold_in(key, 104), (BATCH_SEQUENCES, 1, CACHE_POSITIONS)) < 3.0 / CACHE_POSITIONS
    spike_level = jax.random.uniform(jax.random.fold_in(key, 105), (BATCH_SEQUENCES, 1, CACHE_POSITIONS), minval=-1.4, maxval=0.0)
    return jnp.where(spike_events, spike_level, baseline_level - slowdown_factor + jitter_amount).astype(jnp.float32)


def draw_past_values(key, part):
    values = jnp.clip(jax.random.normal(jax.random.fold_in(key, 201), (BATCH_SEQUENCES, CACHE_POSITIONS, KV, HD)), -5.0, 5.0)
    top_scale = 3.0
    head_ramp = jnp.arange(KV, dtype=jnp.float32) / max(KV - 1, 1)
    scales = top_scale ** head_ramp
    return (values * scales[None, None, :, None]).astype(jnp.bfloat16)


def block_levels(rng, extent, shards, low, high):
    loudness, own = 1.0, jax.random.fold_in(rng, 6)
    for position, shards_of in shards:
        draws = jnp.exp(jax.random.uniform(jax.random.fold_in(own, position), (shards_of,), jnp.float32, low / len(shards), high / len(shards)))
        loudness = loudness * jnp.repeat(draws, extent[position] // shards_of).reshape([-1 if axis == position else 1 for axis in range(len(extent))])
    return loudness


def length_profile(amount, total, limit, slope):
    portions = [(1 << 20) // math.isqrt(rank ** slope) + 1 for rank in range(2, amount + 1)]
    rest, counts = total - limit - (amount - 1), [1] * (amount - 1)
    while rest > 0:
        free = [i for i in range(amount - 1) if counts[i] < limit]
        pool, left = sum([portions[i] for i in free]), rest
        for i in free:
            more = min(limit - counts[i], max(1, left * portions[i] // pool), rest)
            counts[i] = counts[i] + more
            rest = rest - more
    return np.array([limit] + counts)


def ragged_sizes(own_key, count, total, reach, slope):
    if count == 2:
        one = jax.random.randint(own_key, (), max(1, total - reach), min(reach, total - 1) + 1)
        return jnp.stack([one, total - one])
    sizes = jnp.asarray(length_profile(count, total, reach, slope), jnp.int32)
    couples = (count - 1) // 2
    donor, receiver = sizes[1:1 + 2 * couples:2], sizes[2:2 + 2 * couples:2]
    room = jnp.minimum(donor - 1, reach - receiver)
    moved = jax.random.randint(jax.random.fold_in(own_key, 1), (couples,), 0, 1 << 20) % (room + 1)
    sizes = sizes.at[1:1 + 2 * couples:2].set(donor - moved).at[2:2 + 2 * couples:2].set(receiver + moved)
    return sizes[jax.random.permutation(jax.random.fold_in(own_key, 2), count)]


def routed_block(key, own, number, rows, count, top, most, skew):
    ranking = jax.random.permutation(key, count)
    packed, usual = load_shares(count, rows * top, most, skew, True), load_shares(count, rows * top, most, skew, False)
    places = jnp.arange(count)

    def named(tallies, rotation):
        used = int((tallies > 0).sum())
        fixed = max(1, used // 4)
        shifted = fixed + (places - fixed + rotation * (used - fixed)) % max(1, count - fixed)
        return jnp.zeros((count,), jnp.int32).at[ranking[jnp.where(places < fixed, places, shifted)]].set(jnp.asarray(tallies, jnp.int32))

    tallies = jnp.where(number % 4 == 0, named(packed, number // 4), named(usual, number - number // 4 - 1))
    mixed = jax.random.permutation(jax.random.fold_in(own, 3), count)
    source_of, taker = mixed[0:count // 2 * 2:2], mixed[1:count // 2 * 2:2]
    slack = jnp.minimum(tallies[source_of] - 1, most - tallies[taker]) // 2
    slack = jnp.where((source_of == ranking[0]) | (taker == ranking[0]) | (tallies[taker] == 0), 0, jnp.maximum(slack, 0))
    shifted = jax.random.randint(jax.random.fold_in(own, 4), (count // 2,), 0, 1 << 20) % (slack + 1)
    tallies = tallies.at[source_of].add(-shifted).at[taker].add(shifted)
    members = jnp.searchsorted(jnp.cumsum(tallies), jnp.arange(rows * top), side="right").astype(jnp.int32)
    grid = members.reshape(top, rows).T
    grid = grid[jax.random.permutation(jax.random.fold_in(own, 1), rows)]
    rotation = jax.random.randint(jax.random.fold_in(own, 2), (rows, 1), 0, top)
    return jnp.take_along_axis(grid, (jnp.arange(top)[None, :] + rotation) % top, axis=1)


def load_shares(number_of, total, bound, lean, full):
    loads = [(1 << 20) // math.isqrt(rank ** lean) + 1 for rank in range(1, number_of + 1)]
    largest = bound if full else min(bound, max(-(-total // number_of), total * loads[0] // sum(loads)))
    least = 1 if total - largest >= number_of - 1 else 0
    given, spare = [largest] + [least] * (number_of - 1), total - largest - least * (number_of - 1)
    while spare > 0:
        free = [i for i in range(1, number_of) if given[i] < largest] or [i for i in range(1, number_of) if given[i] < bound]
        whole, remaining = sum([loads[i] for i in free]), spare
        for i in free:
            addition = min(bound - given[i], max(1, remaining * loads[i] // whole), spare)
            given[i] = given[i] + addition
            spare = spare - addition
    return np.array(given)


def noise(own_key, dims, width, bound, cuts=(), kind=jnp.bfloat16):
    result = jax.random.normal(own_key, dims, jnp.float32) * width
    if len(cuts) > 0:
        result = block_levels(own_key, dims, cuts, -0.22, 0.18) * result
    return jnp.clip(result, min=-bound, max=bound).astype(kind)


def setup_inputs(seed: int = 0) -> dict:
    arg_keys = jax.random.split(jax.random.key(seed), 21)
    tokens = noise(arg_keys[0], (BATCH_SEQUENCES, D), 1.0, 6.0, ((0, 64),))
    attn_gain = jnp.clip(1.0 + 0.18 * jax.random.normal(arg_keys[1], (D,), jnp.float32), 0.099609375, 1.8984375).astype(jnp.bfloat16)
    query_weight = noise(arg_keys[2], (D, HQ * HD), D ** -0.5, 0.125, ((0, 64), (1, 4)))
    key_weight = noise(arg_keys[3], (D, KV * HD), D ** -0.5, 0.125, ((0, 64), (1, 4)))
    value_weight = noise(arg_keys[4], (D, KV * HD), D ** -0.5, 0.125, ((0, 64), (1, 4)))
    out_weight = noise(arg_keys[5], (D, HQ * HD), (HQ * HD) ** -0.5, 0.1875, ((0, 64), (1, 4)))
    head_gain = jnp.clip(1.0 + 0.18 * jax.random.normal(arg_keys[6], (HQ * HD,), jnp.float32), 0.099609375, 1.8984375).astype(jnp.bfloat16)
    past_keys = noise(arg_keys[7], (BATCH_SEQUENCES, CACHE_POSITIONS, KV, HD), 1.0, 6.0, ((0, 64), (2, 4)))
    past_values = draw_past_values(jax.random.fold_in(arg_keys[20], 71), 0)
    break_offset = draw_break_offset(jax.random.fold_in(arg_keys[20], 71), 0)
    cache_lengths = ragged_sizes(arg_keys[10], BATCH_SEQUENCES, BATCH_SEQUENCES * CACHE_POSITIONS // 2, CACHE_POSITIONS, 2).astype(jnp.int32)
    ffn_gain = jnp.clip(1.0 + 0.18 * jax.random.normal(arg_keys[11], (D,), jnp.float32), 0.099609375, 1.8984375).astype(jnp.bfloat16)
    router_weight = noise(arg_keys[12], (D, EXPERTS), (D // 4) ** -0.5, 0.25)
    expert_routes_keys = jax.random.split(jax.random.fold_in(arg_keys[13], 1), BATCH_SEQUENCES // SEQ_DEV)
    expert_routes_turns = jax.random.permutation(jax.random.fold_in(arg_keys[13], 3), BATCH_SEQUENCES // SEQ_DEV)
    expert_routes = jax.vmap(lambda own, number: routed_block(jax.random.fold_in(arg_keys[13], 2), own, number, SEQ_DEV, EXPERTS, TOP_K, CAP, 2))(expert_routes_keys, expert_routes_turns).reshape((BATCH_SEQUENCES, TOP_K))
    expert_gate = noise(arg_keys[14], (EXPERTS, D, EFF), D ** -0.5, 0.125, ((0, 64), (2, 4)))
    expert_up = noise(arg_keys[15], (EXPERTS, D, EFF), D ** -0.5, 0.125, ((0, 64), (2, 4)))
    expert_down = noise(arg_keys[16], (EXPERTS, EFF, D), EFF ** -0.5, 0.25, ((0, 64), (1, 4)))
    shared_gate = noise(arg_keys[17], (D, SFF), D ** -0.5, 0.125, ((1, 4),))
    shared_up = noise(arg_keys[18], (D, SFF), D ** -0.5, 0.125, ((1, 4),))
    shared_down = noise(arg_keys[19], (SFF, D), SFF ** -0.5, 0.25, ((0, 4),))
    return {"tokens": tokens, "attn_gain": attn_gain, "query_weight": query_weight, "key_weight": key_weight, "value_weight": value_weight, "out_weight": out_weight, "head_gain": head_gain, "past_keys": past_keys, "past_values": past_values, "break_offset": break_offset, "cache_lengths": cache_lengths, "ffn_gain": ffn_gain, "router_weight": router_weight, "expert_routes": expert_routes, "expert_gate": expert_gate, "expert_up": expert_up, "expert_down": expert_down, "shared_gate": shared_gate, "shared_up": shared_up, "shared_down": shared_down}


epsilon = 1e-06
routed_scale = 2.5

def root_norm(values, gain):
    data = values.astype(jnp.float32)
    factor = lax.rsqrt(lax.optimization_barrier(jnp.mean(data * data, axis=-1, keepdims=True)) + epsilon)
    return (data * factor * gain.astype(jnp.float32)).astype(jnp.bfloat16)

def rounded(values):
    return lax.optimization_barrier(values.astype(jnp.bfloat16)).astype(jnp.float32)

def group_sum(left_side, right_side, groups):
    width_part = left_side.shape[1] // groups
    running = jnp.zeros((left_side.shape[0], right_side.shape[1]), jnp.float32)
    for group_index in range(groups):
        piece_left = left_side[:, group_index * width_part:(group_index + 1) * width_part]
        piece_right = right_side[group_index * width_part:(group_index + 1) * width_part]
        running = running + rounded(jnp.dot(piece_left, piece_right, preferred_element_type=jnp.float32))
    return running

def reference(tokens, attn_gain, query_weight, key_weight, value_weight, out_weight, head_gain, past_keys, past_values, break_offset, cache_lengths, ffn_gain, router_weight, expert_routes, expert_gate, expert_up, expert_down, shared_gate, shared_up, shared_down):
    normed = root_norm(tokens, attn_gain)
    queries = jnp.dot(normed, query_weight, preferred_element_type=jnp.float32).astype(jnp.bfloat16)
    fresh_keys = jnp.dot(normed, key_weight, preferred_element_type=jnp.float32).astype(jnp.bfloat16)
    fresh_values = jnp.dot(normed, value_weight, preferred_element_type=jnp.float32).astype(jnp.bfloat16)
    group_size = HQ // KV

    def attend(inputs):
        block_queries, block_keys, block_values, block_offsets, block_lengths = inputs
        grouped = block_queries.astype(jnp.float32).reshape(SEQ_DEV, KV, group_size, HD)
        scores = jnp.einsum('bgrd,blgd->bgrl', grouped, block_keys.astype(jnp.float32))
        logits = scores.reshape(SEQ_DEV, HQ, CACHE_POSITIONS) * HD ** (-0.5) + block_offsets
        places = jnp.arange(CACHE_POSITIONS, dtype=jnp.int32)[None, None, :]
        usable = places < block_lengths[:, None, None]
        keep_log = jnp.where(usable, jax.nn.log_sigmoid(-logits), 0.0)
        after_sum = lax.cumsum(keep_log, axis=2, reverse=True) - keep_log
        sticks = jnp.where(usable, jnp.exp(jax.nn.log_sigmoid(logits) + after_sum), 0.0)
        sticks = rounded(sticks).reshape(SEQ_DEV, KV, group_size, CACHE_POSITIONS)
        outputs = jnp.einsum('bgrl,blgd->bgrd', sticks, block_values.astype(jnp.float32))
        return outputs.reshape(SEQ_DEV, HQ * HD)
    heads_out = lax.map(attend, (queries.reshape(N_EP, SEQ_DEV, HQ * HD), past_keys.reshape(N_EP, SEQ_DEV, CACHE_POSITIONS, KV, HD), past_values.reshape(N_EP, SEQ_DEV, CACHE_POSITIONS, KV, HD), break_offset.reshape(N_EP, SEQ_DEV, HQ, CACHE_POSITIONS), cache_lengths.reshape(N_EP, SEQ_DEV))).reshape(BATCH_SEQUENCES, HQ * HD)
    scaled = (heads_out * head_gain.astype(jnp.float32)).astype(jnp.bfloat16)
    square_sum = lax.optimization_barrier(jnp.sum(heads_out * heads_out, axis=-1))
    head_total = group_sum(scaled, out_weight.T, N_TP)
    attention = head_total * lax.rsqrt(square_sum[:, None] / (HQ * HD) + epsilon)
    residual = (tokens.astype(jnp.float32) + attention).astype(jnp.bfloat16)
    normed_ffn = root_norm(residual, ffn_gain)
    router_prob = jax.nn.sigmoid(jnp.dot(normed_ffn, router_weight, preferred_element_type=jnp.float32))
    picked = jnp.take_along_axis(router_prob, expert_routes, axis=1)
    route_weight = routed_scale * picked / lax.optimization_barrier(jnp.sum(picked, axis=-1, keepdims=True))
    flat_routes = expert_routes.reshape(N_EP, SEQ_DEV * TOP_K)
    flat_hot = (flat_routes[:, :, None] == jnp.arange(EXPERTS, dtype=jnp.int32)[None, None, :]).astype(jnp.int32)
    earlier = jnp.cumsum(flat_hot, axis=1) - flat_hot
    slot_index = lax.optimization_barrier(jnp.sum(earlier * flat_hot, axis=-1)).astype(jnp.int32)
    owner_group = jnp.broadcast_to(jnp.arange(N_EP, dtype=jnp.int32)[:, None], flat_routes.shape)
    pair_row = jnp.broadcast_to((jnp.arange(SEQ_DEV * TOP_K, dtype=jnp.int32) // TOP_K)[None, :], flat_routes.shape)
    row_number = (owner_group * SEQ_DEV + pair_row).astype(jnp.int32)
    row_table = jnp.full((EXPERTS, N_EP, CAP), BATCH_SEQUENCES, jnp.int32).at[flat_routes, owner_group, slot_index].set(row_number)
    padded_rows = jnp.concatenate([normed_ffn, jnp.zeros((1, D), jnp.bfloat16)], axis=0)

    def one_expert(inputs):
        row_ids, gate_matrix, up_matrix, down_matrix = inputs
        chosen_rows = padded_rows[row_ids.reshape(-1)]
        gate_part = jnp.dot(chosen_rows, gate_matrix, preferred_element_type=jnp.float32)
        up_part = jnp.dot(chosen_rows, up_matrix, preferred_element_type=jnp.float32)
        hidden = (jax.nn.silu(gate_part) * up_part).astype(jnp.bfloat16)
        return group_sum(hidden, down_matrix, N_TP).astype(jnp.bfloat16)
    expert_out = lax.map(one_expert, (row_table, expert_gate, expert_up, expert_down))
    taken = expert_out[flat_routes, (owner_group * CAP + slot_index).astype(jnp.int32)]
    taken = taken.reshape(BATCH_SEQUENCES, TOP_K, D).astype(jnp.float32)
    routed = lax.optimization_barrier(jnp.sum(route_weight[:, :, None] * taken, axis=1))
    shared_hidden = (jax.nn.silu(jnp.dot(normed_ffn, shared_gate, preferred_element_type=jnp.float32)) * jnp.dot(normed_ffn, shared_up, preferred_element_type=jnp.float32)).astype(jnp.bfloat16)
    shared_out = group_sum(shared_hidden, shared_down, N_TP)
    mixed = (residual.astype(jnp.float32) + routed + shared_out).astype(jnp.bfloat16)
    return (mixed, fresh_keys, fresh_values)
```

```python
import jax
import jax.numpy as jnp
from jax import lax
from jax.experimental import pallas as pl
from jax.experimental.pallas import tpu as pltpu
from jax.sharding import Mesh
from jax.sharding import PartitionSpec as P

MESH = pl.DeviceIdType.MESH
EP = ("ep_0", "ep_1", "ep_2")
NZ, NX, NC, NT = 8, 4, 2, 4
NE = NZ * NX * NC
SEQ = 16
POS = 1024
HD = 128
EPS = 1e-06
SCALE = 2.5
F32 = jnp.float32
BF16 = jnp.bfloat16


def dot(a, b):
    return jnp.dot(a, b, preferred_element_type=F32)


def dot_nt(a, b):
    return lax.dot_general(a, b, (((1,), (1,)), ((), ())), preferred_element_type=F32)


def iota(shape, dim):
    return lax.broadcasted_iota(jnp.int32, shape, dim)


def ones_where(cond):
    return jnp.where(cond, 1.0, 0.0).astype(BF16)


def root_norm(data, gain):
    factor = lax.rsqrt(jnp.mean(data * data, axis=-1, keepdims=True) + EPS)
    return (data * factor * gain).astype(BF16)


def kernel(
    tok_h, ag_h, wq_h, wk_h, wv_h, wo_h, hg_h, pk_h, pv_h, off_h, lens, fg_h, rt_h, er_h,
    eg_h, eu_h, ed_h, sg_h, su_h, sd_h,
    mixed_o, fk_o, fv_o,
    tok, ag, hg, fg, rt, er, off, kb, vb, wb, ob, wgu, wd, sgu, sd,
    qs, lg, lenb, ho, pc, sq, nf, res, sbuf, rbuf, xb, gs, gr, hs, obuf, cbuf, ssb, ssr,
    lsem, kvsem,
    wxs, wxr, wzs, wzr, wds, wdr,
    oxs, oxr, ozs, ozr, ods, odr,
    ys, yr, cs, cr, as_, ar, gss, gsr, hss, hsr, rs_, rr, sss, ssrr,
):
    z = lax.axis_index("ep_0")
    x = lax.axis_index("ep_1")
    c = lax.axis_index("ep_2")
    t = lax.axis_index("tp")
    e = (z * NX + x) * NC + c

    def ep_dev(i):
        return (i // (NX * NC), lax.rem(i // NC, NX), lax.rem(i, NC), t)

    def tp_dev(i):
        return (z, x, c, i)

    def remote(src, dst, ssem, rsem, dev):
        return pltpu.make_async_remote_copy(
            src_ref=src, dst_ref=dst, send_sem=ssem, recv_sem=rsem,
            device_id=dev, device_id_type=MESH,
        )

    loads = []

    def load(src, dst):
        cp = pltpu.make_async_copy(src, dst, lsem.at[len(loads)])
        cp.start()
        loads.append(cp)
        return cp

    ld_w = [
        load(wq_h, wb.at[z, x, c, :, pl.ds(0, 256)]),
        load(wk_h, wb.at[z, x, c, :, pl.ds(256, 128)]),
        load(wv_h, wb.at[z, x, c, :, pl.ds(384, 128)]),
    ]
    ld_o = load(wo_h, ob.at[z, x, c])
    ld_tok = [load(tok_h, tok), load(ag_h, ag)]
    ld_er = load(er_h, er)
    ld_att = [load(off_h, off), load(hg_h, hg)]
    kv_loads = []
    for i in range(4):
        ds = pl.ds(4 * i, 4)
        kv_loads.append(pltpu.make_async_copy(pk_h.at[ds], kb.at[ds], kvsem.at[i]))
        kv_loads.append(pltpu.make_async_copy(pv_h.at[ds], vb.at[ds], kvsem.at[4 + i]))
    for cp in kv_loads:
        cp.start()
    ld_ffn = [load(fg_h, fg), load(rt_h, rt)]
    ld_sh = [
        load(sg_h, sgu.at[:, pl.ds(0, 128)]),
        load(su_h, sgu.at[:, pl.ds(128, 128)]),
        load(sd_h, sd),
    ]
    mine = pl.ds(pl.multiple_of(t * 512, 512), 512)
    ld_ex = [
        load(eg_h.at[0, mine, :], wgu.at[t, :, pl.ds(0, 128)]),
        load(eu_h.at[0, mine, :], wgu.at[t, :, pl.ds(128, 128)]),
        load(ed_h.at[0, :, mine], wd.at[t]),
    ]

    barrier = pltpu.get_barrier_semaphore()

    @pl.loop(1, NE)
    def _(d):
        pl.semaphore_signal(
            barrier, inc=1, device_id=ep_dev(lax.rem(e + d, NE)), device_id_type=MESH
        )

    for d in range(1, NT):
        pl.semaphore_signal(
            barrier, inc=1, device_id=tp_dev(lax.rem(t + d, NT)), device_id_type=MESH
        )
    pl.semaphore_wait(barrier, NE - 1 + NT - 1)

    pending = []

    def gather(buf, xs, xr, zs, zr, dsm, drm):
        def at(r, i):
            return buf.at[lax.rem(z + r + NZ, NZ), lax.rem(x + i, NX), c]

        up = (lax.rem(z + 1, NZ), x, c, t)
        down = (lax.rem(z + NZ - 1, NZ), x, c, t)
        partner = (z, x, 1 - c, t)

        def send(src, ssem, rsem, dev):
            cp = remote(src, src, ssem, rsem, dev)
            cp.start()
            pending.append(cp)

        def arrived(dst, ssem, rsem, dev):
            remote(dst, dst, ssem, rsem, dev).wait_recv()

        def first():
            for i in (1, 3, 2):
                send(at(0, 0), xs.at[i], xr.at[i], (z, lax.rem(x + i, NX), c, t))
            send(at(0, 0), zs.at[0, 0, 0], zr.at[0, 0, 0], up)
            send(at(0, 0), zs.at[1, 0, 0], zr.at[1, 0, 0], down)
            send(at(0, 0), dsm.at[0, 0], drm.at[0, 0], partner)

        def second():
            for i in (1, 3, 2):
                arrived(at(0, i), xs.at[NX - i], xr.at[NX - i], partner)
                send(at(0, i), zs.at[0, 0, i], zr.at[0, 0, i], up)
                send(at(0, i), zs.at[1, 0, i], zr.at[1, 0, i], down)
                send(at(0, i), dsm.at[0, i], drm.at[0, i], partner)

        def ring(s):
            for i in (0, 1, 3, 2):
                arrived(at(-s, i), zs.at[0, s - 1, i], zr.at[0, s - 1, i], partner)
                if s < 4:
                    send(at(-s, i), zs.at[0, s, i], zr.at[0, s, i], up)
                send(at(-s, i), dsm.at[NZ - s, i], drm.at[NZ - s, i], partner)
                if s < 4:
                    arrived(at(s, i), zs.at[1, s - 1, i], zr.at[1, s - 1, i], partner)
                    if s < 3:
                        send(at(s, i), zs.at[1, s, i], zr.at[1, s, i], down)
                    send(at(s, i), dsm.at[s, i], drm.at[s, i], partner)

        def last():
            for r in range(NZ):
                for i in range(NX):
                    dst = buf.at[lax.rem(z + r, NZ), lax.rem(x + i, NX), 1 - c]
                    arrived(dst, dsm.at[r, i], drm.at[r, i], partner)

        return first, second, ring, last

    w_first, w_second, w_ring, w_last = gather(wb, wxs, wxr, wzs, wzr, wds, wdr)
    o_first, o_second, o_ring, o_last = gather(ob, oxs, oxr, ozs, ozr, ods, odr)
    for cp in ld_w:
        cp.wait()
    w_first()
    ld_o.wait()

    def y_send(src, dst, ssem, rsem, dev):
        cp = remote(src, dst, ssem, rsem, dev)
        cp.start()
        pending.append(cp)

    for d in (1, 3, 2):
        p = lax.rem(t + d, NT)
        theirs = pl.ds(pl.multiple_of(p * 512, 512), 512)
        y_send(eg_h.at[0, theirs, :], wgu.at[t, :, pl.ds(0, 128)], ys.at[0, d], yr.at[0, d], tp_dev(p))
        y_send(eu_h.at[0, theirs, :], wgu.at[t, :, pl.ds(128, 128)], ys.at[1, d], yr.at[1, d], tp_dev(p))
        y_send(ed_h.at[0, :, theirs], wd.at[t], ys.at[2, d], yr.at[2, d], tp_dev(p))

    w_second()
    o_first()

    for cp in ld_tok:
        cp.wait()
    normed = root_norm(tok[...].astype(F32), ag[...])
    w_ring(1)
    o_second()
    w_ring(2)
    w_ring(3)
    w_ring(4)

    ld_er.wait()
    rows = NE * SEQ
    chosen = iota((NE, SEQ), 0) == er[0:1, :]
    for k in range(1, 6):
        chosen = chosen | (iota((NE, SEQ), 0) == er[k : k + 1, :])
    hot_t = ones_where(chosen)
    before = ones_where(iota((SEQ, SEQ), 0) < iota((SEQ, SEQ), 1))
    code_t = jnp.where(chosen, dot(hot_t, before) + 1.0, 0.0).astype(BF16)
    repeat = ones_where((iota((SEQ, 64), 1) & 15) == iota((SEQ, 64), 0))
    eye = ones_where(iota((SEQ, SEQ), 0) == iota((SEQ, SEQ), 1))
    code4_t = dot(code_t, repeat).astype(BF16)
    code = dot_nt(eye, code_t)
    r0 = iota((rows, 64), 0)
    c0 = iota((rows, 64), 1)
    spread = ones_where((r0 >> 4) == c0)
    slot_of = dot(spread, code4_t)
    want = ((r0 & 3) + 1).astype(F32)
    dispatch = ones_where((slot_of == want) & (((r0 >> 2) & 3) == (c0 >> 4)))

    w_last()
    total = jnp.zeros((SEQ, 512), F32)
    for zi in range(NZ):
        total = total + dot(normed[:, 256 * zi : 256 * zi + 256], wb[zi].reshape(256, 512))
    queries = total[:, 0:256].astype(BF16).astype(F32)
    fk_o[...] = total[:, 256:384].astype(BF16)
    fv_o[...] = total[:, 384:512].astype(BF16)
    o_ring(1)

    for h in range(2):
        qs[pl.ds(h, SEQ, stride=2), :] = queries[:, HD * h : HD * h + HD]
    for cp in ld_att:
        cp.wait()
    for b in range(SEQ):
        if b % 4 == 0:
            kv_loads[2 * (b // 4)].wait()
        q = qs[2 * b : 2 * b + 2, :].astype(BF16)
        lg[2 * b : 2 * b + 2, :] = dot_nt(q, kb[b]) * HD ** (-0.5) + off[b]
        lenb[2 * b : 2 * b + 2, :] = jnp.full((2, HD), lens[b], jnp.int32)
    o_ring(2)
    logits = lg[...]
    length = lenb[:, 0:1]
    usable = iota((2 * SEQ, POS), 1) < length
    tail = jnp.log(1.0 + jnp.exp(-jnp.abs(logits)))
    keep = jnp.where(usable, jnp.minimum(-logits, 0.0) - tail, 0.0)
    nb = POS // HD
    stacked = jnp.concatenate([keep[:, HD * i : HD * i + HD] for i in range(nb)], axis=0)
    k1 = stacked.astype(BF16)
    left = stacked - k1.astype(F32)
    k2 = left.astype(BF16)
    k3 = (left - k2.astype(F32)).astype(BF16)
    later = ones_where(iota((HD, HD), 0) > iota((HD, HD), 1))
    inner = dot(k1, later) + dot(k2, later) + dot(k3, later)
    carry = jnp.zeros((2 * SEQ, 1), F32)
    after = [None] * nb
    n2 = 2 * SEQ
    for i in range(nb - 1, -1, -1):
        after[i] = inner[n2 * i : n2 * i + n2] + carry
        carry = carry + jnp.sum(stacked[n2 * i : n2 * i + n2], axis=-1, keepdims=True)
    after = jnp.concatenate(after, axis=1)
    sticks = jnp.where(usable, jnp.exp(jnp.minimum(logits, 0.0) - tail + after), 0.0)
    lg[...] = sticks
    o_ring(3)
    for b in range(SEQ):
        if b % 4 == 0:
            kv_loads[2 * (b // 4) + 1].wait()
        got = dot(lg[2 * b : 2 * b + 2, :].astype(BF16), vb[b])
        ho[b : b + 1, 0:HD] = got[0:1, :]
        ho[b : b + 1, HD : 2 * HD] = got[1:2, :]
    o_ring(4)
    heads_out = ho[...]
    scaled = (heads_out * hg[...]).astype(BF16)
    sq[t] = jnp.broadcast_to(jnp.sum(heads_out * heads_out, axis=-1, keepdims=True), (SEQ, HD))
    o_last()
    for zi in range(NZ):
        part = dot_nt(scaled, ob[zi].reshape(256, 256))
        pc[t, :, 256 * zi : 256 * zi + 256] = part.astype(BF16)

    c_moves = []
    for d in (2, 1, 3):
        p = lax.rem(t + d, NT)
        for k, buf in enumerate((sq, pc)):
            cp = remote(buf.at[t], buf.at[t], cs.at[k, d], cr.at[k, d], tp_dev(p))
            cp.start()
            pending.append(cp)
            c_moves.append((k, d, buf))
    for k, d, buf in c_moves:
        src = lax.rem(t + NT - d, NT)
        remote(buf.at[src], buf.at[src], cs.at[k, d], cr.at[k, d], tp_dev(src)).wait_recv()
    head_total = pc[0].astype(F32)
    square = sq[0]
    for i in range(1, NT):
        head_total = head_total + pc[i].astype(F32)
        square = square + sq[i]
    attention = head_total * lax.rsqrt(square[:, 0:1] / 1024.0 + EPS)
    residual = (tok[...].astype(F32) + attention).astype(BF16)
    for i in range(NT):
        res[i] = residual[:, 512 * i : 512 * i + 512]
    for cp in ld_ffn:
        cp.wait()
    normed_ffn = root_norm(residual.astype(F32), fg[...])
    for i in range(16):
        nf[i] = normed_ffn[:, HD * i : HD * i + HD]

    block = nf[pl.ds(4 * t, 4)].reshape(64, HD)
    sbuf[...] = dot(dispatch, block).astype(BF16).reshape(NE, SEQ, HD)

    @pl.loop(1, NE)
    def _(d):
        p = lax.rem(e + d, NE)
        remote(sbuf.at[p], rbuf.at[e], as_, ar, ep_dev(p)).start()

    rbuf[e] = sbuf[e]

    for cp in ld_sh:
        cp.wait()
    both = dot(normed_ffn, sgu[...])
    gate = both[:, 0:HD]
    shared_hidden = (gate / (1.0 + jnp.exp(-gate)) * both[:, HD : 2 * HD]).astype(BF16)
    shared_part = dot(shared_hidden, sd[...]).astype(BF16)
    for i in range(NT):
        ssb[i] = shared_part[:, 512 * i : 512 * i + 512]
    for d in (2, 1, 3):
        p = lax.rem(t + d, NT)
        y_send(ssb.at[p], ssr.at[t], sss.at[d], ssrr.at[d], tp_dev(p))
    ssr[t] = ssb[t]
    logit = dot_nt(normed_ffn, rt[...])
    prob = 1.0 / (1.0 + jnp.exp(-logit))
    picked = jnp.where(code > 0.5, prob, 0.0)
    weight = SCALE * picked / jnp.sum(picked, axis=-1, keepdims=True)
    weight4 = jnp.concatenate([weight] * 4, axis=0)
    w_hi = weight4.astype(BF16)
    w_lo = (weight4 - w_hi.astype(F32)).astype(BF16)
    code4 = jnp.concatenate([code] * 4, axis=0).astype(BF16)
    r1 = iota((64, rows), 1)
    c1 = iota((64, rows), 0)
    spread_t = ones_where((r1 >> 4) == c1)
    slot_to = dot(code4, spread_t)
    fits = (slot_to == ((r1 & 3) + 1).astype(F32)) & (((r1 >> 2) & 3) == (c1 >> 4))
    comb_hi = jnp.where(fits, dot(w_hi, spread_t), 0.0).astype(BF16)
    comb_lo = jnp.where(fits, dot(w_lo, spread_t), 0.0).astype(BF16)

    def everyone(buf):
        return buf.at[pl.ds(0, NE - 1)]

    def wait_all(src, dst, ssem, rsem):
        cp = remote(everyone(src), everyone(dst), ssem, rsem, tp_dev(lax.rem(t + 1, NT)))
        cp.wait_recv()
        cp.wait_send()

    wait_all(sbuf, rbuf, as_, ar)

    p48 = iota((48, 256), 0)
    q48 = iota((48, 256), 1)
    for g in range(4):
        group = rbuf[16 * g : 16 * g + 16].reshape(256, HD)
        for j in range(4):
            pick = ones_where(q48 == ((p48 & 15) << 4) + 4 * j + (p48 >> 4))
            xb[48 * g : 48 * g + 48, HD * j : HD * j + HD] = dot(pick, group).astype(BF16)
    for cp in ld_ex:
        cp.wait()
    for d in (1, 3, 2):
        src = lax.rem(t + NT - d, NT)
        remote(wgu.at[src, :, pl.ds(0, 128)], wgu.at[src, :, pl.ds(0, 128)], ys.at[0, d], yr.at[0, d], tp_dev(src)).wait_recv()
        remote(wgu.at[src, :, pl.ds(128, 128)], wgu.at[src, :, pl.ds(128, 128)], ys.at[1, d], yr.at[1, d], tp_dev(src)).wait_recv()
        remote(wd.at[src], wd.at[src], ys.at[2, d], yr.at[2, d], tp_dev(src)).wait_recv()
    xv = xb[...]
    for d in (2, 1, 3):
        p = lax.rem(t + d, NT)
        gs[d] = dot(xv, wgu[p]).astype(BF16)
        y_send(gs.at[d], gr.at[d], gss.at[d], gsr.at[d], tp_dev(p))
    gate_up = dot(xv, wgu[t])
    for d in (2, 1, 3):
        src = lax.rem(t + NT - d, NT)
        remote(gr.at[d], gr.at[d], gss.at[d], gsr.at[d], tp_dev(src)).wait_recv()
        gate_up = gate_up + gr[d].astype(F32)
    gate = gate_up[:, 0:HD]
    hidden = (gate / (1.0 + jnp.exp(-gate)) * gate_up[:, HD : 2 * HD]).astype(BF16)
    hs[t] = hidden
    for d in (2, 1, 3):
        p = lax.rem(t + d, NT)
        y_send(hs.at[t], hs.at[t], hss.at[d], hsr.at[d], tp_dev(p))
    for d in (2, 1, 3):
        src = lax.rem(t + NT - d, NT)
        remote(hs.at[src], hs.at[src], hss.at[d], hsr.at[d], tp_dev(src)).wait_recv()
    out = dot(hs[0], wd[0])
    for i in range(1, NT):
        out = out + dot(hs[i], wd[i])
    out = out.astype(BF16)

    pt = iota((256, 48), 1)
    qt = iota((256, 48), 0)
    for g in range(4):
        back = jnp.zeros((256, HD), F32)
        for j in range(4):
            pick = ones_where(qt == ((pt & 15) << 4) + 4 * j + (pt >> 4))
            back = back + dot(pick, out[48 * g : 48 * g + 48, HD * j : HD * j + HD])
        obuf[16 * g : 16 * g + 16] = back.astype(BF16).reshape(16, 16, HD)

    @pl.loop(1, NE)
    def _(d):
        p = lax.rem(e + d, NE)
        remote(obuf.at[p], cbuf.at[e], rs_, rr, ep_dev(p)).start()

    cbuf[e] = obuf[e]
    shared_total = jnp.zeros((SEQ, 512), F32)
    for d in (2, 1, 3):
        src = lax.rem(t + NT - d, NT)
        remote(ssr.at[src], ssr.at[src], sss.at[d], ssrr.at[d], tp_dev(src)).wait_recv()
    for i in range(NT):
        shared_total = shared_total + ssr[i].astype(F32)
    base = res[t].astype(F32) + shared_total
    wait_all(obuf, cbuf, rs_, rr)
    came = cbuf[...].reshape(rows, HD)
    routed = dot(comb_hi, came) + dot(comb_lo, came)
    for j in range(4):
        mixed_o[:, HD * j : HD * j + HD] = (
            base[:, HD * j : HD * j + HD] + routed[SEQ * j : SEQ * j + SEQ]
        ).astype(BF16)
    for cp in pending:
        cp.wait_send()


def body(
    tokens, attn_gain, query_weight, key_weight, value_weight, out_weight, head_gain,
    past_keys, past_values, break_offset, cache_lengths, ffn_gain, router_weight,
    expert_routes, expert_gate, expert_up, expert_down, shared_gate, shared_up, shared_down,
):
    hbm = pl.BlockSpec(memory_space=pl.ANY)
    vmem = pl.BlockSpec(memory_space=pltpu.VMEM)
    smem = pl.BlockSpec(memory_space=pltpu.SMEM)
    v, dma = pltpu.VMEM, pltpu.SemaphoreType.DMA
    ring = [dma((4,)), dma((4,)), dma((2, 4, 4)), dma((2, 4, 4)), dma((8, 4)), dma((8, 4))]
    return pl.pallas_call(
        kernel,
        out_shape=(
            jax.ShapeDtypeStruct((SEQ, 512), BF16),
            jax.ShapeDtypeStruct((SEQ, HD), BF16),
            jax.ShapeDtypeStruct((SEQ, HD), BF16),
        ),
        in_specs=[smem if i == 10 else hbm for i in range(20)],
        out_specs=(vmem, vmem, vmem),
        scratch_shapes=[
            v((SEQ, 2048), BF16), v((1, 2048), F32), v((1, 256), F32), v((1, 2048), F32),
            v((64, 2048), BF16), v((6, SEQ), jnp.int32), v((SEQ, 2, POS), F32),
            v((SEQ, POS, HD), BF16), v((SEQ, POS, HD), BF16),
            v((NZ, NX, NC, 32, 512), BF16), v((NZ, NX, NC, 32, 256), BF16),
            v((NT, 512, 256), BF16), v((NT, 128, 512), BF16),
            v((2048, 256), BF16), v((128, 2048), BF16),
            v((2 * SEQ, HD), F32), v((2 * SEQ, POS), F32), v((2 * SEQ, HD), jnp.int32),
            v((SEQ, 256), F32), v((NT, SEQ, 2048), BF16), v((NT, SEQ, HD), F32),
            v((16, SEQ, HD), BF16), v((NT, SEQ, 512), BF16),
            v((NE, SEQ, HD), BF16), v((NE, SEQ, HD), BF16), v((192, 512), BF16),
            v((NT, 192, 256), BF16), v((NT, 192, 256), BF16), v((NT, 192, HD), BF16),
            v((NE, SEQ, HD), BF16), v((NE, SEQ, HD), BF16),
            v((NT, SEQ, 512), BF16), v((NT, SEQ, 512), BF16),
            dma((24,)), dma((8,)),
            *ring, *ring,
            dma((3, 4)), dma((3, 4)), dma((2, 4)), dma((2, 4)), dma, dma,
            dma((4,)), dma((4,)), dma((4,)), dma((4,)), dma, dma, dma((4,)), dma((4,)),
        ],
        compiler_params=pltpu.CompilerParams(
            collective_id=0, has_side_effects=True, vmem_limit_bytes=60 * 1024 * 1024
        ),
    )(
        tokens, attn_gain.astype(F32)[None], query_weight, key_weight, value_weight, out_weight,
        head_gain.astype(F32)[None], past_keys.reshape(SEQ, POS, HD),
        past_values.reshape(SEQ, POS, HD), break_offset, cache_lengths,
        ffn_gain.astype(F32)[None], router_weight.T, expert_routes.T, expert_gate, expert_up,
        expert_down, shared_gate, shared_up, shared_down,
    )


def solution(mesh):
    torus = Mesh(mesh.devices.reshape(NZ, NX, NC, NT), (*EP, "tp"))
    return jax.shard_map(
        body,
        mesh=torus,
        in_specs=(
            P(EP, None),
            P(),
            P(EP, "tp"),
            P(EP, "tp"),
            P(EP, "tp"),
            P(EP, "tp"),
            P("tp"),
            P(EP, None, "tp", None),
            P(EP, None, "tp", None),
            P(EP, "tp", None),
            P(EP),
            P(),
            P(),
            P(EP, None),
            P(EP, None, "tp"),
            P(EP, None, "tp"),
            P(EP, "tp", None),
            P(None, "tp"),
            P(None, "tp"),
            P("tp", None),
        ),
        out_specs=(P(EP, "tp"), P(EP, "tp"), P(EP, "tp")),
        check_vma=False,
    )
```

```python
import jax
import jax.numpy as jnp
from jax import lax
from jax.experimental import pallas as pl
from jax.experimental.pallas import tpu as pltpu
from jax.sharding import Mesh
from jax.sharding import PartitionSpec as P

MESH = pl.DeviceIdType.MESH
EP = ("ep_0", "ep_1", "ep_2")
NZ, NX, NC, NT = 8, 4, 2, 4
NE = NZ * NX * NC
SEQ = 16
POS = 1024
HD = 128
EPS = 1e-06
SCALE = 2.5
F32 = jnp.float32
BF16 = jnp.bfloat16


def dot(a, b):
    return jnp.dot(a, b, preferred_element_type=F32)


def dot_nt(a, b):
    return lax.dot_general(a, b, (((1,), (1,)), ((), ())), preferred_element_type=F32)


def iota(shape, dim):
    return lax.broadcasted_iota(jnp.int32, shape, dim)


def ones_where(cond):
    return jnp.where(cond, 1.0, 0.0).astype(BF16)


def kernel(
    tok_h, ag_h, wq_h, wk_h, wv_h, wo_h, hg_h, pk_h, pv_h, off_h, lens, fg_h, rt_h, er_h,
    eg_h, eu_h, ed_h, sg_h, su_h, sd_h,
    mixed_o, fk_o, fv_o,
    tok, ag, hg, fg, rt, er, off, kb, vb, qb, kvb, ob, wgu, wd, sgu, sd,
    tkb, tk, part, qp, kvpart, kvp,
    qs, lg, lenb, ho, pc, sq, nf, res, sbuf, rbuf, xb, gs, gr, hs, obuf, cbuf, ssb, ssr,
    lsem, kvsem,
    qzs, qzr, kzs, kzr, ozs, ozr, oxs, oxr, ods, odr, tks, tkr, qps, qpr, kps, kpr,
    ys, yr, cs, cr, as_, ar, gss, gsr, hss, hsr, rs_, rr, sss, ssrr,
):
    z = lax.axis_index("ep_0")
    x = lax.axis_index("ep_1")
    c = lax.axis_index("ep_2")
    t = lax.axis_index("tp")
    e = (z * NX + x) * NC + c
    m = x * NC + c
    zd = [lax.rem(z + d, NZ) for d in range(NZ)]
    xd = [lax.rem(x + d, NX) for d in range(NX)]
    td = [lax.rem(t + d, NT) for d in range(NT)]
    cd = [c, 1 - c]
    mates = [(2, 0), (2, 1), (1, 0), (3, 0), (1, 1), (3, 1), (0, 1)]
    far_first = [4, 3, 5, 2, 6, 1, 7]
    near_first = far_first[::-1]

    def remote(src, dst, ssem, rsem, dev):
        return pltpu.make_async_remote_copy(
            src_ref=src, dst_ref=dst, send_sem=ssem, recv_sem=rsem,
            device_id=dev, device_id_type=MESH,
        )

    pending = []

    def send(src, dst, ssem, rsem, dev):
        cp = remote(src, dst, ssem, rsem, dev)
        cp.start()
        pending.append(cp)

    def arrived(dst, ssem, rsem):
        remote(dst, dst, ssem, rsem, (z, x, 1 - c, t)).wait_recv()

    loads = []

    def load(src, dst):
        cp = pltpu.make_async_copy(src, dst, lsem.at[len(loads)])
        cp.start()
        loads.append(cp)
        return cp

    ld_q = load(wq_h, qb.at[z])
    ld_tok = [load(tok_h, tok), load(ag_h, ag)]
    ld_o = load(wo_h, ob.at[z, x, c])
    ld_kv = [
        load(wk_h, kvb.at[z, :, pl.ds(0, 128)]),
        load(wv_h, kvb.at[z, :, pl.ds(128, 128)]),
    ]
    ld_er = load(er_h, er)
    ld_att = [load(off_h, off), load(hg_h, hg)]
    kv_loads = []
    for i in range(4):
        ds = pl.ds(4 * i, 4)
        kv_loads.append(pltpu.make_async_copy(pk_h.at[ds], kb.at[ds], kvsem.at[i]))
        kv_loads.append(pltpu.make_async_copy(pv_h.at[ds], vb.at[ds], kvsem.at[4 + i]))
    for cp in kv_loads:
        cp.start()
    ld_ffn = [load(fg_h, fg), load(rt_h, rt)]
    ld_sh = [
        load(sg_h, sgu.at[:, pl.ds(0, 128)]),
        load(su_h, sgu.at[:, pl.ds(128, 128)]),
        load(sd_h, sd),
    ]
    mine = pl.ds(pl.multiple_of(t * 512, 512), 512)
    ld_ex = [
        load(eg_h.at[0, mine, :], wgu.at[t, :, pl.ds(0, 128)]),
        load(eu_h.at[0, mine, :], wgu.at[t, :, pl.ds(128, 128)]),
        load(ed_h.at[0, :, mine], wd.at[t]),
    ]

    barrier = pltpu.get_barrier_semaphore()
    first = [(zd[d], x, c, t) for d in range(1, NZ)]
    first += [(z, xd[dx], cd[dc], t) for dx, dc in mates]
    first += [(z, x, c, td[d]) for d in range(1, NT)]
    for dev in first:
        pl.semaphore_signal(barrier, inc=1, device_id=dev, device_id_type=MESH)
    pl.semaphore_wait(barrier, len(first))

    ld_q.wait()
    for d in far_first:
        send(qb.at[z], qb.at[z], qzs.at[d], qzr.at[d], (zd[d], x, c, t))

    for cp in ld_tok:
        cp.wait()
    data = tok[...].astype(F32)
    factor = lax.rsqrt(jnp.mean(data * data, axis=-1, keepdims=True) + EPS)
    gain = ag[...].astype(F32)
    blocks = []
    for i in range(NZ):
        halves = []
        for k in (2 * i, 2 * i + 1):
            halves.append(data[:, HD * k : HD * k + HD] * factor * gain[k : k + 1, :])
        blocks.append(jnp.concatenate(halves, axis=1).astype(BF16).astype(F32))
    chunk = iota((SEQ, 256), 1) >> 5
    for g in range(8):
        own = blocks[g]
        for k in range(1, 8):
            j = (g + k) % 8
            own = jnp.where(chunk == j, pltpu.roll(blocks[j], 32 * k, 1), own)
        part[g] = own
    for dx, dc in mates:
        g = xd[dx] * NC + cd[dc]
        tkb[g] = part[g].astype(BF16)
        send(tkb.at[g], tk.at[m], tks.at[dx, dc], tkr.at[dx, dc], (z, xd[dx], cd[dc], t))
    tk[m] = part[m].astype(BF16)

    ld_o.wait()
    mine_o = ob.at[z, x, c]
    for d in far_first:
        send(mine_o, mine_o, ozs.at[d], ozr.at[d], (zd[d], x, c, t))

    def o_along(r):
        src = ob.at[zd[r], x, c]
        for i in (2, 1, 3):
            send(src, src, oxs.at[r, i], oxr.at[r, i], (z, xd[i], c, t))

    def o_forward(r):
        src = ob.at[zd[r], x, c]
        arrived(src, ozs.at[NZ - r], ozr.at[NZ - r])
        o_along(r)

    def o_across(r):
        for i in (1, 3, 2):
            arrived(ob.at[zd[r], xd[i], c], oxs.at[r, NX - i], oxr.at[r, NX - i])
        src = ob.at[zd[r], :, c]
        send(src, src, ods.at[r], odr.at[r], (z, x, 1 - c, t))

    def o_last():
        for r in range(NZ):
            arrived(ob.at[zd[r], :, 1 - c], ods.at[r], odr.at[r])

    o_along(0)
    for cp in ld_kv:
        cp.wait()
    for d in far_first:
        send(kvb.at[z], kvb.at[z], kzs.at[d], kzr.at[d], (zd[d], x, c, t))

    for d in (1, 3, 2):
        p = td[d]
        dev = (z, x, c, p)
        theirs = pl.ds(pl.multiple_of(p * 512, 512), 512)
        for k, src in enumerate((eg_h, eu_h)):
            half = pl.ds(128 * k, 128)
            send(src.at[0, theirs, :], wgu.at[t, :, half], ys.at[k, d], yr.at[k, d], dev)
        send(ed_h.at[0, :, theirs], wd.at[t], ys.at[2, d], yr.at[2, d], dev)

    ld_er.wait()
    rows = NE * SEQ
    chosen = iota((NE, SEQ), 0) == er[0:1, :]
    for k in range(1, 6):
        chosen = chosen | (iota((NE, SEQ), 0) == er[k : k + 1, :])
    hot_t = ones_where(chosen)
    before = ones_where(iota((SEQ, SEQ), 0) < iota((SEQ, SEQ), 1))
    code_t = jnp.where(chosen, dot(hot_t, before) + 1.0, 0.0).astype(BF16)
    repeat = ones_where((iota((SEQ, 64), 1) & 15) == iota((SEQ, 64), 0))
    eye = ones_where(iota((SEQ, SEQ), 0) == iota((SEQ, SEQ), 1))
    code4_t = dot(code_t, repeat).astype(BF16)
    code = dot_nt(eye, code_t)
    r0 = iota((rows, 64), 0)
    c0 = iota((rows, 64), 1)
    spread = ones_where((r0 >> 4) == c0)
    slot_of = dot(spread, code4_t)
    want = ((r0 & 3) + 1).astype(F32)
    dispatch = ones_where((slot_of == want) & (((r0 >> 2) & 3) == (c0 >> 4)))

    for dx, dc in mates:
        src = tk.at[lax.rem(x + NX - dx, NX) * NC + cd[dc]]
        arrived(src, tks.at[dx, dc], tkr.at[dx, dc])
    for d in near_first:
        arrived(qb.at[lax.rem(z + NZ - d, NZ)], qzs.at[d], qzr.at[d])
    rows_in = tk[...].reshape(8 * SEQ, 256)
    part[...] = dot(rows_in, qb[...].reshape(256, 256)).reshape(8, SEQ, 256)
    for dx, dc in mates:
        g = xd[dx] * NC + cd[dc]
        send(part.at[g], qp.at[m], qps.at[dx, dc], qpr.at[dx, dc], (z, xd[dx], cd[dc], t))
    qp[m] = part[m]
    for r in (7, 1, 6, 2, 5, 3, 4):
        o_forward(r)
    for dx, dc in mates:
        src = qp.at[lax.rem(x + NX - dx, NX) * NC + cd[dc]]
        arrived(src, qps.at[dx, dc], qpr.at[dx, dc])
    total = qp[0]
    for i in range(1, 8):
        total = total + qp[i]
    queries = total.astype(BF16).astype(F32)

    for h in range(2):
        qs[pl.ds(h, SEQ, stride=2), :] = queries[:, HD * h : HD * h + HD]
    for cp in ld_att:
        cp.wait()
    for b in range(SEQ):
        if b % 4 == 0:
            kv_loads[2 * (b // 4)].wait()
        q = qs[2 * b : 2 * b + 2, :].astype(BF16)
        lg[2 * b : 2 * b + 2, :] = dot_nt(q, kb[b]) * HD ** (-0.5) + off[b]
        lenb[2 * b : 2 * b + 2, :] = jnp.full((2, HD), lens[b], jnp.int32)
    for r in (0, 7, 1):
        o_across(r)
    logits = lg[...]
    length = lenb[:, 0:1]
    usable = iota((2 * SEQ, POS), 1) < length
    tail = jnp.log(1.0 + jnp.exp(-jnp.abs(logits)))
    keep = jnp.where(usable, jnp.minimum(-logits, 0.0) - tail, 0.0)
    nb = POS // HD
    stacked = jnp.concatenate([keep[:, HD * i : HD * i + HD] for i in range(nb)], axis=0)
    k1 = stacked.astype(BF16)
    left = stacked - k1.astype(F32)
    k2 = left.astype(BF16)
    k3 = (left - k2.astype(F32)).astype(BF16)
    later = ones_where(iota((HD, HD), 0) > iota((HD, HD), 1))
    inner = dot(k1, later) + dot(k2, later) + dot(k3, later)
    carry = jnp.zeros((2 * SEQ, 1), F32)
    after = [None] * nb
    n2 = 2 * SEQ
    for i in range(nb - 1, -1, -1):
        after[i] = inner[n2 * i : n2 * i + n2] + carry
        carry = carry + jnp.sum(stacked[n2 * i : n2 * i + n2], axis=-1, keepdims=True)
    after = jnp.concatenate(after, axis=1)
    sticks = jnp.where(usable, jnp.exp(jnp.minimum(logits, 0.0) - tail + after), 0.0)
    lg[...] = sticks
    for r in (6, 2):
        o_across(r)
    for b in range(SEQ):
        if b % 4 == 0:
            kv_loads[2 * (b // 4) + 1].wait()
        got = dot(lg[2 * b : 2 * b + 2, :].astype(BF16), vb[b])
        ho[b : b + 1, 0:HD] = got[0:1, :]
        ho[b : b + 1, HD : 2 * HD] = got[1:2, :]
    for r in (5, 3, 4):
        o_across(r)
    heads_out = ho[...]
    scaled = jnp.concatenate(
        [heads_out[:, HD * i : HD * i + HD] * hg[i : i + 1, :].astype(F32) for i in range(2)],
        axis=1,
    ).astype(BF16)
    sq[t] = jnp.broadcast_to(jnp.sum(heads_out * heads_out, axis=-1, keepdims=True), (SEQ, HD))
    o_last()
    for zi in range(NZ):
        part = dot_nt(scaled, ob[zi].reshape(256, 256))
        pc[t, :, 256 * zi : 256 * zi + 256] = part.astype(BF16)

    for d in (2, 1, 3):
        for k, buf in enumerate((sq, pc)):
            send(buf.at[t], buf.at[t], cs.at[k, d], cr.at[k, d], (z, x, c, td[d]))
    for d in near_first:
        arrived(kvb.at[lax.rem(z + NZ - d, NZ)], kzs.at[d], kzr.at[d])
    kvpart[...] = dot(rows_in, kvb[...].reshape(256, 256)).astype(BF16).reshape(8, SEQ, 256)
    for dx, dc in mates:
        g = xd[dx] * NC + cd[dc]
        send(kvpart.at[g], kvp.at[m], kps.at[dx, dc], kpr.at[dx, dc], (z, xd[dx], cd[dc], t))
    kvp[m] = kvpart[m]
    for d in (1, 3, 2):
        src = td[NT - d]
        for k, buf in enumerate((sq, pc)):
            arrived(buf.at[src], cs.at[k, d], cr.at[k, d])
    head_total = pc[0].astype(F32)
    square = sq[0]
    for i in range(1, NT):
        head_total = head_total + pc[i].astype(F32)
        square = square + sq[i]
    attention = head_total * lax.rsqrt(square[:, 0:1] / 1024.0 + EPS)
    residual = (tok[...].astype(F32) + attention).astype(BF16)
    for i in range(NT):
        res[i] = residual[:, 512 * i : 512 * i + 512]
    for cp in ld_ffn:
        cp.wait()
    data = residual.astype(F32)
    factor = lax.rsqrt(jnp.mean(data * data, axis=-1, keepdims=True) + EPS)
    gain = fg[...].astype(F32)
    pieces = []
    for i in range(16):
        pieces.append(data[:, HD * i : HD * i + HD] * factor * gain[i : i + 1, :])
        nf[i] = pieces[i].astype(BF16)
    normed_ffn = jnp.concatenate(pieces, axis=1).astype(BF16)

    def to_all(src, dst, ssem, rsem):
        for d in far_first + [0]:
            for dx, dc in ([(0, 0)] if d else []) + mates:
                p = (zd[d] * NX + xd[dx]) * NC + cd[dc]
                remote(src.at[p], dst.at[e], ssem, rsem, (zd[d], xd[dx], cd[dc], t)).start()

    block = nf[pl.ds(4 * t, 4)].reshape(64, HD)
    sbuf[...] = dot(dispatch, block).astype(BF16).reshape(NE, SEQ, HD)

    to_all(sbuf, rbuf, as_, ar)

    rbuf[e] = sbuf[e]

    for cp in ld_sh:
        cp.wait()
    both = dot(normed_ffn, sgu[...])
    gate = both[:, 0:HD]
    shared_hidden = (gate / (1.0 + jnp.exp(-gate)) * both[:, HD : 2 * HD]).astype(BF16)
    shared_part = dot(shared_hidden, sd[...]).astype(BF16)
    for i in range(NT):
        ssb[i] = shared_part[:, 512 * i : 512 * i + 512]
    for d in (2, 1, 3):
        p = td[d]
        send(ssb.at[p], ssr.at[t], sss.at[d], ssrr.at[d], (z, x, c, p))
    ssr[t] = ssb[t]
    logit = dot_nt(normed_ffn, rt[...])
    prob = 1.0 / (1.0 + jnp.exp(-logit))
    picked = jnp.where(code > 0.5, prob, 0.0)
    weight = SCALE * picked / jnp.sum(picked, axis=-1, keepdims=True)
    weight4 = jnp.concatenate([weight] * 4, axis=0)
    w_hi = weight4.astype(BF16)
    w_lo = (weight4 - w_hi.astype(F32)).astype(BF16)
    code4 = jnp.concatenate([code] * 4, axis=0).astype(BF16)
    r1 = iota((64, rows), 1)
    c1 = iota((64, rows), 0)
    spread_t = ones_where((r1 >> 4) == c1)
    slot_to = dot(code4, spread_t)
    fits = (slot_to == ((r1 & 3) + 1).astype(F32)) & (((r1 >> 2) & 3) == (c1 >> 4))
    comb_hi = jnp.where(fits, dot(w_hi, spread_t), 0.0).astype(BF16)
    comb_lo = jnp.where(fits, dot(w_lo, spread_t), 0.0).astype(BF16)

    def everyone(buf):
        return buf.at[pl.ds(0, NE - 1)]

    def wait_all(src, dst, ssem, rsem):
        cp = remote(everyone(src), everyone(dst), ssem, rsem, (z, x, 1 - c, t))
        cp.wait_recv()
        cp.wait_send()

    wait_all(sbuf, rbuf, as_, ar)

    p48 = iota((48, 256), 0)
    q48 = iota((48, 256), 1)
    for g in range(4):
        group = rbuf[16 * g : 16 * g + 16].reshape(256, HD)
        for j in range(4):
            pick = ones_where(q48 == ((p48 & 15) << 4) + 4 * j + (p48 >> 4))
            xb[48 * g : 48 * g + 48, HD * j : HD * j + HD] = dot(pick, group).astype(BF16)
    for cp in ld_ex:
        cp.wait()
    for d in (1, 3, 2):
        src = td[NT - d]
        for k in range(2):
            arrived(wgu.at[src, :, pl.ds(128 * k, 128)], ys.at[k, d], yr.at[k, d])
        arrived(wd.at[src], ys.at[2, d], yr.at[2, d])
    xv = xb[...]
    for d in (2, 1, 3):
        gs[d] = dot(xv, wgu[td[d]]).astype(BF16)
        send(gs.at[d], gr.at[d], gss.at[d], gsr.at[d], (z, x, c, td[d]))
    gate_up = dot(xv, wgu[t])
    for d in (2, 1, 3):
        arrived(gr.at[d], gss.at[d], gsr.at[d])
        gate_up = gate_up + gr[d].astype(F32)
    gate = gate_up[:, 0:HD]
    hidden = (gate / (1.0 + jnp.exp(-gate)) * gate_up[:, HD : 2 * HD]).astype(BF16)
    hs[t] = hidden
    for d in (2, 1, 3):
        send(hs.at[t], hs.at[t], hss.at[d], hsr.at[d], (z, x, c, td[d]))
    for d in (2, 1, 3):
        arrived(hs.at[td[NT - d]], hss.at[d], hsr.at[d])
    out = dot(hs[0], wd[0])
    for i in range(1, NT):
        out = out + dot(hs[i], wd[i])
    out = out.astype(BF16)

    pt = iota((256, 48), 1)
    qt = iota((256, 48), 0)
    for g in range(4):
        back = jnp.zeros((256, HD), F32)
        for j in range(4):
            pick = ones_where(qt == ((pt & 15) << 4) + 4 * j + (pt >> 4))
            back = back + dot(pick, out[48 * g : 48 * g + 48, HD * j : HD * j + HD])
        obuf[16 * g : 16 * g + 16] = back.astype(BF16).reshape(16, 16, HD)

    to_all(obuf, cbuf, rs_, rr)

    cbuf[e] = obuf[e]
    shared_total = jnp.zeros((SEQ, 512), F32)
    for d in (2, 1, 3):
        arrived(ssr.at[td[NT - d]], sss.at[d], ssrr.at[d])
    for i in range(NT):
        shared_total = shared_total + ssr[i].astype(F32)
    base = res[t].astype(F32) + shared_total
    for dx, dc in mates:
        src = kvp.at[lax.rem(x + NX - dx, NX) * NC + cd[dc]]
        arrived(src, kps.at[dx, dc], kpr.at[dx, dc])
    fresh = kvp[0].astype(F32)
    for i in range(1, 8):
        fresh = fresh + kvp[i].astype(F32)
    fk_o[...] = fresh[:, 0:HD].astype(BF16)
    fv_o[...] = fresh[:, HD : 2 * HD].astype(BF16)
    wait_all(obuf, cbuf, rs_, rr)
    came = cbuf[...].reshape(rows, HD)
    routed = dot(comb_hi, came) + dot(comb_lo, came)
    for j in range(4):
        mixed_o[:, HD * j : HD * j + HD] = (
            base[:, HD * j : HD * j + HD] + routed[SEQ * j : SEQ * j + SEQ]
        ).astype(BF16)
    for cp in pending:
        cp.wait_send()


def body(
    tokens, attn_gain, query_weight, key_weight, value_weight, out_weight, head_gain,
    past_keys, past_values, break_offset, cache_lengths, ffn_gain, router_weight,
    expert_routes, expert_gate, expert_up, expert_down, shared_gate, shared_up, shared_down,
):
    hbm = pl.BlockSpec(memory_space=pl.ANY)
    vmem = pl.BlockSpec(memory_space=pltpu.VMEM)
    smem = pl.BlockSpec(memory_space=pltpu.SMEM)
    v, dma = pltpu.VMEM, pltpu.SemaphoreType.DMA
    return pl.pallas_call(
        kernel,
        out_shape=(
            jax.ShapeDtypeStruct((SEQ, 512), BF16),
            jax.ShapeDtypeStruct((SEQ, HD), BF16),
            jax.ShapeDtypeStruct((SEQ, HD), BF16),
        ),
        in_specs=[smem if i == 10 else hbm for i in range(20)],
        out_specs=(vmem, vmem, vmem),
        scratch_shapes=[
            v((SEQ, 2048), BF16), v((16, HD), BF16), v((2, HD), BF16), v((16, HD), BF16),
            v((64, 2048), BF16), v((6, SEQ), jnp.int32), v((SEQ, 2, POS), F32),
            v((SEQ, POS, HD), BF16), v((SEQ, POS, HD), BF16),
            v((NZ, 32, 256), BF16), v((NZ, 32, 256), BF16), v((NZ, NX, NC, 32, 256), BF16),
            v((NT, 512, 256), BF16), v((NT, 128, 512), BF16),
            v((2048, 256), BF16), v((128, 2048), BF16),
            v((8, SEQ, 256), BF16), v((8, SEQ, 256), BF16),
            v((8, SEQ, 256), F32), v((8, SEQ, 256), F32),
            v((8, SEQ, 256), BF16), v((8, SEQ, 256), BF16),
            v((2 * SEQ, HD), F32), v((2 * SEQ, POS), F32), v((2 * SEQ, HD), jnp.int32),
            v((SEQ, 256), F32), v((NT, SEQ, 2048), BF16), v((NT, SEQ, HD), F32),
            v((16, SEQ, HD), BF16), v((NT, SEQ, 512), BF16),
            v((NE, SEQ, HD), BF16), v((NE, SEQ, HD), BF16), v((192, 512), BF16),
            v((NT, 192, 256), BF16), v((NT, 192, 256), BF16), v((NT, 192, HD), BF16),
            v((NE, SEQ, HD), BF16), v((NE, SEQ, HD), BF16),
            v((NT, SEQ, 512), BF16), v((NT, SEQ, 512), BF16),
            dma((24,)), dma((8,)),
            *[dma((NZ,)) for _ in range(6)],
            dma((NZ, NX)), dma((NZ, NX)), dma((NZ,)), dma((NZ,)),
            *[dma((NX, NC)) for _ in range(6)],
            dma((3, 4)), dma((3, 4)), dma((2, 4)), dma((2, 4)), dma, dma,
            dma((4,)), dma((4,)), dma((4,)), dma((4,)), dma, dma, dma((4,)), dma((4,)),
        ],
        compiler_params=pltpu.CompilerParams(
            collective_id=0, has_side_effects=True, vmem_limit_bytes=36 * 1024 * 1024
        ),
    )(
        tokens, attn_gain.reshape(16, HD), query_weight, key_weight, value_weight, out_weight,
        head_gain.reshape(2, HD), past_keys.reshape(SEQ, POS, HD),
        past_values.reshape(SEQ, POS, HD), break_offset, cache_lengths,
        ffn_gain.reshape(16, HD), router_weight.T, expert_routes.T, expert_gate, expert_up,
        expert_down, shared_gate, shared_up, shared_down,
    )


def solution(mesh):
    torus = Mesh(mesh.devices.reshape(NZ, NX, NC, NT), (*EP, "tp"))
    return jax.shard_map(
        body,
        mesh=torus,
        in_specs=(
            P(EP, None),
            P(),
            P(EP, "tp"),
            P(EP, "tp"),
            P(EP, "tp"),
            P(EP, "tp"),
            P("tp"),
            P(EP, None, "tp", None),
            P(EP, None, "tp", None),
            P(EP, "tp", None),
            P(EP),
            P(),
            P(),
            P(EP, None),
            P(EP, None, "tp"),
            P(EP, None, "tp"),
            P(EP, "tp", None),
            P(None, "tp"),
            P(None, "tp"),
            P("tp", None),
        ),
        out_specs=(P(EP, "tp"), P(EP, "tp"), P(EP, "tp")),
        check_vma=False,
    )
```

```python
import jax
import jax.numpy as jnp
from jax import lax
from jax.experimental import pallas as pl
from jax.experimental.pallas import tpu as pltpu
from jax.sharding import Mesh
from jax.sharding import PartitionSpec as P

MESH = pl.DeviceIdType.MESH
EP = ("ep_0", "ep_1", "ep_2")
NZ, NX, NC, NT = 8, 4, 2, 4
NE = NZ * NX * NC
SEQ = 16
POS = 1024
HD = 128
EPS = 1e-06
SCALE = 2.5
F32 = jnp.float32
BF16 = jnp.bfloat16


def dot(a, b):
    return jnp.dot(a, b, preferred_element_type=F32)


def dot_nt(a, b):
    return lax.dot_general(a, b, (((1,), (1,)), ((), ())), preferred_element_type=F32)


def iota(shape, dim):
    return lax.broadcasted_iota(jnp.int32, shape, dim)


def ones_where(cond):
    return jnp.where(cond, 1.0, 0.0).astype(BF16)


def kernel(
    tok_h, ag_h, wq_h, wk_h, wv_h, wo_h, hg_h, pk_h, pv_h, off_h, lens, fg_h, rt_h, er_h,
    eg_h, eu_h, ed_h, sg_h, su_h, sd_h,
    mixed_o, fk_o, fv_o,
    tok, ag, hg, fg, rt, er, off, kb, vb, qb, kvb, ob, wgu, wd, sgu, sd,
    tkb, tk, part, qp, kvpart, kvp,
    qs, lg, lenb, ho, pc, sq, nf, res, sbuf, rbuf, xb, gs, gr, hs, obuf, cbuf, ssb, ssr,
    lsem, kvsem,
    qzs, qzr, kzs, kzr, ozs, ozr, oxs, oxr, ods, odr, tks, tkr, qps, qpr, kps, kpr,
    ys, yr, cs, cr, as_, ar, gss, gsr, hss, hsr, rs_, rr, sss, ssrr,
):
    z = lax.axis_index("ep_0")
    x = lax.axis_index("ep_1")
    c = lax.axis_index("ep_2")
    t = lax.axis_index("tp")
    e = (z * NX + x) * NC + c
    m = x * NC + c
    zd = [lax.rem(z + d, NZ) for d in range(NZ)]
    xd = [lax.rem(x + d, NX) for d in range(NX)]
    td = [lax.rem(t + d, NT) for d in range(NT)]
    cd = [c, 1 - c]
    mates = [(2, 0), (2, 1), (1, 0), (3, 0), (1, 1), (3, 1), (0, 1)]
    far_first = [4, 3, 5, 2, 6, 1, 7]
    near_first = far_first[::-1]

    def remote(src, dst, ssem, rsem, dev):
        return pltpu.make_async_remote_copy(
            src_ref=src, dst_ref=dst, send_sem=ssem, recv_sem=rsem,
            device_id=dev, device_id_type=MESH,
        )

    pending = []

    def send(src, dst, ssem, rsem, dev):
        cp = remote(src, dst, ssem, rsem, dev)
        cp.start()
        pending.append(cp)

    def arrived(dst, ssem, rsem):
        remote(dst, dst, ssem, rsem, (z, x, 1 - c, t)).wait_recv()

    loads = []

    def load(src, dst):
        cp = pltpu.make_async_copy(src, dst, lsem.at[len(loads)])
        cp.start()
        loads.append(cp)
        return cp

    ld_q = load(wq_h, qb.at[z])
    ld_tok = [load(tok_h, tok), load(ag_h, ag)]
    ld_o = load(wo_h, ob.at[z, x, c])
    ld_kv = [
        load(wk_h, kvb.at[z, :, pl.ds(0, 128)]),
        load(wv_h, kvb.at[z, :, pl.ds(128, 128)]),
    ]
    ld_er = load(er_h, er)
    ld_att = [load(off_h, off), load(hg_h, hg)]
    kv_loads = []
    for i in range(4):
        ds = pl.ds(4 * i, 4)
        kv_loads.append(pltpu.make_async_copy(pk_h.at[ds], kb.at[ds], kvsem.at[i]))
        kv_loads.append(pltpu.make_async_copy(pv_h.at[ds], vb.at[ds], kvsem.at[4 + i]))
    for cp in kv_loads:
        cp.start()
    ld_ffn = [load(fg_h, fg), load(rt_h, rt)]
    ld_sh = [
        load(sg_h, sgu.at[:, pl.ds(0, 128)]),
        load(su_h, sgu.at[:, pl.ds(128, 128)]),
        load(sd_h, sd),
    ]
    mine = pl.ds(pl.multiple_of(t * 512, 512), 512)
    ld_ex = [
        load(eg_h.at[0, mine, :], wgu.at[t, :, pl.ds(0, 128)]),
        load(eu_h.at[0, mine, :], wgu.at[t, :, pl.ds(128, 128)]),
        load(ed_h.at[0, :, mine], wd.at[t]),
    ]

    barrier = pltpu.get_barrier_semaphore()
    first = [(zd[d], x, c, t) for d in range(1, NZ)]
    first += [(z, xd[dx], cd[dc], t) for dx, dc in mates]
    first += [(z, x, c, td[d]) for d in range(1, NT)]
    for dev in first:
        pl.semaphore_signal(barrier, inc=1, device_id=dev, device_id_type=MESH)
    pl.semaphore_wait(barrier, len(first))

    ld_q.wait()
    for d in far_first:
        send(qb.at[z], qb.at[z], qzs.at[d], qzr.at[d], (zd[d], x, c, t))

    for cp in ld_tok:
        cp.wait()
    data = tok[...].astype(F32)
    factor = lax.rsqrt(jnp.mean(data * data, axis=-1, keepdims=True) + EPS)
    gain = ag[...].astype(F32)
    blocks = []
    for i in range(NZ):
        halves = []
        for k in (2 * i, 2 * i + 1):
            halves.append(data[:, HD * k : HD * k + HD] * factor * gain[k : k + 1, :])
        blocks.append(jnp.concatenate(halves, axis=1).astype(BF16).astype(F32))
    chunk = iota((SEQ, 256), 1) >> 5
    for g in range(8):
        own = blocks[g]
        for k in range(1, 8):
            j = (g + k) % 8
            own = jnp.where(chunk == j, pltpu.roll(blocks[j], 32 * k, 1), own)
        part[g] = own
    for dx, dc in mates:
        g = xd[dx] * NC + cd[dc]
        tkb[g] = part[g].astype(BF16)
        send(tkb.at[g], tk.at[m], tks.at[dx, dc], tkr.at[dx, dc], (z, xd[dx], cd[dc], t))
    tk[m] = part[m].astype(BF16)

    ld_o.wait()
    mine_o = ob.at[z, x, c]
    for d in far_first:
        send(mine_o, mine_o, ozs.at[d], ozr.at[d], (zd[d], x, c, t))

    def o_along(r):
        src = ob.at[zd[r], x, c]
        for i in (2, 1, 3):
            send(src, src, oxs.at[r, i], oxr.at[r, i], (z, xd[i], c, t))

    def o_forward(r):
        src = ob.at[zd[r], x, c]
        arrived(src, ozs.at[NZ - r], ozr.at[NZ - r])
        o_along(r)

    def o_across(r):
        for i in (1, 3, 2):
            arrived(ob.at[zd[r], xd[i], c], oxs.at[r, NX - i], oxr.at[r, NX - i])
        src = ob.at[zd[r], :, c]
        send(src, src, ods.at[r], odr.at[r], (z, x, 1 - c, t))

    def o_last():
        for r in range(NZ):
            arrived(ob.at[zd[r], :, 1 - c], ods.at[r], odr.at[r])

    o_along(0)
    for cp in ld_kv:
        cp.wait()
    for d in far_first:
        send(kvb.at[z], kvb.at[z], kzs.at[d], kzr.at[d], (zd[d], x, c, t))

    for d in (1, 3, 2):
        p = td[d]
        dev = (z, x, c, p)
        theirs = pl.ds(pl.multiple_of(p * 512, 512), 512)
        for k, src in enumerate((eg_h, eu_h)):
            half = pl.ds(128 * k, 128)
            send(src.at[0, theirs, :], wgu.at[t, :, half], ys.at[k, d], yr.at[k, d], dev)
        send(ed_h.at[0, :, theirs], wd.at[t], ys.at[2, d], yr.at[2, d], dev)

    ld_er.wait()
    rows = NE * SEQ
    chosen = iota((NE, SEQ), 0) == er[0:1, :]
    for k in range(1, 6):
        chosen = chosen | (iota((NE, SEQ), 0) == er[k : k + 1, :])
    hot_t = ones_where(chosen)
    before = ones_where(iota((SEQ, SEQ), 0) < iota((SEQ, SEQ), 1))
    code_t = jnp.where(chosen, dot(hot_t, before) + 1.0, 0.0).astype(BF16)
    repeat = ones_where((iota((SEQ, 64), 1) & 15) == iota((SEQ, 64), 0))
    eye = ones_where(iota((SEQ, SEQ), 0) == iota((SEQ, SEQ), 1))
    code4_t = dot(code_t, repeat).astype(BF16)
    code = dot_nt(eye, code_t)
    r0 = iota((rows, 64), 0)
    c0 = iota((rows, 64), 1)
    spread = ones_where((r0 >> 4) == c0)
    slot_of = dot(spread, code4_t)
    want = ((r0 & 3) + 1).astype(F32)
    dispatch = ones_where((slot_of == want) & (((r0 >> 2) & 3) == (c0 >> 4)))

    for dx, dc in mates:
        src = tk.at[lax.rem(x + NX - dx, NX) * NC + cd[dc]]
        arrived(src, tks.at[dx, dc], tkr.at[dx, dc])
    for d in near_first:
        arrived(qb.at[lax.rem(z + NZ - d, NZ)], qzs.at[d], qzr.at[d])
    rows_in = tk[...].reshape(8 * SEQ, 256)
    part[...] = dot(rows_in, qb[...].reshape(256, 256)).reshape(8, SEQ, 256)
    for dx, dc in mates:
        g = xd[dx] * NC + cd[dc]
        send(part.at[g], qp.at[m], qps.at[dx, dc], qpr.at[dx, dc], (z, xd[dx], cd[dc], t))
    qp[m] = part[m]
    for r in (7, 1, 6, 2, 5, 3, 4):
        o_forward(r)
    for dx, dc in mates:
        src = qp.at[lax.rem(x + NX - dx, NX) * NC + cd[dc]]
        arrived(src, qps.at[dx, dc], qpr.at[dx, dc])
    total = qp[0]
    for i in range(1, 8):
        total = total + qp[i]
    queries = total.astype(BF16).astype(F32)

    for h in range(2):
        qs[pl.ds(h, SEQ, stride=2), :] = queries[:, HD * h : HD * h + HD]
    for cp in ld_att:
        cp.wait()
    for b in range(SEQ):
        if b % 4 == 0:
            kv_loads[2 * (b // 4)].wait()
        q = qs[2 * b : 2 * b + 2, :].astype(BF16)
        lg[2 * b : 2 * b + 2, :] = dot_nt(q, kb[b]) * HD ** (-0.5) + off[b]
        lenb[2 * b : 2 * b + 2, :] = jnp.full((2, HD), lens[b], jnp.int32)
    for r in (0, 7, 1):
        o_across(r)
    logits = lg[...]
    length = lenb[:, 0:1]
    usable = iota((2 * SEQ, POS), 1) < length
    tail = jnp.log(1.0 + jnp.exp(-jnp.abs(logits)))
    keep = jnp.where(usable, jnp.minimum(-logits, 0.0) - tail, 0.0)
    nb = POS // HD
    stacked = jnp.concatenate([keep[:, HD * i : HD * i + HD] for i in range(nb)], axis=0)
    k1 = stacked.astype(BF16)
    left = stacked - k1.astype(F32)
    k2 = left.astype(BF16)
    k3 = (left - k2.astype(F32)).astype(BF16)
    later = ones_where(iota((HD, HD), 0) > iota((HD, HD), 1))
    inner = dot(k1, later) + dot(k2, later) + dot(k3, later)
    carry = jnp.zeros((2 * SEQ, 1), F32)
    after = [None] * nb
    n2 = 2 * SEQ
    for i in range(nb - 1, -1, -1):
        after[i] = inner[n2 * i : n2 * i + n2] + carry
        carry = carry + jnp.sum(stacked[n2 * i : n2 * i + n2], axis=-1, keepdims=True)
    after = jnp.concatenate(after, axis=1)
    sticks = jnp.where(usable, jnp.exp(jnp.minimum(logits, 0.0) - tail + after), 0.0)
    lg[...] = sticks
    for r in (6, 2):
        o_across(r)
    for b in range(SEQ):
        if b % 4 == 0:
            kv_loads[2 * (b // 4) + 1].wait()
        got = dot(lg[2 * b : 2 * b + 2, :].astype(BF16), vb[b])
        ho[b : b + 1, 0:HD] = got[0:1, :]
        ho[b : b + 1, HD : 2 * HD] = got[1:2, :]
    for r in (5, 3, 4):
        o_across(r)
    heads_out = ho[...]
    scaled = jnp.concatenate(
        [heads_out[:, HD * i : HD * i + HD] * hg[i : i + 1, :].astype(F32) for i in range(2)],
        axis=1,
    ).astype(BF16)
    sq[t] = jnp.broadcast_to(jnp.sum(heads_out * heads_out, axis=-1, keepdims=True), (SEQ, HD))
    o_last()
    for zi in range(NZ):
        part = dot_nt(scaled, ob[zi].reshape(256, 256))
        pc[t, :, 256 * zi : 256 * zi + 256] = part.astype(BF16)

    for d in (2, 1, 3):
        for k, buf in enumerate((sq, pc)):
            send(buf.at[t], buf.at[t], cs.at[k, d], cr.at[k, d], (z, x, c, td[d]))
    for d in near_first:
        arrived(kvb.at[lax.rem(z + NZ - d, NZ)], kzs.at[d], kzr.at[d])
    kvpart[...] = dot(rows_in, kvb[...].reshape(256, 256)).astype(BF16).reshape(8, SEQ, 256)
    for dx, dc in mates:
        g = xd[dx] * NC + cd[dc]
        send(kvpart.at[g], kvp.at[m], kps.at[dx, dc], kpr.at[dx, dc], (z, xd[dx], cd[dc], t))
    kvp[m] = kvpart[m]
    for d in (1, 3, 2):
        src = td[NT - d]
        for k, buf in enumerate((sq, pc)):
            arrived(buf.at[src], cs.at[k, d], cr.at[k, d])
    head_total = pc[0].astype(F32)
    square = sq[0]
    for i in range(1, NT):
        head_total = head_total + pc[i].astype(F32)
        square = square + sq[i]
    attention = head_total * lax.rsqrt(square[:, 0:1] / 1024.0 + EPS)
    residual = (tok[...].astype(F32) + attention).astype(BF16)
    for i in range(NT):
        res[i] = residual[:, 512 * i : 512 * i + 512]
    for cp in ld_ffn:
        cp.wait()
    data = residual.astype(F32)
    factor = lax.rsqrt(jnp.mean(data * data, axis=-1, keepdims=True) + EPS)
    gain = fg[...].astype(F32)
    pieces = []
    for i in range(16):
        pieces.append(data[:, HD * i : HD * i + HD] * factor * gain[i : i + 1, :])
        nf[i] = pieces[i].astype(BF16)
    normed_ffn = jnp.concatenate(pieces, axis=1).astype(BF16)

    def to_all(src, dst, ssem, rsem):
        for d in far_first + [0]:
            for dx, dc in ([(0, 0)] if d else []) + mates:
                p = (zd[d] * NX + xd[dx]) * NC + cd[dc]
                remote(src.at[p], dst.at[e], ssem, rsem, (zd[d], xd[dx], cd[dc], t)).start()

    block = nf[pl.ds(4 * t, 4)].reshape(64, HD)
    sbuf[...] = dot(dispatch, block).astype(BF16).reshape(NE, SEQ, HD)

    to_all(sbuf, rbuf, as_, ar)

    rbuf[e] = sbuf[e]

    for cp in ld_sh:
        cp.wait()
    both = dot(normed_ffn, sgu[...])
    gate = both[:, 0:HD]
    shared_hidden = (gate / (1.0 + jnp.exp(-gate)) * both[:, HD : 2 * HD]).astype(BF16)
    shared_part = dot(shared_hidden, sd[...]).astype(BF16)
    for i in range(NT):
        ssb[i] = shared_part[:, 512 * i : 512 * i + 512]
    for d in (2, 1, 3):
        p = td[d]
        send(ssb.at[p], ssr.at[t], sss.at[d], ssrr.at[d], (z, x, c, p))
    ssr[t] = ssb[t]
    logit = dot_nt(normed_ffn, rt[...])
    prob = 1.0 / (1.0 + jnp.exp(-logit))
    picked = jnp.where(code > 0.5, prob, 0.0)
    weight = SCALE * picked / jnp.sum(picked, axis=-1, keepdims=True)
    weight4 = jnp.concatenate([weight] * 4, axis=0)
    w_hi = weight4.astype(BF16)
    w_lo = (weight4 - w_hi.astype(F32)).astype(BF16)
    code4 = jnp.concatenate([code] * 4, axis=0).astype(BF16)
    r1 = iota((64, rows), 1)
    c1 = iota((64, rows), 0)
    spread_t = ones_where((r1 >> 4) == c1)
    slot_to = dot(code4, spread_t)
    fits = (slot_to == ((r1 & 3) + 1).astype(F32)) & (((r1 >> 2) & 3) == (c1 >> 4))
    comb_hi = jnp.where(fits, dot(w_hi, spread_t), 0.0).astype(BF16)
    comb_lo = jnp.where(fits, dot(w_lo, spread_t), 0.0).astype(BF16)

    def everyone(buf):
        return buf.at[pl.ds(0, NE - 1)]

    def wait_all(src, dst, ssem, rsem):
        cp = remote(everyone(src), everyone(dst), ssem, rsem, (z, x, 1 - c, t))
        cp.wait_recv()
        cp.wait_send()

    wait_all(sbuf, rbuf, as_, ar)

    p48 = iota((48, 256), 0)
    q48 = iota((48, 256), 1)
    for g in range(4):
        group = rbuf[16 * g : 16 * g + 16].reshape(256, HD)
        for j in range(4):
            pick = ones_where(q48 == ((p48 & 15) << 4) + 4 * j + (p48 >> 4))
            xb[48 * g : 48 * g + 48, HD * j : HD * j + HD] = dot(pick, group).astype(BF16)
    for cp in ld_ex:
        cp.wait()
    for d in (1, 3, 2):
        src = td[NT - d]
        for k in range(2):
            arrived(wgu.at[src, :, pl.ds(128 * k, 128)], ys.at[k, d], yr.at[k, d])
        arrived(wd.at[src], ys.at[2, d], yr.at[2, d])
    xv = xb[...]
    for d in (2, 1, 3):
        gs[d] = dot(xv, wgu[td[d]]).astype(BF16)
        send(gs.at[d], gr.at[d], gss.at[d], gsr.at[d], (z, x, c, td[d]))
    gate_up = dot(xv, wgu[t])
    for d in (2, 1, 3):
        arrived(gr.at[d], gss.at[d], gsr.at[d])
        gate_up = gate_up + gr[d].astype(F32)
    gate = gate_up[:, 0:HD]
    hidden = (gate / (1.0 + jnp.exp(-gate)) * gate_up[:, HD : 2 * HD]).astype(BF16)
    hs[t] = hidden
    for d in (2, 1, 3):
        send(hs.at[t], hs.at[t], hss.at[d], hsr.at[d], (z, x, c, td[d]))
    for d in (2, 1, 3):
        arrived(hs.at[td[NT - d]], hss.at[d], hsr.at[d])
    out = dot(hs[0], wd[0])
    for i in range(1, NT):
        out = out + dot(hs[i], wd[i])
    out = out.astype(BF16)

    pt = iota((256, 48), 1)
    qt = iota((256, 48), 0)
    for g in range(4):
        back = jnp.zeros((256, HD), F32)
        for j in range(4):
            pick = ones_where(qt == ((pt & 15) << 4) + 4 * j + (pt >> 4))
            back = back + dot(pick, out[48 * g : 48 * g + 48, HD * j : HD * j + HD])
        obuf[16 * g : 16 * g + 16] = back.astype(BF16).reshape(16, 16, HD)

    to_all(obuf, cbuf, rs_, rr)

    cbuf[e] = obuf[e]
    shared_total = jnp.zeros((SEQ, 512), F32)
    for d in (2, 1, 3):
        arrived(ssr.at[td[NT - d]], sss.at[d], ssrr.at[d])
    for i in range(NT):
        shared_total = shared_total + ssr[i].astype(F32)
    base = res[t].astype(F32) + shared_total
    for dx, dc in mates:
        src = kvp.at[lax.rem(x + NX - dx, NX) * NC + cd[dc]]
        arrived(src, kps.at[dx, dc], kpr.at[dx, dc])
    fresh = kvp[0].astype(F32)
    for i in range(1, 8):
        fresh = fresh + kvp[i].astype(F32)
    fk_o[...] = fresh[:, 0:HD].astype(BF16)
    fv_o[...] = fresh[:, HD : 2 * HD].astype(BF16)
    wait_all(obuf, cbuf, rs_, rr)
    came = cbuf[...].reshape(rows, HD)
    routed = dot(comb_hi, came) + dot(comb_lo, came)
    for j in range(4):
        mixed_o[:, HD * j : HD * j + HD] = (
            base[:, HD * j : HD * j + HD] + routed[SEQ * j : SEQ * j + SEQ]
        ).astype(BF16)
    for cp in pending:
        cp.wait_send()


def body(
    tokens, attn_gain, query_weight, key_weight, value_weight, out_weight, head_gain,
    past_keys, past_values, break_offset, cache_lengths, ffn_gain, router_weight,
    expert_routes, expert_gate, expert_up, expert_down, shared_gate, shared_up, shared_down,
):
    hbm = pl.BlockSpec(memory_space=pl.ANY)
    vmem = pl.BlockSpec(memory_space=pltpu.VMEM)
    smem = pl.BlockSpec(memory_space=pltpu.SMEM)
    v, dma = pltpu.VMEM, pltpu.SemaphoreType.DMA
    return pl.pallas_call(
        kernel,
        out_shape=(
            jax.ShapeDtypeStruct((SEQ, 512), BF16),
            jax.ShapeDtypeStruct((SEQ, HD), BF16),
            jax.ShapeDtypeStruct((SEQ, HD), BF16),
        ),
        in_specs=[smem if i == 10 else hbm for i in range(20)],
        out_specs=(vmem, vmem, vmem),
        scratch_shapes=[
            v((SEQ, 2048), BF16), v((16, HD), BF16), v((2, HD), BF16), v((16, HD), BF16),
            v((64, 2048), BF16), v((6, SEQ), jnp.int32), v((SEQ, 2, POS), F32),
            v((SEQ, POS, HD), BF16), v((SEQ, POS, HD), BF16),
            v((NZ, 32, 256), BF16), v((NZ, 32, 256), BF16), v((NZ, NX, NC, 32, 256), BF16),
            v((NT, 512, 256), BF16), v((NT, 128, 512), BF16),
            v((2048, 256), BF16), v((128, 2048), BF16),
            v((8, SEQ, 256), BF16), v((8, SEQ, 256), BF16),
            v((8, SEQ, 256), F32), v((8, SEQ, 256), F32),
            v((8, SEQ, 256), BF16), v((8, SEQ, 256), BF16),
            v((2 * SEQ, HD), F32), v((2 * SEQ, POS), F32), v((2 * SEQ, HD), jnp.int32),
            v((SEQ, 256), F32), v((NT, SEQ, 2048), BF16), v((NT, SEQ, HD), F32),
            v((16, SEQ, HD), BF16), v((NT, SEQ, 512), BF16),
            v((NE, SEQ, HD), BF16), v((NE, SEQ, HD), BF16), v((192, 512), BF16),
            v((NT, 192, 256), BF16), v((NT, 192, 256), BF16), v((NT, 192, HD), BF16),
            v((NE, SEQ, HD), BF16), v((NE, SEQ, HD), BF16),
            v((NT, SEQ, 512), BF16), v((NT, SEQ, 512), BF16),
            dma((24,)), dma((8,)),
            *[dma((NZ,)) for _ in range(6)],
            dma((NZ, NX)), dma((NZ, NX)), dma((NZ,)), dma((NZ,)),
            *[dma((NX, NC)) for _ in range(6)],
            dma((3, 4)), dma((3, 4)), dma((2, 4)), dma((2, 4)), dma, dma,
            dma((4,)), dma((4,)), dma((4,)), dma((4,)), dma, dma, dma((4,)), dma((4,)),
        ],
        compiler_params=pltpu.CompilerParams(
            collective_id=0, has_side_effects=True, vmem_limit_bytes=60 * 1024 * 1024
        ),
    )(
        tokens, attn_gain.reshape(16, HD), query_weight, key_weight, value_weight, out_weight,
        head_gain.reshape(2, HD), past_keys.reshape(SEQ, POS, HD),
        past_values.reshape(SEQ, POS, HD), break_offset, cache_lengths,
        ffn_gain.reshape(16, HD), router_weight.T, expert_routes.T, expert_gate, expert_up,
        expert_down, shared_gate, shared_up, shared_down,
    )


def solution(mesh):
    torus = Mesh(mesh.devices.reshape(NZ, NX, NC, NT), (*EP, "tp"))
    return jax.shard_map(
        body,
        mesh=torus,
        in_specs=(
            P(EP, None),
            P(),
            P(EP, "tp"),
            P(EP, "tp"),
            P(EP, "tp"),
            P(EP, "tp"),
            P("tp"),
            P(EP, None, "tp", None),
            P(EP, None, "tp", None),
            P(EP, "tp", None),
            P(EP),
            P(),
            P(),
            P(EP, None),
            P(EP, None, "tp"),
            P(EP, None, "tp"),
            P(EP, "tp", None),
            P(None, "tp"),
            P(None, "tp"),
            P("tp", None),
        ),
        out_specs=(P(EP, "tp"), P(EP, "tp"), P(EP, "tp")),
        check_vma=False,
    )
```

```python
import jax
import jax.numpy as jnp
from jax import lax
from jax.experimental import pallas as pl
from jax.experimental.pallas import tpu as pltpu
from jax.sharding import Mesh
from jax.sharding import PartitionSpec as P

MESH = pl.DeviceIdType.MESH
EP = ("ep_0", "ep_1", "ep_2")
NZ, NX, NC, NT = 8, 4, 2, 4
NE = NZ * NX * NC
SEQ = 16
POS = 1024
HD = 128
EPS = 1e-06
SCALE = 2.5
F32 = jnp.float32
BF16 = jnp.bfloat16


def dot(a, b):
    return jnp.dot(a, b, preferred_element_type=F32)


def dot_nt(a, b):
    return lax.dot_general(a, b, (((1,), (1,)), ((), ())), preferred_element_type=F32)


def iota(shape, dim):
    return lax.broadcasted_iota(jnp.int32, shape, dim)


def ones_where(cond):
    return jnp.where(cond, 1.0, 0.0).astype(BF16)


def kernel(
    tok_h, ag_h, wq_h, wk_h, wv_h, wo_h, hg_h, pk_h, pv_h, off_h, lens, fg_h, rt_h, er_h,
    eg_h, eu_h, ed_h, sg_h, su_h, sd_h,
    mixed_o, fk_o, fv_o,
    tok, ag, hg, fg, rt, er, off, kb, vb, qb, kvb, ob, wgu, wd, sgu, sd,
    tkb, tk, part, qp, kvpart, kvp,
    qs, lg, lenb, ho, pc, sq, nf, res, sbuf, rbuf, gs, gr, hs, obuf, cbuf, ssb, ssr,
    lsem, kvsem,
    qzs, qzr, kzs, kzr, ozs, ozr, oxs, oxr, ods, odr, tks, tkr, qps, qpr, kps, kpr,
    ys, yr, cs, cr, as_, ar, gss, gsr, hss, hsr, rs_, rr, sss, ssrr,
):
    z = lax.axis_index("ep_0")
    x = lax.axis_index("ep_1")
    c = lax.axis_index("ep_2")
    t = lax.axis_index("tp")
    e = (z * NX + x) * NC + c
    m = x * NC + c
    zd = [lax.rem(z + d, NZ) for d in range(NZ)]
    xd = [lax.rem(x + d, NX) for d in range(NX)]
    td = [lax.rem(t + d, NT) for d in range(NT)]
    cd = [c, 1 - c]
    mates = [(2, 0), (2, 1), (1, 0), (3, 0), (1, 1), (3, 1), (0, 1)]
    far_first = [4, 3, 5, 2, 6, 1, 7]
    near_first = far_first[::-1]

    def remote(src, dst, ssem, rsem, dev):
        return pltpu.make_async_remote_copy(
            src_ref=src, dst_ref=dst, send_sem=ssem, recv_sem=rsem,
            device_id=dev, device_id_type=MESH,
        )

    pending = []

    def send(src, dst, ssem, rsem, dev):
        cp = remote(src, dst, ssem, rsem, dev)
        cp.start()
        pending.append(cp)

    def arrived(dst, ssem, rsem):
        remote(dst, dst, ssem, rsem, (z, x, 1 - c, t)).wait_recv()

    loads = []

    def load(src, dst):
        cp = pltpu.make_async_copy(src, dst, lsem.at[len(loads)])
        cp.start()
        loads.append(cp)
        return cp

    ld_q = load(wq_h, qb.at[z])
    ld_tok = [load(tok_h, tok), load(ag_h, ag)]
    ld_o = load(wo_h, ob.at[z, x, c])
    ld_kv = [
        load(wk_h, kvb.at[z, :, pl.ds(0, 128)]),
        load(wv_h, kvb.at[z, :, pl.ds(128, 128)]),
    ]
    ld_er = load(er_h, er)
    ld_att = [load(off_h, off), load(hg_h, hg)]
    kv_loads = []
    for i in range(4):
        ds = pl.ds(4 * i, 4)
        kv_loads.append(pltpu.make_async_copy(pk_h.at[ds], kb.at[ds], kvsem.at[i]))
        kv_loads.append(pltpu.make_async_copy(pv_h.at[ds], vb.at[ds], kvsem.at[4 + i]))
    for cp in kv_loads:
        cp.start()
    ld_ffn = [load(fg_h, fg), load(rt_h, rt)]
    ld_sh = [
        load(sg_h, sgu.at[:, pl.ds(0, 128)]),
        load(su_h, sgu.at[:, pl.ds(128, 128)]),
        load(sd_h, sd),
    ]
    mine = pl.ds(pl.multiple_of(t * 512, 512), 512)
    ld_ex = [
        load(eg_h.at[0, mine, :], wgu.at[t, :, pl.ds(0, 128)]),
        load(eu_h.at[0, mine, :], wgu.at[t, :, pl.ds(128, 128)]),
        load(ed_h.at[0, :, mine], wd.at[t]),
    ]

    barrier = pltpu.get_barrier_semaphore()
    first = [(zd[d], x, c, t) for d in range(1, NZ)]
    first += [(z, xd[dx], cd[dc], t) for dx, dc in mates]
    first += [(z, x, c, td[d]) for d in range(1, NT)]
    for dev in first:
        pl.semaphore_signal(barrier, inc=1, device_id=dev, device_id_type=MESH)

    for cp in ld_tok:
        cp.wait()
    data = tok[...].astype(F32)
    factor = lax.rsqrt(jnp.mean(data * data, axis=-1, keepdims=True) + EPS)
    gain = ag[...].astype(F32)
    blocks = []
    for i in range(NZ):
        halves = []
        for k in (2 * i, 2 * i + 1):
            halves.append(data[:, HD * k : HD * k + HD] * factor * gain[k : k + 1, :])
        blocks.append(jnp.concatenate(halves, axis=1).astype(BF16).astype(F32))
    chunk = iota((SEQ, 256), 1) >> 5
    for g in range(8):
        own = blocks[g]
        for k in range(1, 8):
            j = (g + k) % 8
            own = jnp.where(chunk == j, pltpu.roll(blocks[j], 32 * k, 1), own)
        tkb[g] = own.astype(BF16)
    ld_er.wait()
    rows = NE * 12
    chosen = iota((NE, SEQ), 0) == er[0:1, :]
    for k in range(1, 6):
        chosen = chosen | (iota((NE, SEQ), 0) == er[k : k + 1, :])
    hot_t = ones_where(chosen)
    before = ones_where(iota((SEQ, SEQ), 0) < iota((SEQ, SEQ), 1))
    code_t = jnp.where(chosen, dot(hot_t, before) + 1.0, 0.0).astype(BF16)
    repeat = ones_where((iota((SEQ, 64), 1) & 15) == iota((SEQ, 64), 0))
    eye = ones_where(iota((SEQ, SEQ), 0) == iota((SEQ, SEQ), 1))
    code4_t = dot(code_t, repeat).astype(BF16)
    code = dot_nt(eye, code_t)
    q0 = iota((rows, 64), 0) >> 2
    j0 = iota((rows, 64), 0) & 3
    e0 = (q0 * 171) >> 9
    c0 = iota((rows, 64), 1)
    spread = ones_where(e0 == c0)
    slot_of = dot(spread, code4_t)
    want = (q0 - 3 * e0 + 1).astype(F32)
    dispatch = ones_where((slot_of == want) & (j0 == (c0 >> 4)))

    pl.semaphore_wait(barrier, len(first))

    ld_q.wait()
    for d in far_first:
        send(qb.at[z], qb.at[z], qzs.at[d], qzr.at[d], (zd[d], x, c, t))

    for dx, dc in mates:
        g = xd[dx] * NC + cd[dc]
        send(tkb.at[g], tk.at[m], tks.at[dx, dc], tkr.at[dx, dc], (z, xd[dx], cd[dc], t))
    tk[m] = tkb[m]

    ld_o.wait()
    mine_o = ob.at[z, x, c]
    for d in far_first:
        send(mine_o, mine_o, ozs.at[d], ozr.at[d], (zd[d], x, c, t))

    def o_along(r):
        src = ob.at[zd[r], x, c]
        for i in (2, 1, 3):
            send(src, src, oxs.at[r, i], oxr.at[r, i], (z, xd[i], c, t))

    def o_forward(r):
        src = ob.at[zd[r], x, c]
        arrived(src, ozs.at[NZ - r], ozr.at[NZ - r])
        o_along(r)

    def o_across(r):
        for i in (1, 3, 2):
            arrived(ob.at[zd[r], xd[i], c], oxs.at[r, NX - i], oxr.at[r, NX - i])
        src = ob.at[zd[r], :, c]
        send(src, src, ods.at[r], odr.at[r], (z, x, 1 - c, t))

    def o_last():
        for r in range(NZ):
            arrived(ob.at[zd[r], :, 1 - c], ods.at[r], odr.at[r])

    o_along(0)
    for cp in ld_kv:
        cp.wait()
    for d in far_first:
        send(kvb.at[z], kvb.at[z], kzs.at[d], kzr.at[d], (zd[d], x, c, t))

    for d in (1, 3, 2):
        p = td[d]
        dev = (z, x, c, p)
        theirs = pl.ds(pl.multiple_of(p * 512, 512), 512)
        for k, src in enumerate((eg_h, eu_h)):
            half = pl.ds(128 * k, 128)
            send(src.at[0, theirs, :], wgu.at[t, :, half], ys.at[k, d], yr.at[k, d], dev)

    for dx, dc in mates:
        src = tk.at[lax.rem(x + NX - dx, NX) * NC + cd[dc]]
        arrived(src, tks.at[dx, dc], tkr.at[dx, dc])
    for r in (7, 1, 6, 2):
        o_forward(r)
    for d in near_first:
        arrived(qb.at[lax.rem(z + NZ - d, NZ)], qzs.at[d], qzr.at[d])
    rows_in = tk[...].reshape(8 * SEQ, 256)
    part[...] = dot(rows_in, qb[...].reshape(256, 256)).astype(BF16).reshape(8, SEQ, 256)
    for dx, dc in mates:
        g = xd[dx] * NC + cd[dc]
        send(part.at[g], qp.at[m], qps.at[dx, dc], qpr.at[dx, dc], (z, xd[dx], cd[dc], t))
    qp[m] = part[m]
    for r in (5, 3, 4):
        o_forward(r)
    for dx, dc in mates:
        src = qp.at[lax.rem(x + NX - dx, NX) * NC + cd[dc]]
        arrived(src, qps.at[dx, dc], qpr.at[dx, dc])
    total = qp[0].astype(F32)
    for i in range(1, 8):
        total = total + qp[i].astype(F32)
    queries = total.astype(BF16).astype(F32)

    for h in range(2):
        qs[pl.ds(h, SEQ, stride=2), :] = queries[:, HD * h : HD * h + HD]
    for cp in ld_att:
        cp.wait()
    for b in range(SEQ):
        if b % 4 == 0:
            kv_loads[2 * (b // 4)].wait()
        q = qs[2 * b : 2 * b + 2, :].astype(BF16)
        lg[2 * b : 2 * b + 2, :] = dot_nt(q, kb[b]) * HD ** (-0.5) + off[b]
        lenb[2 * b : 2 * b + 2, :] = jnp.full((2, HD), lens[b], jnp.int32)
    for r in (0, 7, 1):
        o_across(r)
    logits = lg[...]
    length = lenb[:, 0:1]
    usable = iota((2 * SEQ, POS), 1) < length
    tail = jnp.log(1.0 + jnp.exp(-jnp.abs(logits)))
    keep = jnp.where(usable, jnp.minimum(-logits, 0.0) - tail, 0.0)
    nb = POS // HD
    stacked = jnp.concatenate([keep[:, HD * i : HD * i + HD] for i in range(nb)], axis=0)
    k1 = stacked.astype(BF16)
    left = stacked - k1.astype(F32)
    k2 = left.astype(BF16)
    k3 = (left - k2.astype(F32)).astype(BF16)
    later = ones_where(iota((HD, HD), 0) > iota((HD, HD), 1))
    inner = dot(k1, later) + dot(k2, later) + dot(k3, later)
    carry = jnp.zeros((2 * SEQ, 1), F32)
    after = [None] * nb
    n2 = 2 * SEQ
    for i in range(nb - 1, -1, -1):
        after[i] = inner[n2 * i : n2 * i + n2] + carry
        carry = carry + jnp.sum(stacked[n2 * i : n2 * i + n2], axis=-1, keepdims=True)
    after = jnp.concatenate(after, axis=1)
    sticks = jnp.where(usable, jnp.exp(jnp.minimum(logits, 0.0) - tail + after), 0.0)
    lg[...] = sticks
    for r in (6, 2):
        o_across(r)
    for b in range(SEQ):
        if b % 4 == 0:
            kv_loads[2 * (b // 4) + 1].wait()
        got = dot(lg[2 * b : 2 * b + 2, :].astype(BF16), vb[b])
        ho[b : b + 1, 0:HD] = got[0:1, :]
        ho[b : b + 1, HD : 2 * HD] = got[1:2, :]
    for r in (5, 3, 4):
        o_across(r)
    heads_out = ho[...]
    scaled = jnp.concatenate(
        [heads_out[:, HD * i : HD * i + HD] * hg[i : i + 1, :].astype(F32) for i in range(2)],
        axis=1,
    ).astype(BF16)
    sq[t] = jnp.broadcast_to(jnp.sum(heads_out * heads_out, axis=-1, keepdims=True), (SEQ, HD))
    o_last()
    for zi in range(NZ):
        part = dot_nt(scaled, ob[zi].reshape(256, 256))
        pc[t, :, 256 * zi : 256 * zi + 256] = part.astype(BF16)

    for d in (2, 1, 3):
        for k, buf in enumerate((sq, pc)):
            send(buf.at[t], buf.at[t], cs.at[k, d], cr.at[k, d], (z, x, c, td[d]))
    for d in near_first:
        arrived(kvb.at[lax.rem(z + NZ - d, NZ)], kzs.at[d], kzr.at[d])
    kvpart[...] = dot(rows_in, kvb[...].reshape(256, 256)).astype(BF16).reshape(8, SEQ, 256)
    for dx, dc in mates:
        g = xd[dx] * NC + cd[dc]
        send(kvpart.at[g], kvp.at[m], kps.at[dx, dc], kpr.at[dx, dc], (z, xd[dx], cd[dc], t))
    kvp[m] = kvpart[m]
    for d in (1, 3, 2):
        src = td[NT - d]
        for k, buf in enumerate((sq, pc)):
            arrived(buf.at[src], cs.at[k, d], cr.at[k, d])
    head_total = pc[0].astype(F32)
    square = sq[0]
    for i in range(1, NT):
        head_total = head_total + pc[i].astype(F32)
        square = square + sq[i]
    attention = head_total * lax.rsqrt(square[:, 0:1] / 1024.0 + EPS)
    residual = (tok[...].astype(F32) + attention).astype(BF16)
    for i in range(NT):
        res[i] = residual[:, 512 * i : 512 * i + 512]
    for cp in ld_ffn:
        cp.wait()
    data = residual.astype(F32)
    factor = lax.rsqrt(jnp.mean(data * data, axis=-1, keepdims=True) + EPS)
    gain = fg[...].astype(F32)
    pieces = []
    for i in range(16):
        pieces.append(data[:, HD * i : HD * i + HD] * factor * gain[i : i + 1, :])
        nf[i] = pieces[i].astype(BF16)
    normed_ffn = jnp.concatenate(pieces, axis=1).astype(BF16)

    for d in (1, 3, 2):
        theirs = pl.ds(pl.multiple_of(td[d] * 512, 512), 512)
        send(ed_h.at[0, :, theirs], wd.at[t], ys.at[2, d], yr.at[2, d], (z, x, c, td[d]))
    block = nf[pl.ds(4 * t, 4)].reshape(64, HD)
    sbuf[...] = dot(dispatch, block).astype(BF16).reshape(3 * NE, 4, HD)
    order = (3, 4, 5, 6, 7, 0, 1, 2)

    def three(i):
        return pl.ds(3 * i, 3)

    def half_of(r):
        return order.index(r) // 4

    def around(r):
        return [(0, 0), *mates] if r else mates

    for r in (4, 5, 3, 6, 2, 7, 1, 0):
        d = (NZ - r) % NZ
        to = three(8 * order.index(r) + m)
        for dx, dc in around(r):
            p = (zd[d] * NX + xd[dx]) * NC + cd[dc]
            dev = (zd[d], xd[dx], cd[dc], t)
            remote(sbuf.at[three(p)], rbuf.at[to], as_.at[half_of(r)], ar.at[half_of(r)], dev).start()
    rbuf[three(8 * order.index(0) + m)] = sbuf[three(e)]

    for cp in ld_sh:
        cp.wait()
    both = dot(normed_ffn, sgu[...])
    gate = both[:, 0:HD]
    shared_hidden = (gate / (1.0 + jnp.exp(-gate)) * both[:, HD : 2 * HD]).astype(BF16)
    shared_part = dot(shared_hidden, sd[...]).astype(BF16)
    for i in range(NT):
        ssb[i] = shared_part[:, 512 * i : 512 * i + 512]
    for d in (2, 1, 3):
        p = td[d]
        send(ssb.at[p], ssr.at[t], sss.at[d], ssrr.at[d], (z, x, c, p))
    ssr[t] = ssb[t]
    logit = dot_nt(normed_ffn, rt[...])
    prob = 1.0 / (1.0 + jnp.exp(-logit))
    picked = jnp.where(code > 0.5, prob, 0.0)
    weight = SCALE * picked / jnp.sum(picked, axis=-1, keepdims=True)
    weight4 = jnp.concatenate([weight] * 4, axis=0)
    w_hi = weight4.astype(BF16)
    w_lo = (weight4 - w_hi.astype(F32)).astype(BF16)
    code4 = jnp.concatenate([code] * 4, axis=0).astype(BF16)
    q1 = iota((64, rows), 1) >> 2
    j1 = iota((64, rows), 1) & 3
    e1 = (q1 * 171) >> 9
    c1 = iota((64, rows), 0)
    spread_t = ones_where(e1 == c1)
    slot_to = dot(code4, spread_t)
    fits = (slot_to == (q1 - 3 * e1 + 1).astype(F32)) & (j1 == (c1 >> 4))
    comb_hi = jnp.where(fits, dot(w_hi, spread_t), 0.0).astype(BF16)
    comb_lo = jnp.where(fits, dot(w_lo, spread_t), 0.0).astype(BF16)

    def to_rows(half, g):
        group = rbuf[96 * half + 48 * g : 96 * half + 48 * g + 48].reshape(192, HD)
        p, q = iota((48, 192), 0), iota((48, 192), 1)
        cols = [dot(ones_where(q == 4 * p + j), group).astype(BF16) for j in range(4)]
        return jnp.concatenate(cols, axis=1)

    def start_half(half):
        n = 96 if half == 0 else 93
        both = remote(
            sbuf.at[pl.ds(0, n)], rbuf.at[pl.ds(0, n)], as_.at[half], ar.at[half],
            (z, x, 1 - c, t),
        )
        both.wait_recv()
        rows_of = jnp.concatenate([to_rows(half, 0), to_rows(half, 1)], axis=0)
        for d in (2, 1, 3):
            gs[half, d] = dot(rows_of, wgu[td[d]]).astype(BF16)
            send(gs.at[half, d], gr.at[half, d], gss.at[half, d], gsr.at[half, d], (z, x, c, td[d]))
        return dot(rows_of, wgu[t]), both

    def middle_half(half, gate_up):
        for d in (2, 1, 3):
            arrived(gr.at[half, d], gss.at[half, d], gsr.at[half, d])
            gate_up = gate_up + gr[half, d].astype(F32)
        gate = gate_up[:, 0:HD]
        hidden = gate / (1.0 + jnp.exp(-gate)) * gate_up[:, HD : 2 * HD]
        hs[half, t] = hidden.astype(BF16)
        for d in (2, 1, 3):
            own = hs.at[half, t]
            send(own, own, hss.at[half, d], hsr.at[half, d], (z, x, c, td[d]))

    def end_half(half):
        for d in (2, 1, 3):
            arrived(hs.at[half, td[NT - d]], hss.at[half, d], hsr.at[half, d])
        out = dot(hs[half, 0], wd[0])
        for i in range(1, NT):
            out = out + dot(hs[half, i], wd[i])
        out = out.astype(BF16)
        p, q = iota((192, 48), 1), iota((192, 48), 0)
        for g in range(2):
            back = jnp.zeros((192, HD), F32)
            for j in range(4):
                block = out[48 * g : 48 * g + 48, HD * j : HD * j + HD]
                back = back + dot(ones_where(q == 4 * p + j), block)
            at = 96 * half + 48 * g
            obuf[at : at + 48] = back.astype(BF16).reshape(48, 4, HD)
        for r in ((4, 5, 3, 6) if half == 0 else (2, 7, 1, 0)):
            for dx, dc in around(r):
                p = 8 * order.index(r) + xd[dx] * NC + cd[dc]
                dev = (zd[r], xd[dx], cd[dc], t)
                remote(obuf.at[three(p)], cbuf.at[three(e)], rs_, rr, dev).start()

    for cp in ld_ex:
        cp.wait()
    for d in (1, 3, 2):
        src = td[NT - d]
        for k in range(2):
            arrived(wgu.at[src, :, pl.ds(128 * k, 128)], ys.at[k, d], yr.at[k, d])
    gate_up0, sent0 = start_half(0)
    gate_up1, sent1 = start_half(1)
    middle_half(0, gate_up0)
    middle_half(1, gate_up1)
    for d in (1, 3, 2):
        arrived(wd.at[td[NT - d]], ys.at[2, d], yr.at[2, d])
    end_half(0)
    end_half(1)
    cbuf[three(e)] = obuf[three(8 * order.index(0) + m)]
    shared_total = jnp.zeros((SEQ, 512), F32)
    for d in (2, 1, 3):
        arrived(ssr.at[td[NT - d]], sss.at[d], ssrr.at[d])
    for i in range(NT):
        shared_total = shared_total + ssr[i].astype(F32)
    base = res[t].astype(F32) + shared_total
    for dx, dc in mates:
        src = kvp.at[lax.rem(x + NX - dx, NX) * NC + cd[dc]]
        arrived(src, kps.at[dx, dc], kpr.at[dx, dc])
    fresh = kvp[0].astype(F32)
    for i in range(1, 8):
        fresh = fresh + kvp[i].astype(F32)
    fk_o[...] = fresh[:, 0:HD].astype(BF16)
    fv_o[...] = fresh[:, HD : 2 * HD].astype(BF16)
    back = remote(
        obuf.at[pl.ds(0, 3 * NE - 3)], cbuf.at[pl.ds(0, 3 * NE - 3)], rs_, rr, (z, x, 1 - c, t)
    )
    back.wait_recv()
    came = cbuf[...].reshape(rows, HD)
    routed = dot(comb_hi, came) + dot(comb_lo, came)
    for j in range(4):
        mixed_o[:, HD * j : HD * j + HD] = (
            base[:, HD * j : HD * j + HD] + routed[SEQ * j : SEQ * j + SEQ]
        ).astype(BF16)
    for cp in [*pending, sent0, sent1, back]:
        cp.wait_send()


def hand_over(a, b, c, a_o, b_o, c_o, sem):
    moves = []
    for i, (src, dst) in enumerate(((a, a_o), (b, b_o), (c, c_o))):
        moves.append(pltpu.make_async_copy(src, dst, sem.at[i]))
        moves[i].start()
    for cp in moves:
        cp.wait()


def body(
    tokens, attn_gain, query_weight, key_weight, value_weight, out_weight, head_gain,
    past_keys, past_values, break_offset, cache_lengths, ffn_gain, router_weight,
    expert_routes, expert_gate, expert_up, expert_down, shared_gate, shared_up, shared_down,
):
    hbm = pl.BlockSpec(memory_space=pl.ANY)
    vmem = pl.BlockSpec(memory_space=pltpu.VMEM)
    smem = pl.BlockSpec(memory_space=pltpu.SMEM)
    v, dma = pltpu.VMEM, pltpu.SemaphoreType.DMA
    outs = pl.pallas_call(
        kernel,
        out_shape=(
            jax.ShapeDtypeStruct((SEQ, 512), BF16),
            jax.ShapeDtypeStruct((SEQ, HD), BF16),
            jax.ShapeDtypeStruct((SEQ, HD), BF16),
        ),
        in_specs=[smem if i == 10 else hbm for i in range(20)],
        out_specs=(vmem, vmem, vmem),
        scratch_shapes=[
            v((SEQ, 2048), BF16), v((16, HD), BF16), v((2, HD), BF16), v((16, HD), BF16),
            v((64, 2048), BF16), v((6, SEQ), jnp.int32), v((SEQ, 2, POS), F32),
            v((SEQ, POS, HD), BF16), v((SEQ, POS, HD), BF16),
            v((NZ, 32, 256), BF16), v((NZ, 32, 256), BF16), v((NZ, NX, NC, 32, 256), BF16),
            v((NT, 512, 256), BF16), v((NT, 128, 512), BF16),
            v((2048, 256), BF16), v((128, 2048), BF16),
            v((8, SEQ, 256), BF16), v((8, SEQ, 256), BF16),
            v((8, SEQ, 256), BF16), v((8, SEQ, 256), BF16),
            v((8, SEQ, 256), BF16), v((8, SEQ, 256), BF16),
            v((2 * SEQ, HD), F32), v((2 * SEQ, POS), F32), v((2 * SEQ, HD), jnp.int32),
            v((SEQ, 256), F32), v((NT, SEQ, 2048), BF16), v((NT, SEQ, HD), F32),
            v((16, SEQ, HD), BF16), v((NT, SEQ, 512), BF16),
            v((3 * NE, 4, HD), BF16), v((3 * NE, 4, HD), BF16),
            v((2, NT, 96, 256), BF16), v((2, NT, 96, 256), BF16), v((2, NT, 96, HD), BF16),
            v((3 * NE, 4, HD), BF16), v((3 * NE, 4, HD), BF16),
            v((NT, SEQ, 512), BF16), v((NT, SEQ, 512), BF16),
            dma((24,)), dma((8,)),
            *[dma((NZ,)) for _ in range(6)],
            dma((NZ, NX)), dma((NZ, NX)), dma((NZ,)), dma((NZ,)),
            *[dma((NX, NC)) for _ in range(6)],
            dma((3, 4)), dma((3, 4)), dma((2, 4)), dma((2, 4)), dma((2,)), dma((2,)),
            dma((2, 4)), dma((2, 4)), dma((2, 4)), dma((2, 4)), dma, dma, dma((4,)), dma((4,)),
        ],
        compiler_params=pltpu.CompilerParams(
            collective_id=0, has_side_effects=True, vmem_limit_bytes=60 * 1024 * 1024
        ),
    )(
        tokens, attn_gain.reshape(16, HD), query_weight, key_weight, value_weight, out_weight,
        head_gain.reshape(2, HD), past_keys.reshape(SEQ, POS, HD),
        past_values.reshape(SEQ, POS, HD), break_offset, cache_lengths,
        ffn_gain.reshape(16, HD), router_weight.T, expert_routes.T, expert_gate, expert_up,
        expert_down, shared_gate, shared_up, shared_down,
    )
    return pl.pallas_call(
        hand_over,
        out_shape=tuple(jax.ShapeDtypeStruct(o.shape, o.dtype) for o in outs),
        in_specs=[hbm] * 3,
        out_specs=(hbm,) * 3,
        scratch_shapes=[dma((3,))],
    )(*outs)


def solution(mesh):
    torus = Mesh(mesh.devices.reshape(NZ, NX, NC, NT), (*EP, "tp"))
    return jax.shard_map(
        body,
        mesh=torus,
        in_specs=(
            P(EP, None),
            P(),
            P(EP, "tp"),
            P(EP, "tp"),
            P(EP, "tp"),
            P(EP, "tp"),
            P("tp"),
            P(EP, None, "tp", None),
            P(EP, None, "tp", None),
            P(EP, "tp", None),
            P(EP),
            P(),
            P(),
            P(EP, None),
            P(EP, None, "tp"),
            P(EP, None, "tp"),
            P(EP, "tp", None),
            P(None, "tp"),
            P(None, "tp"),
            P("tp", None),
        ),
        out_specs=(P(EP, "tp"), P(EP, "tp"), P(EP, "tp")),
        check_vma=False,
    )
```

```python
import jax
import jax.numpy as jnp
from jax import lax
from jax.experimental import pallas as pl
from jax.experimental.pallas import tpu as pltpu
from jax.sharding import Mesh
from jax.sharding import PartitionSpec as P

MESH = pl.DeviceIdType.MESH
EP = ("ep_0", "ep_1", "ep_2")
NZ, NX, NC, NT = 8, 4, 2, 4
NE = NZ * NX * NC
SEQ = 16
POS = 1024
HD = 128
EPS = 1e-06
SCALE = 2.5
F32 = jnp.float32
BF16 = jnp.bfloat16


def dot(a, b):
    return jnp.dot(a, b, preferred_element_type=F32)


def dot_nt(a, b):
    return lax.dot_general(a, b, (((1,), (1,)), ((), ())), preferred_element_type=F32)


def iota(shape, dim):
    return lax.broadcasted_iota(jnp.int32, shape, dim)


def ones_where(cond):
    return jnp.where(cond, 1.0, 0.0).astype(BF16)


def kernel(
    tok_h, ag_h, wq_h, wk_h, wv_h, wo_h, hg_h, pk_h, pv_h, off_h, lens_h, fg_h, rt_h, er_h,
    eg_h, eu_h, ed_h, sg_h, su_h, sd_h,
    mixed_o, fk_o, fv_o,
    tok, ag, hg, fg, rt, er, off, kb, vb, qb, kvb, ob, wgu, wd, sgu, sd,
    tkb, tk, part, qp, kvpart, kvp,
    qs, lg, lenb, ho, pcs, pc, sq, fs, res, sbuf, rbuf, gs, gr, hs, obuf, cbuf, ssb, ssr,
    lens, tokb, mixed, fresh, lsem, kvsem,
    qzs, qzr, kzs, kzr, ozs, ozr, oxs, oxr, ods, odr, tks, tkr, qps, qpr, kps, kpr,
    ys, yr, cs, cr, as_, ar, gss, gsr, hss, hsr, rs_, rr, sss, ssrr, as2, ar2, fss, fsr,
):
    z = lax.axis_index("ep_0")
    x = lax.axis_index("ep_1")
    c = lax.axis_index("ep_2")
    t = lax.axis_index("tp")
    e = (z * NX + x) * NC + c
    m = x * NC + c
    zd = [lax.rem(z + d, NZ) for d in range(NZ)]
    xd = [lax.rem(x + d, NX) for d in range(NX)]
    td = [lax.rem(t + d, NT) for d in range(NT)]
    cd = [c, 1 - c]
    mates = [(2, 0), (2, 1), (1, 0), (3, 0), (1, 1), (3, 1), (0, 1)]
    far_first = [4, 3, 5, 2, 6, 1, 7]
    near_first = far_first[::-1]

    def remote(src, dst, ssem, rsem, dev):
        return pltpu.make_async_remote_copy(
            src_ref=src, dst_ref=dst, send_sem=ssem, recv_sem=rsem,
            device_id=dev, device_id_type=MESH,
        )

    pending = []

    def send(src, dst, ssem, rsem, dev):
        cp = remote(src, dst, ssem, rsem, dev)
        cp.start()
        pending.append(cp)

    def arrived(dst, ssem, rsem):
        remote(dst, dst, ssem, rsem, (z, x, 1 - c, t)).wait_recv()

    loads = []

    def load(src, dst):
        cp = pltpu.make_async_copy(src, dst, lsem.at[len(loads)])
        cp.start()
        loads.append(cp)
        return cp

    ld_q = load(wq_h, qb.at[z])
    ld_tok = [load(tok_h, tok), load(ag_h, ag)]
    ld_o = load(wo_h, ob.at[z, x, c])
    ld_kv = [
        load(wk_h, kvb.at[z, :, pl.ds(0, 128)]),
        load(wv_h, kvb.at[z, :, pl.ds(128, 128)]),
    ]
    ld_er = load(er_h, er)
    ld_att = [load(off_h, off), load(hg_h, hg), load(lens_h, lens)]
    kv_loads = []
    for i in range(4):
        ds = pl.ds(4 * i, 4)
        kv_loads.append(pltpu.make_async_copy(pk_h.at[ds], kb.at[ds], kvsem.at[i]))
        kv_loads.append(pltpu.make_async_copy(pv_h.at[ds], vb.at[ds], kvsem.at[4 + i]))
    for cp in kv_loads:
        cp.start()
    ld_ffn = [load(fg_h, fg), load(rt_h, rt)]
    ld_sh = [
        load(sg_h, sgu.at[:, pl.ds(0, 128)]),
        load(su_h, sgu.at[:, pl.ds(128, 128)]),
        load(sd_h, sd),
    ]
    mine = pl.ds(pl.multiple_of(t * 512, 512), 512)
    ld_own = load(tok_h.at[:, mine], tokb)
    ld_ex = [
        load(eg_h.at[0, mine, :], wgu.at[t, :, pl.ds(0, 128)]),
        load(eu_h.at[0, mine, :], wgu.at[t, :, pl.ds(128, 128)]),
        load(ed_h.at[0, :, mine], wd.at[t]),
    ]

    barrier = pltpu.get_barrier_semaphore()
    first = [(zd[d], x, c, t) for d in range(1, NZ)]
    first += [(z, xd[dx], cd[dc], t) for dx, dc in mates]
    first += [(z, x, c, td[d]) for d in range(1, NT)]
    for dev in first:
        pl.semaphore_signal(barrier, inc=1, device_id=dev, device_id_type=MESH)

    for cp in ld_tok:
        cp.wait()
    data = tok[...].astype(F32)
    factor = lax.rsqrt(jnp.mean(data * data, axis=-1, keepdims=True) + EPS)
    gain = ag[...].astype(F32)
    blocks = []
    for i in range(NZ):
        halves = []
        for k in (2 * i, 2 * i + 1):
            halves.append(data[:, HD * k : HD * k + HD] * factor * gain[k : k + 1, :])
        blocks.append(jnp.concatenate(halves, axis=1).astype(BF16).astype(F32))
    chunk = iota((SEQ, 256), 1) >> 5
    for g in range(8):
        own = blocks[g]
        for k in range(1, 8):
            j = (g + k) % 8
            own = jnp.where(chunk == j, pltpu.roll(blocks[j], 32 * k, 1), own)
        tkb[g] = own.astype(BF16)
    ld_er.wait()
    rows = NE * 12
    chosen = iota((NE, SEQ), 0) == er[0:1, :]
    for k in range(1, 6):
        chosen = chosen | (iota((NE, SEQ), 0) == er[k : k + 1, :])
    hot_t = ones_where(chosen)
    before = ones_where(iota((SEQ, SEQ), 0) < iota((SEQ, SEQ), 1))
    code_t = jnp.where(chosen, dot(hot_t, before) + 1.0, 0.0).astype(BF16)
    repeat = ones_where((iota((SEQ, 64), 1) & 15) == iota((SEQ, 64), 0))
    eye = ones_where(iota((SEQ, SEQ), 0) == iota((SEQ, SEQ), 1))
    code4_t = dot(code_t, repeat).astype(BF16)
    code = dot_nt(eye, code_t)
    q0 = iota((rows, 64), 0) >> 2
    j0 = iota((rows, 64), 0) & 3
    e0 = (q0 * 171) >> 9
    c0 = iota((rows, 64), 1)
    spread = ones_where(e0 == c0)
    slot_of = dot(spread, code4_t)
    want = (q0 - 3 * e0 + 1).astype(F32)
    dispatch = ones_where((slot_of == want) & (j0 == (c0 >> 4)))

    pl.semaphore_wait(barrier, len(first))

    ld_q.wait()
    for d in far_first:
        send(qb.at[z], qb.at[z], qzs.at[d], qzr.at[d], (zd[d], x, c, t))

    for dx, dc in mates:
        g = xd[dx] * NC + cd[dc]
        send(tkb.at[g], tk.at[m], tks.at[dx, dc], tkr.at[dx, dc], (z, xd[dx], cd[dc], t))
    tk[m] = tkb[m]

    ld_o.wait()
    mine_o = ob.at[z, x, c]
    for d in far_first:
        send(mine_o, mine_o, ozs.at[d], ozr.at[d], (zd[d], x, c, t))

    def o_along(r):
        src = ob.at[zd[r], x, c]
        for i in (2, 1, 3):
            send(src, src, oxs.at[r, i], oxr.at[r, i], (z, xd[i], c, t))

    def o_forward(r):
        src = ob.at[zd[r], x, c]
        arrived(src, ozs.at[NZ - r], ozr.at[NZ - r])
        o_along(r)

    def o_across(r):
        for i in (1, 3, 2):
            arrived(ob.at[zd[r], xd[i], c], oxs.at[r, NX - i], oxr.at[r, NX - i])
        src = ob.at[zd[r], :, c]
        send(src, src, ods.at[r], odr.at[r], (z, x, 1 - c, t))

    def o_last():
        for r in range(NZ):
            arrived(ob.at[zd[r], :, 1 - c], ods.at[r], odr.at[r])

    o_along(0)
    for cp in ld_kv:
        cp.wait()
    for d in far_first:
        send(kvb.at[z], kvb.at[z], kzs.at[d], kzr.at[d], (zd[d], x, c, t))

    for d in (1, 3, 2):
        p = td[d]
        dev = (z, x, c, p)
        theirs = pl.ds(pl.multiple_of(p * 512, 512), 512)
        for k, src in enumerate((eg_h, eu_h)):
            half = pl.ds(128 * k, 128)
            send(src.at[0, theirs, :], wgu.at[t, :, half], ys.at[k, d], yr.at[k, d], dev)

    for dx, dc in mates:
        src = tk.at[lax.rem(x + NX - dx, NX) * NC + cd[dc]]
        arrived(src, tks.at[dx, dc], tkr.at[dx, dc])
    for d in near_first:
        arrived(qb.at[lax.rem(z + NZ - d, NZ)], qzs.at[d], qzr.at[d])
    rows_in = tk[...].reshape(8 * SEQ, 256)
    part[...] = dot(rows_in, qb[...].reshape(256, 256)).astype(BF16).reshape(8, SEQ, 256)
    for dx, dc in mates:
        g = xd[dx] * NC + cd[dc]
        send(part.at[g], qp.at[m], qps.at[dx, dc], qpr.at[dx, dc], (z, xd[dx], cd[dc], t))
    qp[m] = part[m]
    for r in (7, 1, 6, 2, 5, 3, 4):
        o_forward(r)
    for dx, dc in mates:
        src = qp.at[lax.rem(x + NX - dx, NX) * NC + cd[dc]]
        arrived(src, qps.at[dx, dc], qpr.at[dx, dc])
    total = qp[0].astype(F32)
    for i in range(1, 8):
        total = total + qp[i].astype(F32)
    queries = total.astype(BF16).astype(F32)

    for h in range(2):
        qs[pl.ds(h, SEQ, stride=2), :] = queries[:, HD * h : HD * h + HD]
    for cp in ld_att:
        cp.wait()
    for b in range(SEQ):
        if b % 4 == 0:
            kv_loads[2 * (b // 4)].wait()
        q = qs[2 * b : 2 * b + 2, :].astype(BF16)
        lg[2 * b : 2 * b + 2, :] = dot_nt(q, kb[b]) * HD ** (-0.5) + off[b]
        lenb[2 * b : 2 * b + 2, :] = jnp.full((2, HD), lens[b], jnp.int32)
    for r in (0, 7, 1):
        o_across(r)
    logits = lg[...]
    length = lenb[:, 0:1]
    usable = iota((2 * SEQ, POS), 1) < length
    tail = jnp.log(1.0 + jnp.exp(-jnp.abs(logits)))
    keep = jnp.where(usable, jnp.minimum(-logits, 0.0) - tail, 0.0)
    nb = POS // HD
    stacked = jnp.concatenate([keep[:, HD * i : HD * i + HD] for i in range(nb)], axis=0)
    k1 = stacked.astype(BF16)
    left = stacked - k1.astype(F32)
    k2 = left.astype(BF16)
    k3 = (left - k2.astype(F32)).astype(BF16)
    later = ones_where(iota((HD, HD), 0) > iota((HD, HD), 1))
    inner = dot(k1, later) + dot(k2, later) + dot(k3, later)
    carry = jnp.zeros((2 * SEQ, 1), F32)
    after = [None] * nb
    n2 = 2 * SEQ
    for i in range(nb - 1, -1, -1):
        after[i] = inner[n2 * i : n2 * i + n2] + carry
        carry = carry + jnp.sum(stacked[n2 * i : n2 * i + n2], axis=-1, keepdims=True)
    after = jnp.concatenate(after, axis=1)
    sticks = jnp.where(usable, jnp.exp(jnp.minimum(logits, 0.0) - tail + after), 0.0)
    lg[...] = sticks
    for r in (6, 2):
        o_across(r)
    for b in range(SEQ):
        if b % 4 == 0:
            kv_loads[2 * (b // 4) + 1].wait()
        got = dot(lg[2 * b : 2 * b + 2, :].astype(BF16), vb[b])
        ho[b : b + 1, 0:HD] = got[0:1, :]
        ho[b : b + 1, HD : 2 * HD] = got[1:2, :]
    for r in (5, 3, 4):
        o_across(r)
    heads_out = ho[...]
    scaled = jnp.concatenate(
        [heads_out[:, HD * i : HD * i + HD] * hg[i : i + 1, :].astype(F32) for i in range(2)],
        axis=1,
    ).astype(BF16)
    sq[t] = jnp.broadcast_to(jnp.sum(heads_out * heads_out, axis=-1, keepdims=True), (SEQ, HD))
    o_last()
    for i in range(NT):
        halves = [dot_nt(scaled, ob[zi].reshape(256, 256)) for zi in (2 * i, 2 * i + 1)]
        pcs[i] = jnp.concatenate(halves, axis=1).astype(BF16)

    for d in (2, 1, 3):
        dev = (z, x, c, td[d])
        send(sq.at[t], sq.at[t], cs.at[0, d], cr.at[0, d], dev)
        send(pcs.at[td[d]], pc.at[t], cs.at[1, d], cr.at[1, d], dev)
    pc[t] = pcs[t]
    for d in near_first:
        arrived(kvb.at[lax.rem(z + NZ - d, NZ)], kzs.at[d], kzr.at[d])
    kvpart[...] = dot(rows_in, kvb[...].reshape(256, 256)).astype(BF16).reshape(8, SEQ, 256)
    for dx, dc in mates:
        g = xd[dx] * NC + cd[dc]
        send(kvpart.at[g], kvp.at[m], kps.at[dx, dc], kpr.at[dx, dc], (z, xd[dx], cd[dc], t))
    kvp[m] = kvpart[m]
    for d in (1, 3, 2):
        src = td[NT - d]
        for k, buf in enumerate((sq, pc)):
            arrived(buf.at[src], cs.at[k, d], cr.at[k, d])
    head_total = pc[0].astype(F32)
    square = sq[0]
    for i in range(1, NT):
        head_total = head_total + pc[i].astype(F32)
        square = square + sq[i]
    attention = head_total * lax.rsqrt(square[:, 0:1] / 1024.0 + EPS)
    ld_own.wait()
    residual = (tokb[...].astype(F32) + attention).astype(BF16)
    res[t] = residual
    for d in (2, 1, 3):
        send(res.at[t], res.at[t], as2.at[d], ar2.at[d], (z, x, c, td[d]))

    block = jnp.concatenate([residual[:, HD * j : HD * j + HD] for j in range(4)], axis=0)
    sbuf[...] = dot(dispatch, block).astype(BF16).reshape(3 * NE, 4, HD)
    order = (3, 4, 5, 6, 7, 0, 1, 2)

    def three(i):
        return pl.ds(3 * i, 3)

    def half_of(r):
        return order.index(r) // 4

    def around(r):
        return [(0, 0), *mates] if r else mates

    for r in (4, 5, 3, 6, 2, 7, 1, 0):
        d = (NZ - r) % NZ
        to = three(8 * order.index(r) + m)
        for dx, dc in around(r):
            p = (zd[d] * NX + xd[dx]) * NC + cd[dc]
            dev = (zd[d], xd[dx], cd[dc], t)
            remote(sbuf.at[three(p)], rbuf.at[to], as_.at[half_of(r)], ar.at[half_of(r)], dev).start()
    rbuf[three(8 * order.index(0) + m)] = sbuf[three(e)]

    for d in (1, 3, 2):
        theirs = pl.ds(pl.multiple_of(td[d] * 512, 512), 512)
        send(ed_h.at[0, :, theirs], wd.at[t], ys.at[2, d], yr.at[2, d], (z, x, c, td[d]))

    for d in (1, 3, 2):
        arrived(res.at[td[NT - d]], as2.at[d], ar2.at[d])
    for cp in ld_ffn:
        cp.wait()
    data = jnp.concatenate([res[i] for i in range(NT)], axis=1).astype(F32)
    factor = lax.rsqrt(jnp.mean(data * data, axis=-1, keepdims=True) + EPS)
    gain = fg[...].astype(F32)
    pieces = [data[:, HD * i : HD * i + HD] * factor * gain[i : i + 1, :] for i in range(16)]
    normed_ffn = jnp.concatenate(pieces, axis=1).astype(BF16)
    own_gain = []
    for j in range(4):
        row = gain[j : j + 1, :]
        for i in range(1, NT):
            row = jnp.where(t == i, gain[4 * i + j : 4 * i + j + 1, :], row)
        own_gain.append(row)
    own_gain = jnp.concatenate(own_gain, axis=1)
    for cp in ld_sh:
        cp.wait()
    both = dot(normed_ffn, sgu[...])
    gate = both[:, 0:HD]
    shared_hidden = (gate / (1.0 + jnp.exp(-gate)) * both[:, HD : 2 * HD]).astype(BF16)
    shared_part = dot(shared_hidden, sd[...]).astype(BF16)
    for i in range(NT):
        ssb[i] = shared_part[:, 512 * i : 512 * i + 512]
    for d in (2, 1, 3):
        p = td[d]
        send(ssb.at[p], ssr.at[t], sss.at[d], ssrr.at[d], (z, x, c, p))
    ssr[t] = ssb[t]
    logit = dot_nt(normed_ffn, rt[...])
    prob = 1.0 / (1.0 + jnp.exp(-logit))
    picked = jnp.where(code > 0.5, prob, 0.0)
    weight = SCALE * picked / jnp.sum(picked, axis=-1, keepdims=True)
    weight4 = jnp.concatenate([weight] * 4, axis=0)
    w_hi = weight4.astype(BF16)
    w_lo = (weight4 - w_hi.astype(F32)).astype(BF16)
    code4 = jnp.concatenate([code] * 4, axis=0).astype(BF16)
    q1 = iota((64, rows), 1) >> 2
    j1 = iota((64, rows), 1) & 3
    e1 = (q1 * 171) >> 9
    c1 = iota((64, rows), 0)
    spread_t = ones_where(e1 == c1)
    slot_to = dot(code4, spread_t)
    fits = (slot_to == (q1 - 3 * e1 + 1).astype(F32)) & (j1 == (c1 >> 4))
    comb_hi = jnp.where(fits, dot(w_hi, spread_t), 0.0).astype(BF16)
    comb_lo = jnp.where(fits, dot(w_lo, spread_t), 0.0).astype(BF16)

    def to_rows(half, g):
        group = rbuf[96 * half + 48 * g : 96 * half + 48 * g + 48].reshape(192, HD)
        p, q = iota((48, 192), 0), iota((48, 192), 1)
        cols = [dot(ones_where(q == 4 * p + j), group).astype(BF16) for j in range(4)]
        return jnp.concatenate(cols, axis=1)

    def start_half(half):
        n = 96 if half == 0 else 93
        both = remote(
            sbuf.at[pl.ds(0, n)], rbuf.at[pl.ds(0, n)], as_.at[half], ar.at[half],
            (z, x, 1 - c, t),
        )
        both.wait_recv()
        raw = jnp.concatenate([to_rows(half, 0), to_rows(half, 1)], axis=0).astype(F32)
        rows_of = (raw * own_gain).astype(BF16)
        square = jnp.sum(raw * raw, axis=-1, keepdims=True)
        square = jnp.concatenate([square, jnp.zeros((32, 1), F32)], axis=0)
        square = jnp.broadcast_to(square, (HD, HD)).T[0:8, :]
        fs[half, 0] = square
        for d in (2, 1, 3):
            gs[half, d] = dot(rows_of, wgu[td[d]]).astype(BF16)
            dev = (z, x, c, td[d])
            send(fs.at[half, 0], fs.at[half, d], fss.at[half, d], fsr.at[half, d], dev)
            send(gs.at[half, d], gr.at[half, d], gss.at[half, d], gsr.at[half, d], dev)
        return dot(rows_of, wgu[t]), both

    def middle_half(half, gate_up):
        for d in (2, 1, 3):
            arrived(gr.at[half, d], gss.at[half, d], gsr.at[half, d])
            gate_up = gate_up + gr[half, d].astype(F32)
            arrived(fs.at[half, d], fss.at[half, d], fsr.at[half, d])
        square = fs[half, 0] + fs[half, 1] + fs[half, 2] + fs[half, 3]
        square = jnp.broadcast_to(square[0:1, :], (HD, HD)).T[0:96, 0:1]
        gate_up = gate_up * lax.rsqrt(square / 2048.0 + EPS)
        gate = gate_up[:, 0:HD]
        hidden = gate / (1.0 + jnp.exp(-gate)) * gate_up[:, HD : 2 * HD]
        hs[half, t] = hidden.astype(BF16)
        for d in (2, 1, 3):
            own = hs.at[half, t]
            send(own, own, hss.at[half, d], hsr.at[half, d], (z, x, c, td[d]))

    def end_half(half):
        for d in (2, 1, 3):
            arrived(hs.at[half, td[NT - d]], hss.at[half, d], hsr.at[half, d])
        out = dot(hs[half, 0], wd[0])
        for i in range(1, NT):
            out = out + dot(hs[half, i], wd[i])
        out = out.astype(BF16)
        p, q = iota((192, 48), 1), iota((192, 48), 0)
        for g in range(2):
            back = jnp.zeros((192, HD), F32)
            for j in range(4):
                block = out[48 * g : 48 * g + 48, HD * j : HD * j + HD]
                back = back + dot(ones_where(q == 4 * p + j), block)
            at = 96 * half + 48 * g
            obuf[at : at + 48] = back.astype(BF16).reshape(48, 4, HD)
        for r in ((4, 5, 3, 6) if half == 0 else (2, 7, 1, 0)):
            for dx, dc in around(r):
                p = 8 * order.index(r) + xd[dx] * NC + cd[dc]
                dev = (zd[r], xd[dx], cd[dc], t)
                remote(obuf.at[three(p)], cbuf.at[three(e)], rs_, rr, dev).start()

    for cp in ld_ex:
        cp.wait()
    for d in (1, 3, 2):
        src = td[NT - d]
        for k in range(2):
            arrived(wgu.at[src, :, pl.ds(128 * k, 128)], ys.at[k, d], yr.at[k, d])
    gate_up0, sent0 = start_half(0)
    gate_up1, sent1 = start_half(1)
    middle_half(0, gate_up0)
    middle_half(1, gate_up1)
    for d in (1, 3, 2):
        arrived(wd.at[td[NT - d]], ys.at[2, d], yr.at[2, d])
    end_half(0)
    end_half(1)
    cbuf[three(e)] = obuf[three(8 * order.index(0) + m)]
    shared_total = jnp.zeros((SEQ, 512), F32)
    for d in (2, 1, 3):
        arrived(ssr.at[td[NT - d]], sss.at[d], ssrr.at[d])
    for i in range(NT):
        shared_total = shared_total + ssr[i].astype(F32)
    base = res[t].astype(F32) + shared_total
    for dx, dc in mates:
        src = kvp.at[lax.rem(x + NX - dx, NX) * NC + cd[dc]]
        arrived(src, kps.at[dx, dc], kpr.at[dx, dc])
    new = kvp[0].astype(F32)
    for i in range(1, 8):
        new = new + kvp[i].astype(F32)
    fresh[0] = new[:, 0:HD].astype(BF16)
    fresh[1] = new[:, HD : 2 * HD].astype(BF16)
    stores = [load(fresh.at[0], fk_o), load(fresh.at[1], fv_o)]
    back = remote(
        obuf.at[pl.ds(0, 3 * NE - 3)], cbuf.at[pl.ds(0, 3 * NE - 3)], rs_, rr, (z, x, 1 - c, t)
    )
    back.wait_recv()
    came = cbuf[...].reshape(rows, HD)
    routed = dot(comb_hi, came) + dot(comb_lo, came)
    for j in range(4):
        mixed[:, HD * j : HD * j + HD] = (
            base[:, HD * j : HD * j + HD] + routed[SEQ * j : SEQ * j + SEQ]
        ).astype(BF16)
    stores.append(load(mixed, mixed_o))
    for cp in [*pending, sent0, sent1, back]:
        cp.wait_send()
    for cp in stores:
        cp.wait()


def hand_over(a, b, c, a_o, b_o, c_o, sem):
    moves = []
    for i, (src, dst) in enumerate(((a, a_o), (b, b_o), (c, c_o))):
        moves.append(pltpu.make_async_copy(src, dst, sem.at[i]))
        moves[i].start()
    for cp in moves:
        cp.wait()


def body(
    tokens, attn_gain, query_weight, key_weight, value_weight, out_weight, head_gain,
    past_keys, past_values, break_offset, cache_lengths, ffn_gain, router_weight,
    expert_routes, expert_gate, expert_up, expert_down, shared_gate, shared_up, shared_down,
):
    hbm = pl.BlockSpec(memory_space=pl.ANY)
    v, dma = pltpu.VMEM, pltpu.SemaphoreType.DMA
    outs = pl.pallas_call(
        kernel,
        out_shape=(
            jax.ShapeDtypeStruct((SEQ, 512), BF16),
            jax.ShapeDtypeStruct((SEQ, HD), BF16),
            jax.ShapeDtypeStruct((SEQ, HD), BF16),
        ),
        in_specs=[hbm] * 20,
        out_specs=(hbm,) * 3,
        scratch_shapes=[
            v((SEQ, 2048), BF16), v((16, HD), BF16), v((2, HD), BF16), v((16, HD), BF16),
            v((64, 2048), BF16), v((6, SEQ), jnp.int32), v((SEQ, 2, POS), F32),
            v((SEQ, POS, HD), BF16), v((SEQ, POS, HD), BF16),
            v((NZ, 32, 256), BF16), v((NZ, 32, 256), BF16), v((NZ, NX, NC, 32, 256), BF16),
            v((NT, 512, 256), BF16), v((NT, 128, 512), BF16),
            v((2048, 256), BF16), v((128, 2048), BF16),
            v((8, SEQ, 256), BF16), v((8, SEQ, 256), BF16),
            v((8, SEQ, 256), BF16), v((8, SEQ, 256), BF16),
            v((8, SEQ, 256), BF16), v((8, SEQ, 256), BF16),
            v((2 * SEQ, HD), F32), v((2 * SEQ, POS), F32), v((2 * SEQ, HD), jnp.int32),
            v((SEQ, 256), F32), v((NT, SEQ, 512), BF16), v((NT, SEQ, 512), BF16),
            v((NT, SEQ, HD), F32), v((2, NT, 8, HD), F32), v((NT, SEQ, 512), BF16),
            v((3 * NE, 4, HD), BF16), v((3 * NE, 4, HD), BF16),
            v((2, NT, 96, 256), BF16), v((2, NT, 96, 256), BF16), v((2, NT, 96, HD), BF16),
            v((3 * NE, 4, HD), BF16), v((3 * NE, 4, HD), BF16),
            v((NT, SEQ, 512), BF16), v((NT, SEQ, 512), BF16),
            pltpu.SMEM((SEQ,), jnp.int32), v((SEQ, 512), BF16), v((SEQ, 512), BF16),
            v((2, SEQ, HD), BF16), dma((32,)), dma((8,)),
            *[dma((NZ,)) for _ in range(6)],
            dma((NZ, NX)), dma((NZ, NX)), dma((NZ,)), dma((NZ,)),
            *[dma((NX, NC)) for _ in range(6)],
            dma((3, 4)), dma((3, 4)), dma((2, 4)), dma((2, 4)), dma((2,)), dma((2,)),
            dma((2, 4)), dma((2, 4)), dma((2, 4)), dma((2, 4)), dma, dma, dma((4,)), dma((4,)),
            dma((4,)), dma((4,)), dma((2, 4)), dma((2, 4)),
        ],
        compiler_params=pltpu.CompilerParams(
            collective_id=0, has_side_effects=True, vmem_limit_bytes=60 * 1024 * 1024
        ),
    )(
        tokens, attn_gain.reshape(16, HD), query_weight, key_weight, value_weight, out_weight,
        head_gain.reshape(2, HD), past_keys.reshape(SEQ, POS, HD),
        past_values.reshape(SEQ, POS, HD), break_offset, cache_lengths,
        ffn_gain.reshape(16, HD), router_weight.T, expert_routes.T, expert_gate, expert_up,
        expert_down, shared_gate, shared_up, shared_down,
    )
    return pl.pallas_call(
        hand_over,
        out_shape=tuple(jax.ShapeDtypeStruct(o.shape, o.dtype) for o in outs),
        in_specs=[hbm] * 3,
        out_specs=(hbm,) * 3,
        scratch_shapes=[dma((3,))],
    )(*outs)


def solution(mesh):
    torus = Mesh(mesh.devices.reshape(NZ, NX, NC, NT), (*EP, "tp"))
    return jax.shard_map(
        body,
        mesh=torus,
        in_specs=(
            P(EP, None),
            P(),
            P(EP, "tp"),
            P(EP, "tp"),
            P(EP, "tp"),
            P(EP, "tp"),
            P("tp"),
            P(EP, None, "tp", None),
            P(EP, None, "tp", None),
            P(EP, "tp", None),
            P(EP),
            P(),
            P(),
            P(EP, None),
            P(EP, None, "tp"),
            P(EP, None, "tp"),
            P(EP, "tp", None),
            P(None, "tp"),
            P(None, "tp"),
            P("tp", None),
        ),
        out_specs=(P(EP, "tp"), P(EP, "tp"), P(EP, "tp")),
        check_vma=False,
    )
```

```python
import jax
import jax.numpy as jnp
from jax import lax
from jax.experimental import pallas as pl
from jax.experimental.pallas import tpu as pltpu
from jax.sharding import Mesh
from jax.sharding import PartitionSpec as P

MESH = pl.DeviceIdType.MESH
EP = ("ep_0", "ep_1", "ep_2")
NZ, NX, NC, NT = 8, 4, 2, 4
NE = NZ * NX * NC
SEQ = 16
POS = 1024
HD = 128
EPS = 1e-06
SCALE = 2.5
F32 = jnp.float32
BF16 = jnp.bfloat16


def dot(a, b):
    return jnp.dot(a, b, preferred_element_type=F32)


def dot_nt(a, b):
    return lax.dot_general(a, b, (((1,), (1,)), ((), ())), preferred_element_type=F32)


def iota(shape, dim):
    return lax.broadcasted_iota(jnp.int32, shape, dim)


def ones_where(cond):
    return jnp.where(cond, 1.0, 0.0).astype(BF16)


def kernel(
    tok_h, ag_h, wq_h, wk_h, wv_h, wo_h, hg_h, pk_h, pv_h, off_h, lens_h, fg_h, rt_h, er_h,
    eg_h, eu_h, ed_h, sg_h, su_h, sd_h,
    mixed_o, fk_o, fv_o,
    tok, ag, hg, fg, rt, er, off, kb, kt, vb, qb, kvb, ob, wgu, wd, sgu, sd,
    tkb, tk, part, qp, kvpart, kvp,
    qs, lg, lenb, ho, pcs, pc, sq, fs, res, sbuf, rbuf, gs, gr, hs, obuf, cbuf, ssb, ssr,
    lens, tokb, mixed, fresh, lsem, kvsem,
    qzs, qzr, kzs, kzr, ozs, ozr, oxs, oxr, ods, odr, tks, tkr, qps, qpr, kps, kpr,
    ys, yr, cs, cr, as_, ar, gss, gsr, hss, hsr, rs_, rr, sss, ssrr, as2, ar2, fss, fsr,
):
    z = lax.axis_index("ep_0")
    x = lax.axis_index("ep_1")
    c = lax.axis_index("ep_2")
    t = lax.axis_index("tp")
    e = (z * NX + x) * NC + c
    m = x * NC + c
    zd = [lax.rem(z + d, NZ) for d in range(NZ)]
    xd = [lax.rem(x + d, NX) for d in range(NX)]
    td = [lax.rem(t + d, NT) for d in range(NT)]
    cd = [c, 1 - c]
    mates = [(2, 0), (2, 1), (1, 0), (3, 0), (1, 1), (3, 1), (0, 1)]
    far_first = [4, 3, 5, 2, 6, 1, 7]
    near_first = far_first[::-1]

    def remote(src, dst, ssem, rsem, dev):
        return pltpu.make_async_remote_copy(
            src_ref=src, dst_ref=dst, send_sem=ssem, recv_sem=rsem,
            device_id=dev, device_id_type=MESH,
        )

    pending = []

    def send(src, dst, ssem, rsem, dev):
        cp = remote(src, dst, ssem, rsem, dev)
        cp.start()
        pending.append(cp)

    def arrived(dst, ssem, rsem):
        remote(dst, dst, ssem, rsem, (z, x, 1 - c, t)).wait_recv()

    loads = []

    def load(src, dst):
        cp = pltpu.make_async_copy(src, dst, lsem.at[len(loads)])
        cp.start()
        loads.append(cp)
        return cp

    ld_q = load(wq_h, qb.at[z])
    ld_tok = [load(tok_h, tok), load(ag_h, ag)]
    ld_o = load(wo_h, ob.at[z, x, c])
    ld_kv = [
        load(wk_h, kvb.at[z, :, pl.ds(0, 128)]),
        load(wv_h, kvb.at[z, :, pl.ds(128, 128)]),
    ]
    barrier = pltpu.get_barrier_semaphore()
    first = [(zd[d], x, c, t) for d in range(1, NZ)]
    first += [(z, xd[dx], cd[dc], t) for dx, dc in mates]
    first += [(z, x, c, td[d]) for d in range(1, NT)]
    for dev in first:
        pl.semaphore_signal(barrier, inc=1, device_id=dev, device_id_type=MESH)

    pl.semaphore_wait(barrier, len(first))

    mine_o = ob.at[z, x, c]

    def q_around(*steps):
        for d in steps:
            send(qb.at[z], qb.at[z], qzs.at[d], qzr.at[d], (zd[d], x, c, t))

    def o_around(*steps):
        for d in steps:
            send(mine_o, mine_o, ozs.at[d], ozr.at[d], (zd[d], x, c, t))

    ld_q.wait()
    q_around(*far_first)

    ld_o.wait()
    for cp in ld_tok:
        cp.wait()
    data = tok[...].astype(F32)
    factor = lax.rsqrt(jnp.mean(data * data, axis=-1, keepdims=True) + EPS)
    gain = ag[...].astype(F32)
    blocks = []
    for i in range(NZ):
        halves = []
        for k in (2 * i, 2 * i + 1):
            halves.append(data[:, HD * k : HD * k + HD] * factor * gain[k : k + 1, :])
        blocks.append(jnp.concatenate(halves, axis=1).astype(BF16).astype(F32))
    chunk = iota((SEQ, 256), 1) >> 5
    for g in range(8):
        own = blocks[g]
        for k in range(1, 8):
            j = (g + k) % 8
            own = jnp.where(chunk == j, pltpu.roll(blocks[j], 32 * k, 1), own)
        tkb[g] = own.astype(BF16)
    for dx, dc in mates:
        g = xd[dx] * NC + cd[dc]
        send(tkb.at[g], tk.at[m], tks.at[dx, dc], tkr.at[dx, dc], (z, xd[dx], cd[dc], t))
    tk[m] = tkb[m]

    def o_along(r):
        src = ob.at[zd[r], x, c]
        for i in (2, 1, 3):
            send(src, src, oxs.at[r, i], oxr.at[r, i], (z, xd[i], c, t))

    def o_forward(r):
        src = ob.at[zd[r], x, c]
        arrived(src, ozs.at[NZ - r], ozr.at[NZ - r])
        o_along(r)

    def o_across(r):
        for i in (1, 3, 2):
            arrived(ob.at[zd[r], xd[i], c], oxs.at[r, NX - i], oxr.at[r, NX - i])
        src = ob.at[zd[r], :, c]
        send(src, src, ods.at[r], odr.at[r], (z, x, 1 - c, t))

    def o_last():
        for r in range(NZ):
            arrived(ob.at[zd[r], :, 1 - c], ods.at[r], odr.at[r])

    o_along(0)
    ld_er = load(er_h, er)
    ld_att = [load(off_h, off), load(hg_h, hg), load(lens_h, lens)]
    kv_loads = []
    for i in range(4):
        ds = pl.ds(4 * i, 4)
        kv_loads.append(pltpu.make_async_copy(pk_h.at[ds], kb.at[ds], kvsem.at[i]))
        kv_loads.append(pltpu.make_async_copy(pv_h.at[ds], vb.at[ds], kvsem.at[4 + i]))
    for cp in kv_loads:
        cp.start()
    ld_ffn = [load(fg_h, fg), load(rt_h, rt)]
    ld_sh = [
        load(sg_h, sgu.at[:, pl.ds(0, 128)]),
        load(su_h, sgu.at[:, pl.ds(128, 128)]),
        load(sd_h, sd),
    ]
    mine = pl.ds(pl.multiple_of(t * 512, 512), 512)
    ld_own = load(tok_h.at[:, mine], tokb)
    ld_ex = [
        load(eg_h.at[0, mine, :], wgu.at[t, :, pl.ds(0, 128)]),
        load(eu_h.at[0, mine, :], wgu.at[t, :, pl.ds(128, 128)]),
        load(ed_h.at[0, :, mine], wd.at[t]),
    ]

    def recut_down(peers):
        for d in peers:
            theirs = pl.ds(pl.multiple_of(td[d] * 512, 512), 512)
            send(ed_h.at[0, :, theirs], wd.at[t], ys.at[2, d], yr.at[2, d], (z, x, c, td[d]))

    for d in (1, 3, 2):
        p = td[d]
        dev = (z, x, c, p)
        theirs = pl.ds(pl.multiple_of(p * 512, 512), 512)
        for k, src in enumerate((eg_h, eu_h)):
            half = pl.ds(128 * k, 128)
            send(src.at[0, theirs, :], wgu.at[t, :, half], ys.at[k, d], yr.at[k, d], dev)
    recut_down((1, 3))

    ld_er.wait()
    rows = NE * 12
    chosen = iota((NE, SEQ), 0) == er[0:1, :]
    for k in range(1, 6):
        chosen = chosen | (iota((NE, SEQ), 0) == er[k : k + 1, :])
    hot_t = ones_where(chosen)
    before = ones_where(iota((SEQ, SEQ), 0) < iota((SEQ, SEQ), 1))
    code_t = jnp.where(chosen, dot(hot_t, before) + 1.0, 0.0).astype(BF16)
    repeat = ones_where((iota((SEQ, 64), 1) & 15) == iota((SEQ, 64), 0))
    eye = ones_where(iota((SEQ, SEQ), 0) == iota((SEQ, SEQ), 1))
    code4_t = dot(code_t, repeat).astype(BF16)
    code = dot_nt(eye, code_t)
    q0 = iota((rows, 64), 0) >> 2
    j0 = iota((rows, 64), 0) & 3
    e0 = (q0 * 171) >> 9
    c0 = iota((rows, 64), 1)
    spread = ones_where(e0 == c0)
    slot_of = dot(spread, code4_t)
    want = (q0 - 3 * e0 + 1).astype(F32)
    dispatch = ones_where((slot_of == want) & (j0 == (c0 >> 4)))

    o_around(1, 7, 4, 3, 5, 2, 6)
    for b in range(SEQ):
        if b % 4 == 0:
            kv_loads[2 * (b // 4)].wait()
        kt[b] = kb[b].T

    for dx, dc in mates:
        src = tk.at[lax.rem(x + NX - dx, NX) * NC + cd[dc]]
        arrived(src, tks.at[dx, dc], tkr.at[dx, dc])
    for d in near_first:
        arrived(qb.at[lax.rem(z + NZ - d, NZ)], qzs.at[d], qzr.at[d])
    rows_in = tk[...].reshape(8 * SEQ, 256)
    part[...] = dot(rows_in, qb[...].reshape(256, 256)).reshape(8, SEQ, 256)
    for dx, dc in mates:
        g = xd[dx] * NC + cd[dc]
        send(part.at[g], qp.at[m], qps.at[dx, dc], qpr.at[dx, dc], (z, xd[dx], cd[dc], t))
    qp[m] = part[m]
    for r in (7, 1, 6, 2, 5, 3, 4):
        o_forward(r)
    for r in (0, 7, 1):
        o_across(r)
    for dx, dc in mates:
        src = qp.at[lax.rem(x + NX - dx, NX) * NC + cd[dc]]
        arrived(src, qps.at[dx, dc], qpr.at[dx, dc])
    total = qp[0]
    for i in range(1, 8):
        total = total + qp[i]
    queries = total.astype(BF16).astype(F32)

    for h in range(2):
        qs[pl.ds(h, SEQ, stride=2), :] = queries[:, HD * h : HD * h + HD]
    for cp in ld_att:
        cp.wait()
    for b in range(SEQ):
        q = qs[2 * b : 2 * b + 2, :].astype(BF16)
        lg[2 * b : 2 * b + 2, :] = dot(q, kt[b]) * HD ** (-0.5) + off[b]
        lenb[2 * b : 2 * b + 2, :] = jnp.full((2, HD), lens[b], jnp.int32)
    for cp in ld_kv:
        cp.wait()
    for d in far_first:
        send(kvb.at[z], kvb.at[z], kzs.at[d], kzr.at[d], (zd[d], x, c, t))
    for r in (6, 2):
        o_across(r)
    logits = lg[...]
    length = lenb[:, 0:1]
    usable = iota((2 * SEQ, POS), 1) < length
    tail = jnp.log(1.0 + jnp.exp(-jnp.abs(logits)))
    keep = jnp.where(usable, jnp.minimum(-logits, 0.0) - tail, 0.0)
    nb = POS // HD
    stacked = jnp.concatenate([keep[:, HD * i : HD * i + HD] for i in range(nb)], axis=0)
    k1 = stacked.astype(BF16)
    left = stacked - k1.astype(F32)
    k2 = left.astype(BF16)
    k3 = (left - k2.astype(F32)).astype(BF16)
    later = ones_where(iota((HD, HD), 0) > iota((HD, HD), 1))
    inner = dot(k1, later) + dot(k2, later) + dot(k3, later)
    carry = jnp.zeros((2 * SEQ, 1), F32)
    after = [None] * nb
    n2 = 2 * SEQ
    for i in range(nb - 1, -1, -1):
        after[i] = inner[n2 * i : n2 * i + n2] + carry
        carry = carry + jnp.sum(stacked[n2 * i : n2 * i + n2], axis=-1, keepdims=True)
    after = jnp.concatenate(after, axis=1)
    sticks = jnp.where(usable, jnp.exp(jnp.minimum(logits, 0.0) - tail + after), 0.0)
    lg[...] = sticks
    for b in range(SEQ):
        if b % 4 == 0:
            kv_loads[2 * (b // 4) + 1].wait()
        got = dot(lg[2 * b : 2 * b + 2, :].astype(BF16), vb[b])
        ho[b : b + 1, 0:HD] = got[0:1, :]
        ho[b : b + 1, HD : 2 * HD] = got[1:2, :]
    for r in (5, 3, 4):
        o_across(r)
    heads_out = ho[...]
    scaled = jnp.concatenate(
        [heads_out[:, HD * i : HD * i + HD] * hg[i : i + 1, :].astype(F32) for i in range(2)],
        axis=1,
    ).astype(BF16)
    sq[t] = jnp.broadcast_to(jnp.sum(heads_out * heads_out, axis=-1, keepdims=True), (SEQ, HD))
    o_last()
    for i in range(NT):
        halves = [dot_nt(scaled, ob[zi].reshape(256, 256)) for zi in (2 * i, 2 * i + 1)]
        pcs[i] = jnp.concatenate(halves, axis=1).astype(BF16)

    for d in (2, 1, 3):
        dev = (z, x, c, td[d])
        send(sq.at[t], sq.at[t], cs.at[0, d], cr.at[0, d], dev)
        send(pcs.at[td[d]], pc.at[t], cs.at[1, d], cr.at[1, d], dev)
    pc[t] = pcs[t]
    for d in (1, 3, 2):
        src = td[NT - d]
        for k, buf in enumerate((sq, pc)):
            arrived(buf.at[src], cs.at[k, d], cr.at[k, d])
    head_total = pc[0].astype(F32)
    square = sq[0]
    for i in range(1, NT):
        head_total = head_total + pc[i].astype(F32)
        square = square + sq[i]
    attention = head_total * lax.rsqrt(square[:, 0:1] / 1024.0 + EPS)
    ld_own.wait()
    residual = (tokb[...].astype(F32) + attention).astype(BF16)
    res[t] = residual
    for d in (2, 1, 3):
        send(res.at[t], res.at[t], as2.at[d], ar2.at[d], (z, x, c, td[d]))

    block = jnp.concatenate([residual[:, HD * j : HD * j + HD] for j in range(4)], axis=0)
    sbuf[...] = dot(dispatch, block).astype(BF16).reshape(3 * NE, 4, HD)
    order = (3, 4, 5, 6, 7, 0, 1, 2)

    def three(i):
        return pl.ds(3 * i, 3)

    def half_of(r):
        return order.index(r) // 4

    def around(r):
        return [(0, 0), *mates] if r else mates

    for r in (4, 5, 3, 6, 2, 7, 1, 0):
        d = (NZ - r) % NZ
        to = three(8 * order.index(r) + m)
        for dx, dc in around(r):
            p = (zd[d] * NX + xd[dx]) * NC + cd[dc]
            dev = (zd[d], xd[dx], cd[dc], t)
            remote(sbuf.at[three(p)], rbuf.at[to], as_.at[half_of(r)], ar.at[half_of(r)], dev).start()
    rbuf[three(8 * order.index(0) + m)] = sbuf[three(e)]

    recut_down((2,))

    for d in (1, 3, 2):
        arrived(res.at[td[NT - d]], as2.at[d], ar2.at[d])
    for cp in ld_ffn:
        cp.wait()
    data = jnp.concatenate([res[i] for i in range(NT)], axis=1).astype(F32)
    factor = lax.rsqrt(jnp.mean(data * data, axis=-1, keepdims=True) + EPS)
    gain = fg[...].astype(F32)
    pieces = [data[:, HD * i : HD * i + HD] * factor * gain[i : i + 1, :] for i in range(16)]
    normed_ffn = jnp.concatenate(pieces, axis=1).astype(BF16)
    own_gain = []
    for j in range(4):
        row = gain[j : j + 1, :]
        for i in range(1, NT):
            row = jnp.where(t == i, gain[4 * i + j : 4 * i + j + 1, :], row)
        own_gain.append(row)
    own_gain = jnp.concatenate(own_gain, axis=1)
    for cp in ld_sh:
        cp.wait()
    both = dot(normed_ffn, sgu[...])
    gate = both[:, 0:HD]
    shared_hidden = (gate / (1.0 + jnp.exp(-gate)) * both[:, HD : 2 * HD]).astype(BF16)
    shared_part = dot(shared_hidden, sd[...]).astype(BF16)
    for i in range(NT):
        ssb[i] = shared_part[:, 512 * i : 512 * i + 512]
    for d in (2, 1, 3):
        p = td[d]
        send(ssb.at[p], ssr.at[t], sss.at[d], ssrr.at[d], (z, x, c, p))
    ssr[t] = ssb[t]
    logit = dot_nt(normed_ffn, rt[...])
    prob = 1.0 / (1.0 + jnp.exp(-logit))
    picked = jnp.where(code > 0.5, prob, 0.0)
    weight = SCALE * picked / jnp.sum(picked, axis=-1, keepdims=True)
    weight4 = jnp.concatenate([weight] * 4, axis=0)
    w_hi = weight4.astype(BF16)
    w_lo = (weight4 - w_hi.astype(F32)).astype(BF16)
    code4 = jnp.concatenate([code] * 4, axis=0).astype(BF16)
    q1 = iota((64, rows), 1) >> 2
    j1 = iota((64, rows), 1) & 3
    e1 = (q1 * 171) >> 9
    c1 = iota((64, rows), 0)
    spread_t = ones_where(e1 == c1)
    slot_to = dot(code4, spread_t)
    fits = (slot_to == (q1 - 3 * e1 + 1).astype(F32)) & (j1 == (c1 >> 4))
    comb_hi = jnp.where(fits, dot(w_hi, spread_t), 0.0).astype(BF16)
    comb_lo = jnp.where(fits, dot(w_lo, spread_t), 0.0).astype(BF16)

    for d in near_first:
        arrived(kvb.at[lax.rem(z + NZ - d, NZ)], kzs.at[d], kzr.at[d])
    kvpart[...] = dot(rows_in, kvb[...].reshape(256, 256)).astype(BF16).reshape(8, SEQ, 256)
    for dx, dc in mates:
        g = xd[dx] * NC + cd[dc]
        send(kvpart.at[g], kvp.at[m], kps.at[dx, dc], kpr.at[dx, dc], (z, xd[dx], cd[dc], t))
    kvp[m] = kvpart[m]
    def to_rows(half, g):
        group = rbuf[96 * half + 48 * g : 96 * half + 48 * g + 48].reshape(192, HD)
        p, q = iota((48, 192), 0), iota((48, 192), 1)
        cols = [dot(ones_where(q == 4 * p + j), group).astype(BF16) for j in range(4)]
        return jnp.concatenate(cols, axis=1)

    def start_half(half):
        n = 96 if half == 0 else 93
        both = remote(
            sbuf.at[pl.ds(0, n)], rbuf.at[pl.ds(0, n)], as_.at[half], ar.at[half],
            (z, x, 1 - c, t),
        )
        both.wait_recv()
        raw = jnp.concatenate([to_rows(half, 0), to_rows(half, 1)], axis=0).astype(F32)
        rows_of = (raw * own_gain).astype(BF16)
        for d in (2, 1, 3):
            gs[half, d] = dot(rows_of, wgu[td[d]]).astype(BF16)
        for d in (2, 1, 3):
            dev = (z, x, c, td[d])
            send(gs.at[half, d], gr.at[half, d], gss.at[half, d], gsr.at[half, d], dev)
        gate_up = dot(rows_of, wgu[t])
        square = jnp.sum(raw * raw, axis=-1, keepdims=True)
        square = jnp.concatenate([square, jnp.zeros((32, 1), F32)], axis=0)
        fs[half, 0] = jnp.broadcast_to(square, (HD, HD)).T[0:8, :]
        for d in (2, 1, 3):
            dev = (z, x, c, td[d])
            send(fs.at[half, 0], fs.at[half, d], fss.at[half, d], fsr.at[half, d], dev)
        return gate_up, both

    def middle_half(half, gate_up):
        for d in (2, 1, 3):
            arrived(gr.at[half, d], gss.at[half, d], gsr.at[half, d])
            gate_up = gate_up + gr[half, d].astype(F32)
            arrived(fs.at[half, d], fss.at[half, d], fsr.at[half, d])
        square = fs[half, 0] + fs[half, 1] + fs[half, 2] + fs[half, 3]
        square = jnp.broadcast_to(square[0:1, :], (HD, HD)).T[0:96, 0:1]
        gate_up = gate_up * lax.rsqrt(square / 2048.0 + EPS)
        gate = gate_up[:, 0:HD]
        hidden = gate / (1.0 + jnp.exp(-gate)) * gate_up[:, HD : 2 * HD]
        hs[half, t] = hidden.astype(BF16)
        for d in (2, 1, 3):
            own = hs.at[half, t]
            send(own, own, hss.at[half, d], hsr.at[half, d], (z, x, c, td[d]))

    def end_half(half):
        for d in (2, 1, 3):
            arrived(hs.at[half, td[NT - d]], hss.at[half, d], hsr.at[half, d])
        out = dot(hs[half, 0], wd[0])
        for i in range(1, NT):
            out = out + dot(hs[half, i], wd[i])
        out = out.astype(BF16)
        p, q = iota((192, 48), 1), iota((192, 48), 0)
        for g in range(2):
            back = jnp.zeros((192, HD), F32)
            for j in range(4):
                block = out[48 * g : 48 * g + 48, HD * j : HD * j + HD]
                back = back + dot(ones_where(q == 4 * p + j), block)
            at = 96 * half + 48 * g
            obuf[at : at + 48] = back.astype(BF16).reshape(48, 4, HD)
        for r in ((4, 5, 3, 6) if half == 0 else (2, 7, 1, 0)):
            for dx, dc in around(r):
                p = 8 * order.index(r) + xd[dx] * NC + cd[dc]
                dev = (zd[r], xd[dx], cd[dc], t)
                remote(obuf.at[three(p)], cbuf.at[three(e)], rs_, rr, dev).start()

    for cp in ld_ex:
        cp.wait()
    for d in (1, 3, 2):
        src = td[NT - d]
        for k in range(2):
            arrived(wgu.at[src, :, pl.ds(128 * k, 128)], ys.at[k, d], yr.at[k, d])
    gate_up0, sent0 = start_half(0)
    gate_up1, sent1 = start_half(1)
    middle_half(0, gate_up0)
    middle_half(1, gate_up1)
    for d in (1, 3, 2):
        arrived(wd.at[td[NT - d]], ys.at[2, d], yr.at[2, d])
    end_half(0)
    end_half(1)
    cbuf[three(e)] = obuf[three(8 * order.index(0) + m)]
    shared_total = jnp.zeros((SEQ, 512), F32)
    for d in (2, 1, 3):
        arrived(ssr.at[td[NT - d]], sss.at[d], ssrr.at[d])
    for i in range(NT):
        shared_total = shared_total + ssr[i].astype(F32)
    base = res[t].astype(F32) + shared_total
    for dx, dc in mates:
        src = kvp.at[lax.rem(x + NX - dx, NX) * NC + cd[dc]]
        arrived(src, kps.at[dx, dc], kpr.at[dx, dc])
    new = kvp[0].astype(F32)
    for i in range(1, 8):
        new = new + kvp[i].astype(F32)
    fresh[0] = new[:, 0:HD].astype(BF16)
    fresh[1] = new[:, HD : 2 * HD].astype(BF16)
    stores = [load(fresh.at[0], fk_o), load(fresh.at[1], fv_o)]
    back = remote(
        obuf.at[pl.ds(0, 3 * NE - 3)], cbuf.at[pl.ds(0, 3 * NE - 3)], rs_, rr, (z, x, 1 - c, t)
    )
    back.wait_recv()
    came = cbuf[...].reshape(rows, HD)
    routed = dot(comb_hi, came) + dot(comb_lo, came)
    for j in range(4):
        mixed[:, HD * j : HD * j + HD] = (
            base[:, HD * j : HD * j + HD] + routed[SEQ * j : SEQ * j + SEQ]
        ).astype(BF16)
    stores.append(load(mixed, mixed_o))
    for cp in [*pending, sent0, sent1, back]:
        cp.wait_send()
    for cp in stores:
        cp.wait()


def hand_over(a, b, c, a_o, b_o, c_o):
    a_o[...] = a[...]
    b_o[...] = b[...]
    c_o[...] = c[...]


def body(
    tokens, attn_gain, query_weight, key_weight, value_weight, out_weight, head_gain,
    past_keys, past_values, break_offset, cache_lengths, ffn_gain, router_weight,
    expert_routes, expert_gate, expert_up, expert_down, shared_gate, shared_up, shared_down,
):
    hbm = pl.BlockSpec(memory_space=pl.ANY)
    v, dma = pltpu.VMEM, pltpu.SemaphoreType.DMA
    outs = pl.pallas_call(
        kernel,
        out_shape=(
            jax.ShapeDtypeStruct((SEQ, 512), BF16),
            jax.ShapeDtypeStruct((SEQ, HD), BF16),
            jax.ShapeDtypeStruct((SEQ, HD), BF16),
        ),
        in_specs=[hbm] * 20,
        out_specs=(hbm,) * 3,
        scratch_shapes=[
            v((SEQ, 2048), BF16), v((16, HD), BF16), v((2, HD), BF16), v((16, HD), BF16),
            v((64, 2048), BF16), v((6, SEQ), jnp.int32), v((SEQ, 2, POS), F32),
            v((SEQ, POS, HD), BF16), v((SEQ, HD, POS), BF16), v((SEQ, POS, HD), BF16),
            v((NZ, 32, 256), BF16), v((NZ, 32, 256), BF16), v((NZ, NX, NC, 32, 256), BF16),
            v((NT, 512, 256), BF16), v((NT, 128, 512), BF16),
            v((2048, 256), BF16), v((128, 2048), BF16),
            v((8, SEQ, 256), BF16), v((8, SEQ, 256), BF16),
            v((8, SEQ, 256), F32), v((8, SEQ, 256), F32),
            v((8, SEQ, 256), BF16), v((8, SEQ, 256), BF16),
            v((2 * SEQ, HD), F32), v((2 * SEQ, POS), F32), v((2 * SEQ, HD), jnp.int32),
            v((SEQ, 256), F32), v((NT, SEQ, 512), BF16), v((NT, SEQ, 512), BF16),
            v((NT, SEQ, HD), F32), v((2, NT, 8, HD), F32), v((NT, SEQ, 512), BF16),
            v((3 * NE, 4, HD), BF16), v((3 * NE, 4, HD), BF16),
            v((2, NT, 96, 256), BF16), v((2, NT, 96, 256), BF16), v((2, NT, 96, HD), BF16),
            v((3 * NE, 4, HD), BF16), v((3 * NE, 4, HD), BF16),
            v((NT, SEQ, 512), BF16), v((NT, SEQ, 512), BF16),
            pltpu.SMEM((SEQ,), jnp.int32), v((SEQ, 512), BF16), v((SEQ, 512), BF16),
            v((2, SEQ, HD), BF16), dma((32,)), dma((8,)),
            *[dma((NZ,)) for _ in range(6)],
            dma((NZ, NX)), dma((NZ, NX)), dma((NZ,)), dma((NZ,)),
            *[dma((NX, NC)) for _ in range(6)],
            dma((3, 4)), dma((3, 4)), dma((2, 4)), dma((2, 4)), dma((2,)), dma((2,)),
            dma((2, 4)), dma((2, 4)), dma((2, 4)), dma((2, 4)), dma, dma, dma((4,)), dma((4,)),
            dma((4,)), dma((4,)), dma((2, 4)), dma((2, 4)),
        ],
        compiler_params=pltpu.CompilerParams(
            collective_id=0, has_side_effects=True, vmem_limit_bytes=60 * 1024 * 1024
        ),
    )(
        tokens, attn_gain.reshape(16, HD), query_weight, key_weight, value_weight, out_weight,
        head_gain.reshape(2, HD), past_keys.reshape(SEQ, POS, HD),
        past_values.reshape(SEQ, POS, HD), break_offset, cache_lengths,
        ffn_gain.reshape(16, HD), router_weight.T, expert_routes.T, expert_gate, expert_up,
        expert_down, shared_gate, shared_up, shared_down,
    )
    return pl.pallas_call(
        hand_over,
        out_shape=tuple(jax.ShapeDtypeStruct(o.shape, o.dtype) for o in outs),
        in_specs=[pl.BlockSpec(memory_space=pltpu.VMEM)] * 3,
        out_specs=(pl.BlockSpec(memory_space=pltpu.VMEM),) * 3,
    )(*outs)


def solution(mesh):
    torus = Mesh(mesh.devices.reshape(NZ, NX, NC, NT), (*EP, "tp"))
    return jax.shard_map(
        body,
        mesh=torus,
        in_specs=(
            P(EP, None),
            P(),
            P(EP, "tp"),
            P(EP, "tp"),
            P(EP, "tp"),
            P(EP, "tp"),
            P("tp"),
            P(EP, None, "tp", None),
            P(EP, None, "tp", None),
            P(EP, "tp", None),
            P(EP),
            P(),
            P(),
            P(EP, None),
            P(EP, None, "tp"),
            P(EP, None, "tp"),
            P(EP, "tp", None),
            P(None, "tp"),
            P(None, "tp"),
            P("tp", None),
        ),
        out_specs=(P(EP, "tp"), P(EP, "tp"), P(EP, "tp")),
        check_vma=False,
    )
```

```python
import jax
import jax.numpy as jnp
from jax import lax
from jax.experimental import pallas as pl
from jax.experimental.pallas import tpu as pltpu
from jax.sharding import Mesh
from jax.sharding import PartitionSpec as P

MESH = pl.DeviceIdType.MESH
EP = ("ep_0", "ep_1", "ep_2")
NZ, NX, NC, NT = 8, 4, 2, 4
NE = NZ * NX * NC
SEQ = 16
POS = 1024
HD = 128
EPS = 1e-06
SCALE = 2.5
F32 = jnp.float32
BF16 = jnp.bfloat16


def dot(a, b):
    return jnp.dot(a, b, preferred_element_type=F32)


def dot_nt(a, b):
    return lax.dot_general(a, b, (((1,), (1,)), ((), ())), preferred_element_type=F32)


def iota(shape, dim):
    return lax.broadcasted_iota(jnp.int32, shape, dim)


def ones_where(cond):
    return jnp.where(cond, 1.0, 0.0).astype(BF16)


def kernel(
    tok_h, ag_h, wq_h, wk_h, wv_h, wo_h, hg_h, pk_h, pv_h, off_h, lens_h, fg_h, rt_h, er_h,
    eg_h, eu_h, ed_h, sg_h, su_h, sd_h,
    mixed_o, fk_o, fv_o,
    tok, ag, hg, fg, rt, er, off, kb, kt, vb, qb, kvb, ob, wgu, wd, sgu, sd,
    tkb, tk, part, qp, kvpart, kvp,
    qs, lg, lenb, ho, pcs, pc, sq, fs, res, sbuf, rbuf, gs0, gs1, gs2, gr0, gr1, gr2, hs0, hs1, hs2,
    pick72, back72, pick48, back48, obuf, cbuf, ssb, ssr,
    lens, tokb, mixed, fresh, lsem, kvsem,
    qzs, qzr, kzs, kzr, ozs, ozr, oxs, oxr, ods, odr, tks, tkr, qps, qpr, kps, kpr,
    ys, yr, cs, cr, as_, ar, gss, gsr, hss, hsr, rs_, rr, sss, ssrr, as2, ar2, fss, fsr,
):
    z = lax.axis_index("ep_0")
    x = lax.axis_index("ep_1")
    c = lax.axis_index("ep_2")
    t = lax.axis_index("tp")
    e = (z * NX + x) * NC + c
    m = x * NC + c
    zd = [lax.rem(z + d, NZ) for d in range(NZ)]
    xd = [lax.rem(x + d, NX) for d in range(NX)]
    td = [lax.rem(t + d, NT) for d in range(NT)]
    cd = [c, 1 - c]
    mates = [(2, 0), (2, 1), (1, 0), (3, 0), (1, 1), (3, 1), (0, 1)]
    far_first = [4, 3, 5, 2, 6, 1, 7]
    near_first = far_first[::-1]

    def remote(src, dst, ssem, rsem, dev):
        return pltpu.make_async_remote_copy(
            src_ref=src, dst_ref=dst, send_sem=ssem, recv_sem=rsem,
            device_id=dev, device_id_type=MESH,
        )

    pending = []

    def send(src, dst, ssem, rsem, dev):
        cp = remote(src, dst, ssem, rsem, dev)
        cp.start()
        pending.append(cp)

    def arrived(dst, ssem, rsem):
        remote(dst, dst, ssem, rsem, (z, x, 1 - c, t)).wait_recv()

    loads = []

    def load(src, dst):
        cp = pltpu.make_async_copy(src, dst, lsem.at[len(loads)])
        cp.start()
        loads.append(cp)
        return cp

    ld_q = load(wq_h, qb.at[z])
    ld_tok = [load(tok_h, tok), load(ag_h, ag)]
    ld_o = load(wo_h, ob.at[z, x, c])
    ld_kv = [
        load(wk_h, kvb.at[z, :, pl.ds(0, 128)]),
        load(wv_h, kvb.at[z, :, pl.ds(128, 128)]),
    ]
    barrier = pltpu.get_barrier_semaphore()
    first = [(zd[d], x, c, t) for d in range(1, NZ)]
    first += [(z, xd[dx], cd[dc], t) for dx, dc in mates]
    first += [(z, x, c, td[d]) for d in range(1, NT)]
    for dev in first:
        pl.semaphore_signal(barrier, inc=1, device_id=dev, device_id_type=MESH)

    pl.semaphore_wait(barrier, len(first))

    mine_o = ob.at[z, x, c]

    def q_around(*steps):
        for d in steps:
            send(qb.at[z], qb.at[z], qzs.at[d], qzr.at[d], (zd[d], x, c, t))

    def o_around(*steps):
        for d in steps:
            send(mine_o, mine_o, ozs.at[d], ozr.at[d], (zd[d], x, c, t))

    ld_q.wait()
    q_around(*far_first)

    ld_o.wait()
    for cp in ld_tok:
        cp.wait()
    data = tok[...].astype(F32)
    factor = lax.rsqrt(jnp.mean(data * data, axis=-1, keepdims=True) + EPS)
    gain = ag[...].astype(F32)
    blocks = []
    for i in range(NZ):
        halves = []
        for k in (2 * i, 2 * i + 1):
            halves.append(data[:, HD * k : HD * k + HD] * factor * gain[k : k + 1, :])
        blocks.append(jnp.concatenate(halves, axis=1).astype(BF16).astype(F32))
    chunk = iota((SEQ, 256), 1) >> 5
    for g in range(8):
        own = blocks[g]
        for k in range(1, 8):
            j = (g + k) % 8
            own = jnp.where(chunk == j, pltpu.roll(blocks[j], 32 * k, 1), own)
        tkb[g] = own.astype(BF16)
    for dx, dc in mates:
        g = xd[dx] * NC + cd[dc]
        send(tkb.at[g], tk.at[m], tks.at[dx, dc], tkr.at[dx, dc], (z, xd[dx], cd[dc], t))
    tk[m] = tkb[m]

    def o_along(r):
        src = ob.at[zd[r], x, c]
        for i in (2, 1, 3):
            send(src, src, oxs.at[r, i], oxr.at[r, i], (z, xd[i], c, t))

    def o_forward(r):
        src = ob.at[zd[r], x, c]
        arrived(src, ozs.at[NZ - r], ozr.at[NZ - r])
        o_along(r)

    def o_across(r):
        for i in (1, 3, 2):
            arrived(ob.at[zd[r], xd[i], c], oxs.at[r, NX - i], oxr.at[r, NX - i])
        src = ob.at[zd[r], :, c]
        send(src, src, ods.at[r], odr.at[r], (z, x, 1 - c, t))

    def o_last():
        for r in range(NZ):
            arrived(ob.at[zd[r], :, 1 - c], ods.at[r], odr.at[r])

    o_along(0)
    ld_er = load(er_h, er)
    ld_att = [load(off_h, off), load(hg_h, hg), load(lens_h, lens)]
    kv_loads = []
    for i in range(4):
        ds = pl.ds(4 * i, 4)
        kv_loads.append(pltpu.make_async_copy(pk_h.at[ds], kb.at[ds], kvsem.at[i]))
        kv_loads.append(pltpu.make_async_copy(pv_h.at[ds], vb.at[ds], kvsem.at[4 + i]))
    for cp in kv_loads:
        cp.start()
    ld_ffn = [load(fg_h, fg), load(rt_h, rt)]
    ld_sh = [
        load(sg_h, sgu.at[:, pl.ds(0, 128)]),
        load(su_h, sgu.at[:, pl.ds(128, 128)]),
        load(sd_h, sd),
    ]
    mine = pl.ds(pl.multiple_of(t * 512, 512), 512)
    ld_own = load(tok_h.at[:, mine], tokb)
    ld_ex = [
        load(eg_h.at[0, mine, :], wgu.at[t, :, pl.ds(0, 128)]),
        load(eu_h.at[0, mine, :], wgu.at[t, :, pl.ds(128, 128)]),
        load(ed_h.at[0, :, mine], wd.at[t]),
    ]

    def recut_down(peers):
        for d in peers:
            theirs = pl.ds(pl.multiple_of(td[d] * 512, 512), 512)
            send(ed_h.at[0, :, theirs], wd.at[t], ys.at[2, d], yr.at[2, d], (z, x, c, td[d]))

    for d in (1, 3, 2):
        p = td[d]
        dev = (z, x, c, p)
        theirs = pl.ds(pl.multiple_of(p * 512, 512), 512)
        for k, src in enumerate((eg_h, eu_h)):
            half = pl.ds(128 * k, 128)
            send(src.at[0, theirs, :], wgu.at[t, :, half], ys.at[k, d], yr.at[k, d], dev)
    recut_down((1, 3))

    ld_er.wait()
    rows = NE * 12
    chosen = iota((NE, SEQ), 0) == er[0:1, :]
    for k in range(1, 6):
        chosen = chosen | (iota((NE, SEQ), 0) == er[k : k + 1, :])
    hot_t = ones_where(chosen)
    before = ones_where(iota((SEQ, SEQ), 0) < iota((SEQ, SEQ), 1))
    code_t = jnp.where(chosen, dot(hot_t, before) + 1.0, 0.0).astype(BF16)
    repeat = ones_where((iota((SEQ, 64), 1) & 15) == iota((SEQ, 64), 0))
    eye = ones_where(iota((SEQ, SEQ), 0) == iota((SEQ, SEQ), 1))
    code4_t = dot(code_t, repeat).astype(BF16)
    code = dot_nt(eye, code_t)
    q0 = iota((rows, 64), 0) >> 2
    j0 = iota((rows, 64), 0) & 3
    e0 = (q0 * 171) >> 9
    c0 = iota((rows, 64), 1)
    spread = ones_where(e0 == c0)
    slot_of = dot(spread, code4_t)
    want = (q0 - 3 * e0 + 1).astype(F32)
    dispatch = ones_where((slot_of == want) & (j0 == (c0 >> 4)))

    o_around(1, 7, 4, 3, 5, 2, 6)
    for n, pick, back in ((72, pick72, back72), (48, pick48, back48)):
        for j in range(4):
            p, q = iota((n, 4 * n), 0), iota((n, 4 * n), 1)
            pick[n * j : n * j + n, :] = jnp.where(q == 4 * p + j, 1.0, 0.0)
        p, q = iota((4 * n, 4 * n), 1), iota((4 * n, 4 * n), 0)
        j = (p >= n).astype(jnp.int32) + (p >= 2 * n) + (p >= 3 * n)
        back[...] = ones_where(q == 4 * (p - n * j) + j)
    for b in range(SEQ):
        if b % 4 == 0:
            kv_loads[2 * (b // 4)].wait()
        kt[b] = kb[b].T

    for dx, dc in mates:
        src = tk.at[lax.rem(x + NX - dx, NX) * NC + cd[dc]]
        arrived(src, tks.at[dx, dc], tkr.at[dx, dc])
    for d in near_first:
        arrived(qb.at[lax.rem(z + NZ - d, NZ)], qzs.at[d], qzr.at[d])
    rows_in = tk[...].reshape(8 * SEQ, 256)
    part[...] = dot(rows_in, qb[...].reshape(256, 256)).reshape(8, SEQ, 256)
    for dx, dc in mates:
        g = xd[dx] * NC + cd[dc]
        send(part.at[g], qp.at[m], qps.at[dx, dc], qpr.at[dx, dc], (z, xd[dx], cd[dc], t))
    qp[m] = part[m]
    for r in (7, 1, 6, 2, 5, 3, 4):
        o_forward(r)
    for r in (0, 7, 1):
        o_across(r)
    for dx, dc in mates:
        src = qp.at[lax.rem(x + NX - dx, NX) * NC + cd[dc]]
        arrived(src, qps.at[dx, dc], qpr.at[dx, dc])
    total = qp[0]
    for i in range(1, 8):
        total = total + qp[i]
    queries = total.astype(BF16).astype(F32)

    for h in range(2):
        qs[pl.ds(h, SEQ, stride=2), :] = queries[:, HD * h : HD * h + HD]
    for cp in ld_att:
        cp.wait()
    for b in range(SEQ):
        q = qs[2 * b : 2 * b + 2, :].astype(BF16)
        lg[2 * b : 2 * b + 2, :] = dot(q, kt[b]) * HD ** (-0.5) + off[b]
        lenb[2 * b : 2 * b + 2, :] = jnp.full((2, HD), lens[b], jnp.int32)
    for cp in ld_kv:
        cp.wait()
    for d in far_first:
        send(kvb.at[z], kvb.at[z], kzs.at[d], kzr.at[d], (zd[d], x, c, t))
    for r in (6, 2):
        o_across(r)
    logits = lg[...]
    length = lenb[:, 0:1]
    usable = iota((2 * SEQ, POS), 1) < length
    tail = jnp.log(1.0 + jnp.exp(-jnp.abs(logits)))
    keep = jnp.where(usable, jnp.minimum(-logits, 0.0) - tail, 0.0)
    nb = POS // HD
    stacked = jnp.concatenate([keep[:, HD * i : HD * i + HD] for i in range(nb)], axis=0)
    k1 = stacked.astype(BF16)
    left = stacked - k1.astype(F32)
    k2 = left.astype(BF16)
    k3 = (left - k2.astype(F32)).astype(BF16)
    later = ones_where(iota((HD, HD), 0) > iota((HD, HD), 1))
    inner = dot(k1, later) + dot(k2, later) + dot(k3, later)
    carry = jnp.zeros((2 * SEQ, 1), F32)
    after = [None] * nb
    n2 = 2 * SEQ
    for i in range(nb - 1, -1, -1):
        after[i] = inner[n2 * i : n2 * i + n2] + carry
        carry = carry + jnp.sum(stacked[n2 * i : n2 * i + n2], axis=-1, keepdims=True)
    after = jnp.concatenate(after, axis=1)
    sticks = jnp.where(usable, jnp.exp(jnp.minimum(logits, 0.0) - tail + after), 0.0)
    lg[...] = sticks
    for b in range(SEQ):
        if b % 4 == 0:
            kv_loads[2 * (b // 4) + 1].wait()
        got = dot(lg[2 * b : 2 * b + 2, :].astype(BF16), vb[b])
        ho[b : b + 1, 0:HD] = got[0:1, :]
        ho[b : b + 1, HD : 2 * HD] = got[1:2, :]
    for r in (5, 3, 4):
        o_across(r)
    heads_out = ho[...]
    scaled = jnp.concatenate(
        [heads_out[:, HD * i : HD * i + HD] * hg[i : i + 1, :].astype(F32) for i in range(2)],
        axis=1,
    ).astype(BF16)
    sq[t] = jnp.broadcast_to(jnp.sum(heads_out * heads_out, axis=-1, keepdims=True), (SEQ, HD))
    o_last()
    for i in range(NT):
        halves = [dot_nt(scaled, ob[zi].reshape(256, 256)) for zi in (2 * i, 2 * i + 1)]
        pcs[i] = jnp.concatenate(halves, axis=1).astype(BF16)

    for d in (2, 1, 3):
        dev = (z, x, c, td[d])
        send(sq.at[t], sq.at[t], cs.at[0, d], cr.at[0, d], dev)
        send(pcs.at[td[d]], pc.at[t], cs.at[1, d], cr.at[1, d], dev)
    pc[t] = pcs[t]
    for d in (1, 3, 2):
        src = td[NT - d]
        for k, buf in enumerate((sq, pc)):
            arrived(buf.at[src], cs.at[k, d], cr.at[k, d])
    head_total = pc[0].astype(F32)
    square = sq[0]
    for i in range(1, NT):
        head_total = head_total + pc[i].astype(F32)
        square = square + sq[i]
    attention = head_total * lax.rsqrt(square[:, 0:1] / 1024.0 + EPS)
    ld_own.wait()
    residual = (tokb[...].astype(F32) + attention).astype(BF16)
    res[t] = residual
    for d in (2, 1, 3):
        send(res.at[t], res.at[t], as2.at[d], ar2.at[d], (z, x, c, td[d]))

    block = jnp.concatenate([residual[:, HD * j : HD * j + HD] for j in range(4)], axis=0)
    sbuf[...] = dot(dispatch, block).astype(BF16).reshape(3 * NE, 4, HD)
    order = (3, 4, 5, 2, 6, 7, 0, 1)
    part_rows = (72, 48, 72)
    first_row = (0, 72, 120)

    def three(i):
        return pl.ds(3 * i, 3)

    def part_of(r):
        return (0, 0, 0, 1, 1, 2, 2, 2)[order.index(r)]

    def around(r):
        return [(0, 0), *mates] if r else mates

    for r in (7, 1, 0, 4, 5, 3, 6, 2):
        d = (NZ - r) % NZ
        to = three(8 * order.index(r) + m)
        for dx, dc in around(r):
            p = (zd[d] * NX + xd[dx]) * NC + cd[dc]
            dev = (zd[d], xd[dx], cd[dc], t)
            remote(sbuf.at[three(p)], rbuf.at[to], as_.at[part_of(r)], ar.at[part_of(r)], dev).start()
    rbuf[three(8 * order.index(0) + m)] = sbuf[three(e)]

    recut_down((2,))

    for cp in ld_ffn:
        cp.wait()
    gain = fg[...].astype(F32)
    own_gain = []
    for j in range(4):
        row = gain[j : j + 1, :]
        for i in range(1, NT):
            row = jnp.where(t == i, gain[4 * i + j : 4 * i + j + 1, :], row)
        own_gain.append(row)
    own_gain = jnp.concatenate(own_gain, axis=1)

    gs, gr, hs = (gs0, gs1, gs2), (gr0, gr1, gr2), (hs0, hs1, hs2)

    def start_part(k):
        n, at = part_rows[k], first_row[k]
        pick = pick48 if n == 48 else pick72
        remote_rows = n if k < 2 else n - 3
        both = remote(
            sbuf.at[pl.ds(0, remote_rows)], rbuf.at[pl.ds(0, remote_rows)], as_.at[k], ar.at[k],
            (z, x, 1 - c, t),
        )
        both.wait_recv()
        came = dot(pick[...].astype(BF16), rbuf[at : at + n].reshape(4 * n, HD))
        raw = jnp.concatenate([came[n * j : n * j + n] for j in range(4)], axis=1)
        rows_of = (raw * own_gain).astype(BF16)
        for d in (2, 1, 3):
            gs[k][d] = dot(rows_of, wgu[td[d]]).astype(BF16)
        for d in (2, 1, 3):
            send(gs[k].at[d], gr[k].at[d], gss.at[k, d], gsr.at[k, d], (z, x, c, td[d]))
        gate_up = dot(rows_of, wgu[t])
        square = jnp.sum(raw * raw, axis=-1, keepdims=True)
        square = jnp.concatenate([square, jnp.zeros((HD - n, 1), F32)], axis=0)
        fs[k, 0] = jnp.broadcast_to(square, (HD, HD)).T[0:8, :]
        for d in (2, 1, 3):
            send(fs.at[k, 0], fs.at[k, d], fss.at[k, d], fsr.at[k, d], (z, x, c, td[d]))
        return gate_up, both

    def middle_part(k, gate_up):
        for d in (2, 1, 3):
            arrived(gr[k].at[d], gss.at[k, d], gsr.at[k, d])
            gate_up = gate_up + gr[k][d].astype(F32)
            arrived(fs.at[k, d], fss.at[k, d], fsr.at[k, d])
        square = fs[k, 0] + fs[k, 1] + fs[k, 2] + fs[k, 3]
        square = jnp.broadcast_to(square[0:1, :], (HD, HD)).T[0 : part_rows[k], 0:1]
        gate_up = gate_up * lax.rsqrt(square / 2048.0 + EPS)
        gate = gate_up[:, 0:HD]
        hidden = gate / (1.0 + jnp.exp(-gate)) * gate_up[:, HD : 2 * HD]
        hs[k][t] = hidden.astype(BF16)
        own = hs[k].at[t]
        for d in (2, 1, 3):
            send(own, own, hss.at[k, d], hsr.at[k, d], (z, x, c, td[d]))

    def end_part(k):
        n, at = part_rows[k], first_row[k]
        back = back48 if n == 48 else back72
        for d in (2, 1, 3):
            arrived(hs[k].at[td[NT - d]], hss.at[k, d], hsr.at[k, d])
        out = dot(hs[k][0], wd[0])
        for i in range(1, NT):
            out = out + dot(hs[k][i], wd[i])
        out = jnp.concatenate([out[:, HD * j : HD * j + HD] for j in range(4)], axis=0)
        obuf[at : at + n] = dot(back[...], out.astype(BF16)).astype(BF16).reshape(n, 4, HD)
        for r in ((4, 5, 3), (6, 2), (7, 1, 0))[k]:
            for dx, dc in around(r):
                p = 8 * order.index(r) + xd[dx] * NC + cd[dc]
                dev = (zd[r], xd[dx], cd[dc], t)
                remote(obuf.at[three(p)], cbuf.at[three(e)], rs_, rr, dev).start()

    for cp in ld_ex:
        cp.wait()
    for d in (1, 3, 2):
        src = td[NT - d]
        for k in range(2):
            arrived(wgu.at[src, :, pl.ds(128 * k, 128)], ys.at[k, d], yr.at[k, d])
    gate_up2, sent2 = start_part(2)

    for d in (1, 3, 2):
        arrived(res.at[td[NT - d]], as2.at[d], ar2.at[d])
    data = jnp.concatenate([res[i] for i in range(NT)], axis=1).astype(F32)
    factor = lax.rsqrt(jnp.mean(data * data, axis=-1, keepdims=True) + EPS)
    pieces = [data[:, HD * i : HD * i + HD] * factor * gain[i : i + 1, :] for i in range(16)]
    normed_ffn = jnp.concatenate(pieces, axis=1).astype(BF16)
    for cp in ld_sh:
        cp.wait()
    both = dot(normed_ffn, sgu[...])
    gate = both[:, 0:HD]
    shared_hidden = (gate / (1.0 + jnp.exp(-gate)) * both[:, HD : 2 * HD]).astype(BF16)
    shared_part = dot(shared_hidden, sd[...]).astype(BF16)
    for i in range(NT):
        ssb[i] = shared_part[:, 512 * i : 512 * i + 512]
    for d in (2, 1, 3):
        p = td[d]
        send(ssb.at[p], ssr.at[t], sss.at[d], ssrr.at[d], (z, x, c, p))
    ssr[t] = ssb[t]
    logit = dot_nt(normed_ffn, rt[...])
    prob = 1.0 / (1.0 + jnp.exp(-logit))
    picked = jnp.where(code > 0.5, prob, 0.0)
    weight = SCALE * picked / jnp.sum(picked, axis=-1, keepdims=True)
    weight4 = jnp.concatenate([weight] * 4, axis=0)
    w_hi = weight4.astype(BF16)
    w_lo = (weight4 - w_hi.astype(F32)).astype(BF16)
    code4 = jnp.concatenate([code] * 4, axis=0).astype(BF16)
    q1 = iota((64, rows), 1) >> 2
    j1 = iota((64, rows), 1) & 3
    e1 = (q1 * 171) >> 9
    c1 = iota((64, rows), 0)
    spread_t = ones_where(e1 == c1)
    slot_to = dot(code4, spread_t)
    fits = (slot_to == (q1 - 3 * e1 + 1).astype(F32)) & (j1 == (c1 >> 4))
    comb_hi = jnp.where(fits, dot(w_hi, spread_t), 0.0).astype(BF16)
    comb_lo = jnp.where(fits, dot(w_lo, spread_t), 0.0).astype(BF16)

    for d in near_first:
        arrived(kvb.at[lax.rem(z + NZ - d, NZ)], kzs.at[d], kzr.at[d])
    kvpart[...] = dot(rows_in, kvb[...].reshape(256, 256)).astype(BF16).reshape(8, SEQ, 256)
    for dx, dc in mates:
        g = xd[dx] * NC + cd[dc]
        send(kvpart.at[g], kvp.at[m], kps.at[dx, dc], kpr.at[dx, dc], (z, xd[dx], cd[dc], t))
    kvp[m] = kvpart[m]
    gate_up0, sent0 = start_part(0)
    gate_up1, sent1 = start_part(1)
    middle_part(2, gate_up2)
    middle_part(0, gate_up0)
    middle_part(1, gate_up1)
    for d in (1, 3, 2):
        arrived(wd.at[td[NT - d]], ys.at[2, d], yr.at[2, d])
    end_part(0)
    end_part(2)
    end_part(1)
    cbuf[three(e)] = obuf[three(8 * order.index(0) + m)]
    shared_total = jnp.zeros((SEQ, 512), F32)
    for d in (2, 1, 3):
        arrived(ssr.at[td[NT - d]], sss.at[d], ssrr.at[d])
    for i in range(NT):
        shared_total = shared_total + ssr[i].astype(F32)
    base = res[t].astype(F32) + shared_total
    for dx, dc in mates:
        src = kvp.at[lax.rem(x + NX - dx, NX) * NC + cd[dc]]
        arrived(src, kps.at[dx, dc], kpr.at[dx, dc])
    new = kvp[0].astype(F32)
    for i in range(1, 8):
        new = new + kvp[i].astype(F32)
    fresh[0] = new[:, 0:HD].astype(BF16)
    fresh[1] = new[:, HD : 2 * HD].astype(BF16)
    stores = [load(fresh.at[0], fk_o), load(fresh.at[1], fv_o)]
    back = remote(
        obuf.at[pl.ds(0, 3 * NE - 3)], cbuf.at[pl.ds(0, 3 * NE - 3)], rs_, rr, (z, x, 1 - c, t)
    )
    back.wait_recv()
    came = cbuf[...].reshape(rows, HD)
    routed = dot(comb_hi, came) + dot(comb_lo, came)
    for j in range(4):
        mixed[:, HD * j : HD * j + HD] = (
            base[:, HD * j : HD * j + HD] + routed[SEQ * j : SEQ * j + SEQ]
        ).astype(BF16)
    stores.append(load(mixed, mixed_o))
    for cp in [*pending, sent0, sent1, sent2, back]:
        cp.wait_send()
    for cp in stores:
        cp.wait()


def hand_over(a, b, c, a_o, b_o, c_o):
    a_o[...] = a[...]
    b_o[...] = b[...]
    c_o[...] = c[...]


def body(
    tokens, attn_gain, query_weight, key_weight, value_weight, out_weight, head_gain,
    past_keys, past_values, break_offset, cache_lengths, ffn_gain, router_weight,
    expert_routes, expert_gate, expert_up, expert_down, shared_gate, shared_up, shared_down,
):
    hbm = pl.BlockSpec(memory_space=pl.ANY)
    v, dma = pltpu.VMEM, pltpu.SemaphoreType.DMA
    outs = pl.pallas_call(
        kernel,
        out_shape=(
            jax.ShapeDtypeStruct((SEQ, 512), BF16),
            jax.ShapeDtypeStruct((SEQ, HD), BF16),
            jax.ShapeDtypeStruct((SEQ, HD), BF16),
        ),
        in_specs=[hbm] * 20,
        out_specs=(hbm,) * 3,
        scratch_shapes=[
            v((SEQ, 2048), BF16), v((16, HD), BF16), v((2, HD), BF16), v((16, HD), BF16),
            v((64, 2048), BF16), v((6, SEQ), jnp.int32), v((SEQ, 2, POS), F32),
            v((SEQ, POS, HD), BF16), v((SEQ, HD, POS), BF16), v((SEQ, POS, HD), BF16),
            v((NZ, 32, 256), BF16), v((NZ, 32, 256), BF16), v((NZ, NX, NC, 32, 256), BF16),
            v((NT, 512, 256), BF16), v((NT, 128, 512), BF16),
            v((2048, 256), BF16), v((128, 2048), BF16),
            v((8, SEQ, 256), BF16), v((8, SEQ, 256), BF16),
            v((8, SEQ, 256), F32), v((8, SEQ, 256), F32),
            v((8, SEQ, 256), BF16), v((8, SEQ, 256), BF16),
            v((2 * SEQ, HD), F32), v((2 * SEQ, POS), F32), v((2 * SEQ, HD), jnp.int32),
            v((SEQ, 256), F32), v((NT, SEQ, 512), BF16), v((NT, SEQ, 512), BF16),
            v((NT, SEQ, HD), F32), v((3, NT, 8, HD), F32), v((NT, SEQ, 512), BF16),
            v((3 * NE, 4, HD), BF16), v((3 * NE, 4, HD), BF16),
            *[v((NT, n, 256), BF16) for _ in range(2) for n in (72, 48, 72)],
            *[v((NT, n, HD), BF16) for n in (72, 48, 72)],
            v((288, 288), F32), v((288, 288), BF16), v((192, 192), F32), v((192, 192), BF16),

            v((3 * NE, 4, HD), BF16), v((3 * NE, 4, HD), BF16),
            v((NT, SEQ, 512), BF16), v((NT, SEQ, 512), BF16),
            pltpu.SMEM((SEQ,), jnp.int32), v((SEQ, 512), BF16), v((SEQ, 512), BF16),
            v((2, SEQ, HD), BF16), dma((32,)), dma((8,)),
            *[dma((NZ,)) for _ in range(6)],
            dma((NZ, NX)), dma((NZ, NX)), dma((NZ,)), dma((NZ,)),
            *[dma((NX, NC)) for _ in range(6)],
            dma((3, 4)), dma((3, 4)), dma((2, 4)), dma((2, 4)), dma((3,)), dma((3,)),
            dma((3, 4)), dma((3, 4)), dma((3, 4)), dma((3, 4)), dma, dma, dma((4,)), dma((4,)),
            dma((4,)), dma((4,)), dma((3, 4)), dma((3, 4)),
        ],
        compiler_params=pltpu.CompilerParams(
            collective_id=0, has_side_effects=True, vmem_limit_bytes=60 * 1024 * 1024
        ),
    )(
        tokens, attn_gain.reshape(16, HD), query_weight, key_weight, value_weight, out_weight,
        head_gain.reshape(2, HD), past_keys.reshape(SEQ, POS, HD),
        past_values.reshape(SEQ, POS, HD), break_offset, cache_lengths,
        ffn_gain.reshape(16, HD), router_weight.T, expert_routes.T, expert_gate, expert_up,
        expert_down, shared_gate, shared_up, shared_down,
    )
    return pl.pallas_call(
        hand_over,
        out_shape=tuple(jax.ShapeDtypeStruct(o.shape, o.dtype) for o in outs),
        in_specs=[pl.BlockSpec(memory_space=pltpu.VMEM)] * 3,
        out_specs=(pl.BlockSpec(memory_space=pltpu.VMEM),) * 3,
    )(*outs)


def solution(mesh):
    torus = Mesh(mesh.devices.reshape(NZ, NX, NC, NT), (*EP, "tp"))
    return jax.shard_map(
        body,
        mesh=torus,
        in_specs=(
            P(EP, None),
            P(),
            P(EP, "tp"),
            P(EP, "tp"),
            P(EP, "tp"),
            P(EP, "tp"),
            P("tp"),
            P(EP, None, "tp", None),
            P(EP, None, "tp", None),
            P(EP, "tp", None),
            P(EP),
            P(),
            P(),
            P(EP, None),
            P(EP, None, "tp"),
            P(EP, None, "tp"),
            P(EP, "tp", None),
            P(None, "tp"),
            P(None, "tp"),
            P("tp", None),
        ),
        out_specs=(P(EP, "tp"), P(EP, "tp"), P(EP, "tp")),
        check_vma=False,
    )
```

```python
import jax
import jax.numpy as jnp
from jax import lax
from jax.experimental import pallas as pl
from jax.experimental.pallas import tpu as pltpu
from jax.sharding import Mesh
from jax.sharding import PartitionSpec as P

MESH = pl.DeviceIdType.MESH
EP = ("ep_0", "ep_1", "ep_2")
NZ, NX, NC, NT = 8, 4, 2, 4
NE = NZ * NX * NC
SEQ = 16
POS = 1024
HD = 128
EPS = 1e-06
SCALE = 2.5
F32 = jnp.float32
BF16 = jnp.bfloat16


def dot(a, b):
    return jnp.dot(a, b, preferred_element_type=F32)


def dot_nt(a, b):
    return lax.dot_general(a, b, (((1,), (1,)), ((), ())), preferred_element_type=F32)


def iota(shape, dim):
    return lax.broadcasted_iota(jnp.int32, shape, dim)


def ones_where(cond):
    return jnp.where(cond, 1.0, 0.0).astype(BF16)


def kernel(
    tok_h, ag_h, wq_h, wk_h, wv_h, wo_h, hg_h, pk_h, pv_h, off_h, lens_h, fg_h, rt_h, er_h,
    eg_h, eu_h, ed_h, sg_h, su_h, sd_h,
    mixed_o, fk_o, fv_o,
    tok, ag, hg, fg, rt, er, off, kb, kt, vb, qb, kvb, ob, wgu, wd, sgu, sd,
    tkb, tk, part, qp, kvpart, kvp,
    qs, lg, lenb, ho, pcs, pc, sq, fs, res, sbuf, rbuf, gs0, gs1, gs2, gr0, gr1, gr2, hs0, hs1, hs2,
    pick72, back72, pick48, back48, obuf, cbuf, ssb, ssr,
    lens, tokb, lsem, kvsem,
    qzs, qzr, kzs, kzr, ozs, ozr, oxs, oxr, ods, odr, tks, tkr, qps, qpr, kps, kpr,
    ys, yr, cs, cr, as_, ar, gss, gsr, hss, hsr, rs_, rr, sss, ssrr, as2, ar2, fss, fsr,
):
    z = lax.axis_index("ep_0")
    x = lax.axis_index("ep_1")
    c = lax.axis_index("ep_2")
    t = lax.axis_index("tp")
    e = (z * NX + x) * NC + c
    m = x * NC + c
    zd = [lax.rem(z + d, NZ) for d in range(NZ)]
    xd = [lax.rem(x + d, NX) for d in range(NX)]
    td = [lax.rem(t + d, NT) for d in range(NT)]
    cd = [c, 1 - c]
    mates = [(2, 0), (2, 1), (1, 0), (3, 0), (1, 1), (3, 1), (0, 1)]
    far_first = [4, 3, 5, 2, 6, 1, 7]
    near_first = far_first[::-1]

    def remote(src, dst, ssem, rsem, dev):
        return pltpu.make_async_remote_copy(
            src_ref=src, dst_ref=dst, send_sem=ssem, recv_sem=rsem,
            device_id=dev, device_id_type=MESH,
        )

    pending = []

    def send(src, dst, ssem, rsem, dev):
        cp = remote(src, dst, ssem, rsem, dev)
        cp.start()
        pending.append(cp)

    def arrived(dst, ssem, rsem):
        remote(dst, dst, ssem, rsem, (z, x, 1 - c, t)).wait_recv()

    loads = []

    def load(src, dst):
        cp = pltpu.make_async_copy(src, dst, lsem.at[len(loads)])
        cp.start()
        loads.append(cp)
        return cp

    ld_q = load(wq_h, qb.at[z])
    ld_tok = [load(tok_h, tok), load(ag_h, ag)]
    ld_o = load(wo_h, ob.at[z, x, c])
    ld_kv = [
        load(wk_h, kvb.at[z, :, pl.ds(0, 128)]),
        load(wv_h, kvb.at[z, :, pl.ds(128, 128)]),
    ]
    barrier = pltpu.get_barrier_semaphore()
    first = [(zd[d], x, c, t) for d in range(1, NZ)]
    first += [(z, xd[dx], cd[dc], t) for dx, dc in mates]
    first += [(z, x, c, td[d]) for d in range(1, NT)]
    for dev in first:
        pl.semaphore_signal(barrier, inc=1, device_id=dev, device_id_type=MESH)

    pl.semaphore_wait(barrier, len(first))

    mine_o = ob.at[z, x, c]

    def q_around(*steps):
        for d in steps:
            send(qb.at[z], qb.at[z], qzs.at[d], qzr.at[d], (zd[d], x, c, t))

    def o_around(*steps):
        for d in steps:
            send(mine_o, mine_o, ozs.at[d], ozr.at[d], (zd[d], x, c, t))

    ld_q.wait()
    q_around(*far_first)

    ld_o.wait()
    for cp in ld_tok:
        cp.wait()
    data = tok[...].astype(F32)
    factor = lax.rsqrt(jnp.mean(data * data, axis=-1, keepdims=True) + EPS)
    gain = ag[...].astype(F32)
    blocks = []
    for i in range(NZ):
        halves = []
        for k in (2 * i, 2 * i + 1):
            halves.append(data[:, HD * k : HD * k + HD] * factor * gain[k : k + 1, :])
        blocks.append(jnp.concatenate(halves, axis=1).astype(BF16).astype(F32))
    chunk = iota((SEQ, 256), 1) >> 5
    for g in range(8):
        own = blocks[g]
        for k in range(1, 8):
            j = (g + k) % 8
            own = jnp.where(chunk == j, pltpu.roll(blocks[j], 32 * k, 1), own)
        tkb[g] = own.astype(BF16)
    for dx, dc in mates:
        g = xd[dx] * NC + cd[dc]
        send(tkb.at[g], tk.at[m], tks.at[dx, dc], tkr.at[dx, dc], (z, xd[dx], cd[dc], t))
    tk[m] = tkb[m]

    def o_along(r):
        src = ob.at[zd[r], x, c]
        for i in (2, 1, 3):
            send(src, src, oxs.at[r, i], oxr.at[r, i], (z, xd[i], c, t))

    def o_forward(r):
        src = ob.at[zd[r], x, c]
        arrived(src, ozs.at[NZ - r], ozr.at[NZ - r])
        o_along(r)

    def o_across(r):
        for i in (1, 3, 2):
            arrived(ob.at[zd[r], xd[i], c], oxs.at[r, NX - i], oxr.at[r, NX - i])
        src = ob.at[zd[r], :, c]
        send(src, src, ods.at[r], odr.at[r], (z, x, 1 - c, t))

    def o_last():
        for r in range(NZ):
            arrived(ob.at[zd[r], :, 1 - c], ods.at[r], odr.at[r])

    o_along(0)
    ld_er = load(er_h, er)
    ld_att = [load(off_h, off), load(hg_h, hg), load(lens_h, lens)]
    kv_loads = []
    for i in range(4):
        ds = pl.ds(4 * i, 4)
        kv_loads.append(pltpu.make_async_copy(pk_h.at[ds], kb.at[ds], kvsem.at[i]))
        kv_loads.append(pltpu.make_async_copy(pv_h.at[ds], vb.at[ds], kvsem.at[4 + i]))
    for cp in kv_loads:
        cp.start()
    ld_ffn = [load(fg_h, fg), load(rt_h, rt)]
    ld_sh = [
        load(sg_h, sgu.at[:, pl.ds(0, 128)]),
        load(su_h, sgu.at[:, pl.ds(128, 128)]),
        load(sd_h, sd),
    ]
    mine = pl.ds(pl.multiple_of(t * 512, 512), 512)
    ld_own = load(tok_h.at[:, mine], tokb)
    ld_ex = [
        load(eg_h.at[0, mine, :], wgu.at[t, :, pl.ds(0, 128)]),
        load(eu_h.at[0, mine, :], wgu.at[t, :, pl.ds(128, 128)]),
        load(ed_h.at[0, :, mine], wd.at[t]),
    ]

    def recut_down(peers):
        for d in peers:
            theirs = pl.ds(pl.multiple_of(td[d] * 512, 512), 512)
            send(ed_h.at[0, :, theirs], wd.at[t], ys.at[2, d], yr.at[2, d], (z, x, c, td[d]))

    for d in (1, 3, 2):
        p = td[d]
        dev = (z, x, c, p)
        theirs = pl.ds(pl.multiple_of(p * 512, 512), 512)
        for k, src in enumerate((eg_h, eu_h)):
            half = pl.ds(128 * k, 128)
            send(src.at[0, theirs, :], wgu.at[t, :, half], ys.at[k, d], yr.at[k, d], dev)
    recut_down((1, 3))

    ld_er.wait()
    rows = NE * 12
    chosen = iota((NE, SEQ), 0) == er[0:1, :]
    for k in range(1, 6):
        chosen = chosen | (iota((NE, SEQ), 0) == er[k : k + 1, :])
    hot_t = ones_where(chosen)
    before = ones_where(iota((SEQ, SEQ), 0) < iota((SEQ, SEQ), 1))
    code_t = jnp.where(chosen, dot(hot_t, before) + 1.0, 0.0).astype(BF16)
    repeat = ones_where((iota((SEQ, 64), 1) & 15) == iota((SEQ, 64), 0))
    eye = ones_where(iota((SEQ, SEQ), 0) == iota((SEQ, SEQ), 1))
    code4_t = dot(code_t, repeat).astype(BF16)
    code = dot_nt(eye, code_t)
    q0 = iota((rows, 64), 0) >> 2
    j0 = iota((rows, 64), 0) & 3
    e0 = (q0 * 171) >> 9
    c0 = iota((rows, 64), 1)
    spread = ones_where(e0 == c0)
    slot_of = dot(spread, code4_t)
    want = (q0 - 3 * e0 + 1).astype(F32)
    dispatch = ones_where((slot_of == want) & (j0 == (c0 >> 4)))

    o_around(1, 7, 4, 3, 5, 2, 6)
    for n, pick, back in ((72, pick72, back72), (48, pick48, back48)):
        for j in range(4):
            p, q = iota((n, 4 * n), 0), iota((n, 4 * n), 1)
            pick[n * j : n * j + n, :] = jnp.where(q == 4 * p + j, 1.0, 0.0)
        p, q = iota((4 * n, 4 * n), 1), iota((4 * n, 4 * n), 0)
        j = (p >= n).astype(jnp.int32) + (p >= 2 * n) + (p >= 3 * n)
        back[...] = ones_where(q == 4 * (p - n * j) + j)
    for b in range(SEQ):
        if b % 4 == 0:
            kv_loads[2 * (b // 4)].wait()
        kt[b] = kb[b].T

    for dx, dc in mates:
        src = tk.at[lax.rem(x + NX - dx, NX) * NC + cd[dc]]
        arrived(src, tks.at[dx, dc], tkr.at[dx, dc])
    for d in near_first:
        arrived(qb.at[lax.rem(z + NZ - d, NZ)], qzs.at[d], qzr.at[d])
    rows_in = tk[...].reshape(8 * SEQ, 256)
    part[...] = dot(rows_in, qb[...].reshape(256, 256)).reshape(8, SEQ, 256)
    for dx, dc in mates:
        g = xd[dx] * NC + cd[dc]
        send(part.at[g], qp.at[m], qps.at[dx, dc], qpr.at[dx, dc], (z, xd[dx], cd[dc], t))
    qp[m] = part[m]
    for r in (7, 1, 6, 2, 5, 3, 4):
        o_forward(r)
    for dx, dc in mates:
        src = qp.at[lax.rem(x + NX - dx, NX) * NC + cd[dc]]
        arrived(src, qps.at[dx, dc], qpr.at[dx, dc])
    total = qp[0]
    for i in range(1, 8):
        total = total + qp[i]
    queries = total.astype(BF16).astype(F32)

    for h in range(2):
        qs[pl.ds(h, SEQ, stride=2), :] = queries[:, HD * h : HD * h + HD]
    for cp in ld_att:
        cp.wait()
    for b in range(SEQ):
        q = qs[2 * b : 2 * b + 2, :].astype(BF16)
        lg[2 * b : 2 * b + 2, :] = dot(q, kt[b]) * HD ** (-0.5) + off[b]
        lenb[2 * b : 2 * b + 2, :] = jnp.full((2, HD), lens[b], jnp.int32)
    for cp in ld_kv:
        cp.wait()
    for d in far_first:
        send(kvb.at[z], kvb.at[z], kzs.at[d], kzr.at[d], (zd[d], x, c, t))
    for r in (0, 7, 1, 6, 2):
        o_across(r)
    logits = lg[...]
    length = lenb[:, 0:1]
    usable = iota((2 * SEQ, POS), 1) < length
    tail = jnp.log(1.0 + jnp.exp(-jnp.abs(logits)))
    keep = jnp.where(usable, jnp.minimum(-logits, 0.0) - tail, 0.0)
    nb = POS // HD
    stacked = jnp.concatenate([keep[:, HD * i : HD * i + HD] for i in range(nb)], axis=0)
    k1 = stacked.astype(BF16)
    left = stacked - k1.astype(F32)
    k2 = left.astype(BF16)
    k3 = (left - k2.astype(F32)).astype(BF16)
    later = ones_where(iota((HD, HD), 0) > iota((HD, HD), 1))
    inner = dot(k1, later) + dot(k2, later) + dot(k3, later)
    carry = jnp.zeros((2 * SEQ, 1), F32)
    after = [None] * nb
    n2 = 2 * SEQ
    for i in range(nb - 1, -1, -1):
        after[i] = inner[n2 * i : n2 * i + n2] + carry
        carry = carry + jnp.sum(stacked[n2 * i : n2 * i + n2], axis=-1, keepdims=True)
    after = jnp.concatenate(after, axis=1)
    sticks = jnp.where(usable, jnp.exp(jnp.minimum(logits, 0.0) - tail + after), 0.0)
    lg[...] = sticks
    for b in range(SEQ):
        if b % 4 == 0:
            kv_loads[2 * (b // 4) + 1].wait()
        got = dot(lg[2 * b : 2 * b + 2, :].astype(BF16), vb[b])
        ho[b : b + 1, 0:HD] = got[0:1, :]
        ho[b : b + 1, HD : 2 * HD] = got[1:2, :]
    for r in (5, 3, 4):
        o_across(r)
    heads_out = ho[...]
    scaled = jnp.concatenate(
        [heads_out[:, HD * i : HD * i + HD] * hg[i : i + 1, :].astype(F32) for i in range(2)],
        axis=1,
    ).astype(BF16)
    sq[t] = jnp.broadcast_to(jnp.sum(heads_out * heads_out, axis=-1, keepdims=True), (SEQ, HD))
    o_last()
    for i in range(NT):
        halves = [dot_nt(scaled, ob[zi].reshape(256, 256)) for zi in (2 * i, 2 * i + 1)]
        pcs[i] = jnp.concatenate(halves, axis=1).astype(BF16)

    for d in (2, 1, 3):
        dev = (z, x, c, td[d])
        send(sq.at[t], sq.at[t], cs.at[0, d], cr.at[0, d], dev)
        send(pcs.at[td[d]], pc.at[t], cs.at[1, d], cr.at[1, d], dev)
    pc[t] = pcs[t]
    for d in (1, 3, 2):
        src = td[NT - d]
        for k, buf in enumerate((sq, pc)):
            arrived(buf.at[src], cs.at[k, d], cr.at[k, d])
    head_total = pc[0].astype(F32)
    square = sq[0]
    for i in range(1, NT):
        head_total = head_total + pc[i].astype(F32)
        square = square + sq[i]
    attention = head_total * lax.rsqrt(square[:, 0:1] / 1024.0 + EPS)
    ld_own.wait()
    residual = (tokb[...].astype(F32) + attention).astype(BF16)
    res[t] = residual
    for d in (2, 1, 3):
        send(res.at[t], res.at[t], as2.at[d], ar2.at[d], (z, x, c, td[d]))

    block = jnp.concatenate([residual[:, HD * j : HD * j + HD] for j in range(4)], axis=0)
    sbuf[...] = dot(dispatch, block).astype(BF16).reshape(3 * NE, 4, HD)
    order = (3, 4, 5, 2, 6, 7, 0, 1)
    part_rows = (72, 48, 72)
    first_row = (0, 72, 120)

    def three(i):
        return pl.ds(3 * i, 3)

    def part_of(r):
        return (0, 0, 0, 1, 1, 2, 2, 2)[order.index(r)]

    def around(r):
        return [(0, 0), *mates] if r else mates

    for r in (7, 1, 0, 4, 5, 3, 6, 2):
        d = (NZ - r) % NZ
        to = three(8 * order.index(r) + m)
        for dx, dc in around(r):
            p = (zd[d] * NX + xd[dx]) * NC + cd[dc]
            dev = (zd[d], xd[dx], cd[dc], t)
            remote(sbuf.at[three(p)], rbuf.at[to], as_.at[part_of(r)], ar.at[part_of(r)], dev).start()
    rbuf[three(8 * order.index(0) + m)] = sbuf[three(e)]

    recut_down((2,))

    for cp in ld_ffn:
        cp.wait()
    gain = fg[...].astype(F32)
    own_gain = []
    for j in range(4):
        row = gain[j : j + 1, :]
        for i in range(1, NT):
            row = jnp.where(t == i, gain[4 * i + j : 4 * i + j + 1, :], row)
        own_gain.append(row)
    own_gain = jnp.concatenate(own_gain, axis=1)

    gs, gr, hs = (gs0, gs1, gs2), (gr0, gr1, gr2), (hs0, hs1, hs2)

    def start_part(k):
        n, at = part_rows[k], first_row[k]
        pick = pick48 if n == 48 else pick72
        remote_rows = n if k < 2 else n - 3
        both = remote(
            sbuf.at[pl.ds(0, remote_rows)], rbuf.at[pl.ds(0, remote_rows)], as_.at[k], ar.at[k],
            (z, x, 1 - c, t),
        )
        both.wait_recv()
        came = dot(pick[...].astype(BF16), rbuf[at : at + n].reshape(4 * n, HD))
        raw = jnp.concatenate([came[n * j : n * j + n] for j in range(4)], axis=1)
        rows_of = (raw * own_gain).astype(BF16)
        for d in (2, 1, 3):
            gs[k][d] = dot(rows_of, wgu[td[d]]).astype(BF16)
        for d in (2, 1, 3):
            send(gs[k].at[d], gr[k].at[d], gss.at[k, d], gsr.at[k, d], (z, x, c, td[d]))
        gate_up = dot(rows_of, wgu[t])
        square = jnp.sum(raw * raw, axis=-1, keepdims=True)
        square = jnp.concatenate([square, jnp.zeros((HD - n, 1), F32)], axis=0)
        fs[k, 0] = jnp.broadcast_to(square, (HD, HD)).T[0:8, :]
        for d in (2, 1, 3):
            send(fs.at[k, 0], fs.at[k, d], fss.at[k, d], fsr.at[k, d], (z, x, c, td[d]))
        return gate_up, both

    def middle_part(k, gate_up):
        for d in (2, 1, 3):
            arrived(gr[k].at[d], gss.at[k, d], gsr.at[k, d])
            gate_up = gate_up + gr[k][d].astype(F32)
            arrived(fs.at[k, d], fss.at[k, d], fsr.at[k, d])
        square = fs[k, 0] + fs[k, 1] + fs[k, 2] + fs[k, 3]
        square = jnp.broadcast_to(square[0:1, :], (HD, HD)).T[0 : part_rows[k], 0:1]
        gate_up = gate_up * lax.rsqrt(square / 2048.0 + EPS)
        gate = gate_up[:, 0:HD]
        hidden = gate / (1.0 + jnp.exp(-gate)) * gate_up[:, HD : 2 * HD]
        hs[k][t] = hidden.astype(BF16)
        own = hs[k].at[t]
        for d in (2, 1, 3):
            send(own, own, hss.at[k, d], hsr.at[k, d], (z, x, c, td[d]))

    def end_part(k):
        n, at = part_rows[k], first_row[k]
        back = back48 if n == 48 else back72
        for d in (2, 1, 3):
            arrived(hs[k].at[td[NT - d]], hss.at[k, d], hsr.at[k, d])
        out = dot(hs[k][0], wd[0])
        for i in range(1, NT):
            out = out + dot(hs[k][i], wd[i])
        out = jnp.concatenate([out[:, HD * j : HD * j + HD] for j in range(4)], axis=0)
        obuf[at : at + n] = dot(back[...], out.astype(BF16)).astype(BF16).reshape(n, 4, HD)
        for r in ((4, 5, 3), (6, 2), (7, 1, 0))[k]:
            for dx, dc in around(r):
                p = 8 * order.index(r) + xd[dx] * NC + cd[dc]
                dev = (zd[r], xd[dx], cd[dc], t)
                remote(obuf.at[three(p)], cbuf.at[three(e)], rs_, rr, dev).start()

    for cp in ld_ex:
        cp.wait()
    for d in (1, 3, 2):
        src = td[NT - d]
        for k in range(2):
            arrived(wgu.at[src, :, pl.ds(128 * k, 128)], ys.at[k, d], yr.at[k, d])
    gate_up2, sent2 = start_part(2)

    for d in (1, 3, 2):
        arrived(res.at[td[NT - d]], as2.at[d], ar2.at[d])
    data = jnp.concatenate([res[i] for i in range(NT)], axis=1).astype(F32)
    factor = lax.rsqrt(jnp.mean(data * data, axis=-1, keepdims=True) + EPS)
    pieces = [data[:, HD * i : HD * i + HD] * factor * gain[i : i + 1, :] for i in range(16)]
    normed_ffn = jnp.concatenate(pieces, axis=1).astype(BF16)
    for cp in ld_sh:
        cp.wait()
    both = dot(normed_ffn, sgu[...])
    gate = both[:, 0:HD]
    shared_hidden = (gate / (1.0 + jnp.exp(-gate)) * both[:, HD : 2 * HD]).astype(BF16)
    shared_part = dot(shared_hidden, sd[...]).astype(BF16)
    for i in range(NT):
        ssb[i] = shared_part[:, 512 * i : 512 * i + 512]
    for d in (2, 1, 3):
        p = td[d]
        send(ssb.at[p], ssr.at[t], sss.at[d], ssrr.at[d], (z, x, c, p))
    ssr[t] = ssb[t]
    logit = dot_nt(normed_ffn, rt[...])
    prob = 1.0 / (1.0 + jnp.exp(-logit))
    picked = jnp.where(code > 0.5, prob, 0.0)
    weight = SCALE * picked / jnp.sum(picked, axis=-1, keepdims=True)
    weight4 = jnp.concatenate([weight] * 4, axis=0)
    w_hi = weight4.astype(BF16)
    w_lo = (weight4 - w_hi.astype(F32)).astype(BF16)
    code4 = jnp.concatenate([code] * 4, axis=0).astype(BF16)
    q1 = iota((64, rows), 1) >> 2
    j1 = iota((64, rows), 1) & 3
    e1 = (q1 * 171) >> 9
    c1 = iota((64, rows), 0)
    spread_t = ones_where(e1 == c1)
    slot_to = dot(code4, spread_t)
    fits = (slot_to == (q1 - 3 * e1 + 1).astype(F32)) & (j1 == (c1 >> 4))
    comb_hi = jnp.where(fits, dot(w_hi, spread_t), 0.0).astype(BF16)
    comb_lo = jnp.where(fits, dot(w_lo, spread_t), 0.0).astype(BF16)

    for d in near_first:
        arrived(kvb.at[lax.rem(z + NZ - d, NZ)], kzs.at[d], kzr.at[d])
    kvpart[...] = dot(rows_in, kvb[...].reshape(256, 256)).astype(BF16).reshape(8, SEQ, 256)
    for dx, dc in mates:
        g = xd[dx] * NC + cd[dc]
        send(kvpart.at[g], kvp.at[m], kps.at[dx, dc], kpr.at[dx, dc], (z, xd[dx], cd[dc], t))
    kvp[m] = kvpart[m]
    gate_up0, sent0 = start_part(0)
    gate_up1, sent1 = start_part(1)
    middle_part(2, gate_up2)
    middle_part(0, gate_up0)
    middle_part(1, gate_up1)
    for d in (1, 3, 2):
        arrived(wd.at[td[NT - d]], ys.at[2, d], yr.at[2, d])
    end_part(0)
    end_part(2)
    end_part(1)
    cbuf[three(e)] = obuf[three(8 * order.index(0) + m)]
    shared_total = jnp.zeros((SEQ, 512), F32)
    for d in (2, 1, 3):
        arrived(ssr.at[td[NT - d]], sss.at[d], ssrr.at[d])
    for i in range(NT):
        shared_total = shared_total + ssr[i].astype(F32)
    base = res[t].astype(F32) + shared_total
    for dx, dc in mates:
        src = kvp.at[lax.rem(x + NX - dx, NX) * NC + cd[dc]]
        arrived(src, kps.at[dx, dc], kpr.at[dx, dc])
    new = kvp[0].astype(F32)
    for i in range(1, 8):
        new = new + kvp[i].astype(F32)
    fk_o[...] = new[:, 0:HD].astype(BF16)
    fv_o[...] = new[:, HD : 2 * HD].astype(BF16)
    back = remote(
        obuf.at[pl.ds(0, 3 * NE - 3)], cbuf.at[pl.ds(0, 3 * NE - 3)], rs_, rr, (z, x, 1 - c, t)
    )
    back.wait_recv()
    came = cbuf[...].reshape(rows, HD)
    routed = dot(comb_hi, came) + dot(comb_lo, came)
    for j in range(4):
        mixed_o[:, HD * j : HD * j + HD] = (
            base[:, HD * j : HD * j + HD] + routed[SEQ * j : SEQ * j + SEQ]
        ).astype(BF16)
    for cp in [*pending, sent0, sent1, sent2, back]:
        cp.wait_send()


def hand_over(a, b, c, a_o, b_o, c_o, sem):
    moves = []
    for i, (src, dst) in enumerate(((a, a_o), (b, b_o), (c, c_o))):
        moves.append(pltpu.make_async_copy(src, dst, sem.at[i]))
        moves[i].start()
    for cp in moves:
        cp.wait()


def body(
    tokens, attn_gain, query_weight, key_weight, value_weight, out_weight, head_gain,
    past_keys, past_values, break_offset, cache_lengths, ffn_gain, router_weight,
    expert_routes, expert_gate, expert_up, expert_down, shared_gate, shared_up, shared_down,
):
    hbm = pl.BlockSpec(memory_space=pl.ANY)
    v, dma = pltpu.VMEM, pltpu.SemaphoreType.DMA
    outs = pl.pallas_call(
        kernel,
        out_shape=(v((SEQ, 512), BF16), v((SEQ, HD), BF16), v((SEQ, HD), BF16)),
        in_specs=[hbm] * 20,
        out_specs=(pl.BlockSpec(memory_space=pltpu.VMEM),) * 3,
        scratch_shapes=[
            v((SEQ, 2048), BF16), v((16, HD), BF16), v((2, HD), BF16), v((16, HD), BF16),
            v((64, 2048), BF16), v((6, SEQ), jnp.int32), v((SEQ, 2, POS), F32),
            v((SEQ, POS, HD), BF16), v((SEQ, HD, POS), BF16), v((SEQ, POS, HD), BF16),
            v((NZ, 32, 256), BF16), v((NZ, 32, 256), BF16), v((NZ, NX, NC, 32, 256), BF16),
            v((NT, 512, 256), BF16), v((NT, 128, 512), BF16),
            v((2048, 256), BF16), v((128, 2048), BF16),
            v((8, SEQ, 256), BF16), v((8, SEQ, 256), BF16),
            v((8, SEQ, 256), F32), v((8, SEQ, 256), F32),
            v((8, SEQ, 256), BF16), v((8, SEQ, 256), BF16),
            v((2 * SEQ, HD), F32), v((2 * SEQ, POS), F32), v((2 * SEQ, HD), jnp.int32),
            v((SEQ, 256), F32), v((NT, SEQ, 512), BF16), v((NT, SEQ, 512), BF16),
            v((NT, SEQ, HD), F32), v((3, NT, 8, HD), F32), v((NT, SEQ, 512), BF16),
            v((3 * NE, 4, HD), BF16), v((3 * NE, 4, HD), BF16),
            *[v((NT, n, 256), BF16) for _ in range(2) for n in (72, 48, 72)],
            *[v((NT, n, HD), BF16) for n in (72, 48, 72)],
            v((288, 288), F32), v((288, 288), BF16), v((192, 192), F32), v((192, 192), BF16),

            v((3 * NE, 4, HD), BF16), v((3 * NE, 4, HD), BF16),
            v((NT, SEQ, 512), BF16), v((NT, SEQ, 512), BF16),
            pltpu.SMEM((SEQ,), jnp.int32), v((SEQ, 512), BF16), dma((32,)), dma((8,)),
            *[dma((NZ,)) for _ in range(6)],
            dma((NZ, NX)), dma((NZ, NX)), dma((NZ,)), dma((NZ,)),
            *[dma((NX, NC)) for _ in range(6)],
            dma((3, 4)), dma((3, 4)), dma((2, 4)), dma((2, 4)), dma((3,)), dma((3,)),
            dma((3, 4)), dma((3, 4)), dma((3, 4)), dma((3, 4)), dma, dma, dma((4,)), dma((4,)),
            dma((4,)), dma((4,)), dma((3, 4)), dma((3, 4)),
        ],
        compiler_params=pltpu.CompilerParams(
            collective_id=0, has_side_effects=True, vmem_limit_bytes=60 * 1024 * 1024
        ),
    )(
        tokens, attn_gain.reshape(16, HD), query_weight, key_weight, value_weight, out_weight,
        head_gain.reshape(2, HD), past_keys.reshape(SEQ, POS, HD),
        past_values.reshape(SEQ, POS, HD), break_offset, cache_lengths,
        ffn_gain.reshape(16, HD), router_weight.T, expert_routes.T, expert_gate, expert_up,
        expert_down, shared_gate, shared_up, shared_down,
    )
    return pl.pallas_call(
        hand_over,
        out_shape=tuple(jax.ShapeDtypeStruct(o.shape, o.dtype) for o in outs),
        in_specs=[pl.BlockSpec(memory_space=pltpu.VMEM)] * 3,
        out_specs=(hbm,) * 3,
        scratch_shapes=[dma((3,))],
    )(*[pltpu.with_memory_space_constraint(o, pltpu.VMEM) for o in outs])


def solution(mesh):
    torus = Mesh(mesh.devices.reshape(NZ, NX, NC, NT), (*EP, "tp"))
    return jax.shard_map(
        body,
        mesh=torus,
        in_specs=(
            P(EP, None),
            P(),
            P(EP, "tp"),
            P(EP, "tp"),
            P(EP, "tp"),
            P(EP, "tp"),
            P("tp"),
            P(EP, None, "tp", None),
            P(EP, None, "tp", None),
            P(EP, "tp", None),
            P(EP),
            P(),
            P(),
            P(EP, None),
            P(EP, None, "tp"),
            P(EP, None, "tp"),
            P(EP, "tp", None),
            P(None, "tp"),
            P(None, "tp"),
            P("tp", None),
        ),
        out_specs=(P(EP, "tp"), P(EP, "tp"), P(EP, "tp")),
        check_vma=False,
    )
```

```python
import jax
import jax.numpy as jnp
from jax import lax
from jax.experimental import pallas as pl
from jax.experimental.pallas import tpu as pltpu
from jax.sharding import Mesh
from jax.sharding import PartitionSpec as P

MESH = pl.DeviceIdType.MESH
EP = ("ep_0", "ep_1", "ep_2")
NZ, NX, NC, NT = 8, 4, 2, 4
NE = NZ * NX * NC
SEQ = 16
POS = 1024
HD = 128
EPS = 1e-06
SCALE = 2.5
F32 = jnp.float32
BF16 = jnp.bfloat16


def dot(a, b):
    return jnp.dot(a, b, preferred_element_type=F32)


def dot_nt(a, b):
    return lax.dot_general(a, b, (((1,), (1,)), ((), ())), preferred_element_type=F32)


def iota(shape, dim):
    return lax.broadcasted_iota(jnp.int32, shape, dim)


def ones_where(cond):
    return jnp.where(cond, 1.0, 0.0).astype(BF16)


def kernel(
    tok_h, ag_h, wq_h, wk_h, wv_h, wo_h, hg_h, pk_h, pv_h, off_h, lens_h, fg_h, rt_h, er_h,
    eg_h, eu_h, ed_h, sg_h, su_h, sd_h,
    mixed_o, fk_o, fv_o,
    tok, ag, hg, fg, rt, er, off, kb, kt, vb, qb, kvb, ob, wgu, wd, sgu, sd,
    tkb, tk, part, qp, kvpart, kvp,
    qs, lg, lenb, ho, pcs, pc, sq, fs, res, sbuf, rbuf, gs0, gs1, gs2, gr0, gr1, gr2, hs0, hs1, hs2,
    pick72, back72, pick48, back48, obuf, cbuf, ssb, ssr,
    lens, tokb, lsem, kvsem,
    qzs, qzr, kzs, kzr, ozs, ozr, oxs, oxr, ods, odr, tks, tkr, qps, qpr, kps, kpr,
    ys, yr, cs, cr, as_, ar, gss, gsr, hss, hsr, rs_, rr, sss, ssrr, as2, ar2, fss, fsr,
):
    z = lax.axis_index("ep_0")
    x = lax.axis_index("ep_1")
    c = lax.axis_index("ep_2")
    t = lax.axis_index("tp")
    e = (z * NX + x) * NC + c
    m = x * NC + c
    zd = [lax.rem(z + d, NZ) for d in range(NZ)]
    xd = [lax.rem(x + d, NX) for d in range(NX)]
    td = [lax.rem(t + d, NT) for d in range(NT)]
    cd = [c, 1 - c]
    mates = [(2, 0), (2, 1), (1, 0), (3, 0), (1, 1), (3, 1), (0, 1)]
    far_first = [4, 3, 5, 2, 6, 1, 7]
    near_first = far_first[::-1]

    def remote(src, dst, ssem, rsem, dev):
        return pltpu.make_async_remote_copy(
            src_ref=src, dst_ref=dst, send_sem=ssem, recv_sem=rsem,
            device_id=dev, device_id_type=MESH,
        )

    pending = []

    def send(src, dst, ssem, rsem, dev):
        cp = remote(src, dst, ssem, rsem, dev)
        cp.start()
        pending.append(cp)

    def arrived(dst, ssem, rsem):
        remote(dst, dst, ssem, rsem, (z, x, 1 - c, t)).wait_recv()

    loads = []

    def load(src, dst):
        cp = pltpu.make_async_copy(src, dst, lsem.at[len(loads)])
        cp.start()
        loads.append(cp)
        return cp

    ld_q = load(wq_h, qb.at[z])
    ld_tok = [load(tok_h, tok), load(ag_h, ag)]
    ld_o = load(wo_h, ob.at[z, x, c])
    ld_kv = [
        load(wk_h, kvb.at[z, :, pl.ds(0, 128)]),
        load(wv_h, kvb.at[z, :, pl.ds(128, 128)]),
    ]
    barrier = pltpu.get_barrier_semaphore()
    first = [(zd[d], x, c, t) for d in range(1, NZ)]
    first += [(z, xd[dx], cd[dc], t) for dx, dc in mates]
    first += [(z, x, c, td[d]) for d in range(1, NT)]
    for dev in first:
        pl.semaphore_signal(barrier, inc=1, device_id=dev, device_id_type=MESH)

    pl.semaphore_wait(barrier, len(first))

    mine_o = ob.at[z, x, c]

    def q_around(*steps):
        for d in steps:
            send(qb.at[z], qb.at[z], qzs.at[d], qzr.at[d], (zd[d], x, c, t))

    def o_around(*steps):
        for d in steps:
            send(mine_o, mine_o, ozs.at[d], ozr.at[d], (zd[d], x, c, t))

    ld_o.wait()
    o_around(*(1, 7, 2, 6))
    ld_q.wait()
    q_around(*far_first)

    for cp in ld_tok:
        cp.wait()
    data = tok[...].astype(F32)
    factor = lax.rsqrt(jnp.mean(data * data, axis=-1, keepdims=True) + EPS)
    gain = ag[...].astype(F32)
    blocks = []
    for i in range(NZ):
        halves = []
        for k in (2 * i, 2 * i + 1):
            halves.append(data[:, HD * k : HD * k + HD] * factor * gain[k : k + 1, :])
        blocks.append(jnp.concatenate(halves, axis=1).astype(BF16).astype(F32))
    chunk = iota((SEQ, 256), 1) >> 5
    for g in range(8):
        own = blocks[g]
        for k in range(1, 8):
            j = (g + k) % 8
            own = jnp.where(chunk == j, pltpu.roll(blocks[j], 32 * k, 1), own)
        tkb[g] = own.astype(BF16)
    for dx, dc in mates:
        g = xd[dx] * NC + cd[dc]
        send(tkb.at[g], tk.at[m], tks.at[dx, dc], tkr.at[dx, dc], (z, xd[dx], cd[dc], t))
    tk[m] = tkb[m]

    def o_along(r):
        src = ob.at[zd[r], x, c]
        for i in (2, 1, 3):
            send(src, src, oxs.at[r, i], oxr.at[r, i], (z, xd[i], c, t))

    def o_forward(r):
        src = ob.at[zd[r], x, c]
        arrived(src, ozs.at[NZ - r], ozr.at[NZ - r])
        o_along(r)

    def o_across(r):
        for i in (1, 3, 2):
            arrived(ob.at[zd[r], xd[i], c], oxs.at[r, NX - i], oxr.at[r, NX - i])
        src = ob.at[zd[r], :, c]
        send(src, src, ods.at[r], odr.at[r], (z, x, 1 - c, t))

    def o_last():
        for r in range(NZ):
            arrived(ob.at[zd[r], :, 1 - c], ods.at[r], odr.at[r])

    o_along(0)
    ld_er = load(er_h, er)
    ld_att = [load(off_h, off), load(hg_h, hg), load(lens_h, lens)]
    kv_loads = []
    for i in range(4):
        ds = pl.ds(4 * i, 4)
        kv_loads.append(pltpu.make_async_copy(pk_h.at[ds], kb.at[ds], kvsem.at[i]))
        kv_loads.append(pltpu.make_async_copy(pv_h.at[ds], vb.at[ds], kvsem.at[4 + i]))
    for cp in kv_loads:
        cp.start()
    ld_ffn = [load(fg_h, fg), load(rt_h, rt)]
    ld_sh = [
        load(sg_h, sgu.at[:, pl.ds(0, 128)]),
        load(su_h, sgu.at[:, pl.ds(128, 128)]),
        load(sd_h, sd),
    ]
    mine = pl.ds(pl.multiple_of(t * 512, 512), 512)
    ld_own = load(tok_h.at[:, mine], tokb)
    ld_ex = [
        load(eg_h.at[0, mine, :], wgu.at[t, :, pl.ds(0, 128)]),
        load(eu_h.at[0, mine, :], wgu.at[t, :, pl.ds(128, 128)]),
        load(ed_h.at[0, :, mine], wd.at[t]),
    ]

    def recut_down(peers):
        for d in peers:
            theirs = pl.ds(pl.multiple_of(td[d] * 512, 512), 512)
            send(ed_h.at[0, :, theirs], wd.at[t], ys.at[2, d], yr.at[2, d], (z, x, c, td[d]))

    for d in (1, 3, 2):
        p = td[d]
        dev = (z, x, c, p)
        theirs = pl.ds(pl.multiple_of(p * 512, 512), 512)
        for k, src in enumerate((eg_h, eu_h)):
            half = pl.ds(128 * k, 128)
            send(src.at[0, theirs, :], wgu.at[t, :, half], ys.at[k, d], yr.at[k, d], dev)
    recut_down((1, 3))

    ld_er.wait()
    rows = NE * 12
    chosen = iota((NE, SEQ), 0) == er[0:1, :]
    for k in range(1, 6):
        chosen = chosen | (iota((NE, SEQ), 0) == er[k : k + 1, :])
    hot_t = ones_where(chosen)
    before = ones_where(iota((SEQ, SEQ), 0) < iota((SEQ, SEQ), 1))
    code_t = jnp.where(chosen, dot(hot_t, before) + 1.0, 0.0).astype(BF16)
    repeat = ones_where((iota((SEQ, 64), 1) & 15) == iota((SEQ, 64), 0))
    eye = ones_where(iota((SEQ, SEQ), 0) == iota((SEQ, SEQ), 1))
    code4_t = dot(code_t, repeat).astype(BF16)
    code = dot_nt(eye, code_t)
    q0 = iota((rows, 64), 0) >> 2
    j0 = iota((rows, 64), 0) & 3
    e0 = (q0 * 171) >> 9
    c0 = iota((rows, 64), 1)
    spread = ones_where(e0 == c0)
    slot_of = dot(spread, code4_t)
    want = (q0 - 3 * e0 + 1).astype(F32)
    dispatch = ones_where((slot_of == want) & (j0 == (c0 >> 4)))

    o_around(*(4, 3, 5))
    for n, pick, back in ((72, pick72, back72), (48, pick48, back48)):
        for j in range(4):
            p, q = iota((n, 4 * n), 0), iota((n, 4 * n), 1)
            pick[n * j : n * j + n, :] = jnp.where(q == 4 * p + j, 1.0, 0.0)
        p, q = iota((4 * n, 4 * n), 1), iota((4 * n, 4 * n), 0)
        j = (p >= n).astype(jnp.int32) + (p >= 2 * n) + (p >= 3 * n)
        back[...] = ones_where(q == 4 * (p - n * j) + j)
    for b in range(SEQ):
        if b % 4 == 0:
            kv_loads[2 * (b // 4)].wait()
        kt[b] = kb[b].T
    o_forward(7)
    o_forward(1)
    o_forward(6)
    o_forward(2)

    for dx, dc in mates:
        src = tk.at[lax.rem(x + NX - dx, NX) * NC + cd[dc]]
        arrived(src, tks.at[dx, dc], tkr.at[dx, dc])
    for d in near_first:
        arrived(qb.at[lax.rem(z + NZ - d, NZ)], qzs.at[d], qzr.at[d])
    rows_in = tk[...].reshape(8 * SEQ, 256)
    part[...] = dot(rows_in, qb[...].reshape(256, 256)).reshape(8, SEQ, 256)
    for dx, dc in mates:
        g = xd[dx] * NC + cd[dc]
        send(part.at[g], qp.at[m], qps.at[dx, dc], qpr.at[dx, dc], (z, xd[dx], cd[dc], t))
    qp[m] = part[m]
    for r in (5, 3, 4):
        o_forward(r)
    for dx, dc in mates:
        src = qp.at[lax.rem(x + NX - dx, NX) * NC + cd[dc]]
        arrived(src, qps.at[dx, dc], qpr.at[dx, dc])
    total = qp[0]
    for i in range(1, 8):
        total = total + qp[i]
    queries = total.astype(BF16).astype(F32)

    for h in range(2):
        qs[pl.ds(h, SEQ, stride=2), :] = queries[:, HD * h : HD * h + HD]
    for cp in ld_att:
        cp.wait()
    for b in range(SEQ):
        q = qs[2 * b : 2 * b + 2, :].astype(BF16)
        lg[2 * b : 2 * b + 2, :] = dot(q, kt[b]) * HD ** (-0.5) + off[b]
        lenb[2 * b : 2 * b + 2, :] = jnp.full((2, HD), lens[b], jnp.int32)
    for cp in ld_kv:
        cp.wait()
    for d in far_first:
        send(kvb.at[z], kvb.at[z], kzs.at[d], kzr.at[d], (zd[d], x, c, t))
    for r in (0, 7, 1, 6, 2):
        o_across(r)
    logits = lg[...]
    length = lenb[:, 0:1]
    usable = iota((2 * SEQ, POS), 1) < length
    tail = jnp.log(1.0 + jnp.exp(-jnp.abs(logits)))
    keep = jnp.where(usable, jnp.minimum(-logits, 0.0) - tail, 0.0)
    nb = POS // HD
    stacked = jnp.concatenate([keep[:, HD * i : HD * i + HD] for i in range(nb)], axis=0)
    k1 = stacked.astype(BF16)
    left = stacked - k1.astype(F32)
    k2 = left.astype(BF16)
    k3 = (left - k2.astype(F32)).astype(BF16)
    later = ones_where(iota((HD, HD), 0) > iota((HD, HD), 1))
    inner = dot(k1, later) + dot(k2, later) + dot(k3, later)
    carry = jnp.zeros((2 * SEQ, 1), F32)
    after = [None] * nb
    n2 = 2 * SEQ
    for i in range(nb - 1, -1, -1):
        after[i] = inner[n2 * i : n2 * i + n2] + carry
        carry = carry + jnp.sum(stacked[n2 * i : n2 * i + n2], axis=-1, keepdims=True)
    after = jnp.concatenate(after, axis=1)
    sticks = jnp.where(usable, jnp.exp(jnp.minimum(logits, 0.0) - tail + after), 0.0)
    lg[...] = sticks
    for r in (5, 3, 4):
        o_across(r)
    for b in range(SEQ):
        if b % 4 == 0:
            kv_loads[2 * (b // 4) + 1].wait()
        got = dot(lg[2 * b : 2 * b + 2, :].astype(BF16), vb[b])
        ho[b : b + 1, 0:HD] = got[0:1, :]
        ho[b : b + 1, HD : 2 * HD] = got[1:2, :]
    heads_out = ho[...]
    scaled = jnp.concatenate(
        [heads_out[:, HD * i : HD * i + HD] * hg[i : i + 1, :].astype(F32) for i in range(2)],
        axis=1,
    ).astype(BF16)
    sq[t] = jnp.broadcast_to(jnp.sum(heads_out * heads_out, axis=-1, keepdims=True), (SEQ, HD))
    o_last()
    for i in range(NT):
        halves = [dot_nt(scaled, ob[zi].reshape(256, 256)) for zi in (2 * i, 2 * i + 1)]
        pcs[i] = jnp.concatenate(halves, axis=1).astype(BF16)

    for d in (2, 1, 3):
        dev = (z, x, c, td[d])
        send(sq.at[t], sq.at[t], cs.at[0, d], cr.at[0, d], dev)
        send(pcs.at[td[d]], pc.at[t], cs.at[1, d], cr.at[1, d], dev)
    pc[t] = pcs[t]
    for d in (1, 3, 2):
        src = td[NT - d]
        for k, buf in enumerate((sq, pc)):
            arrived(buf.at[src], cs.at[k, d], cr.at[k, d])
    head_total = pc[0].astype(F32)
    square = sq[0]
    for i in range(1, NT):
        head_total = head_total + pc[i].astype(F32)
        square = square + sq[i]
    attention = head_total * lax.rsqrt(square[:, 0:1] / 1024.0 + EPS)
    ld_own.wait()
    residual = (tokb[...].astype(F32) + attention).astype(BF16)
    res[t] = residual
    for d in (2, 1, 3):
        send(res.at[t], res.at[t], as2.at[d], ar2.at[d], (z, x, c, td[d]))

    block = jnp.concatenate([residual[:, HD * j : HD * j + HD] for j in range(4)], axis=0)
    sbuf[...] = dot(dispatch, block).astype(BF16).reshape(3 * NE, 4, HD)
    order = (3, 4, 5, 2, 6, 7, 0, 1)
    part_rows = (72, 48, 72)
    first_row = (0, 72, 120)

    def three(i):
        return pl.ds(3 * i, 3)

    def part_of(r):
        return (0, 0, 0, 1, 1, 2, 2, 2)[order.index(r)]

    def around(r):
        return [(0, 0), *mates] if r else mates

    for r in (7, 1, 0, 4, 5, 3, 6, 2):
        d = (NZ - r) % NZ
        to = three(8 * order.index(r) + m)
        for dx, dc in around(r):
            p = (zd[d] * NX + xd[dx]) * NC + cd[dc]
            dev = (zd[d], xd[dx], cd[dc], t)
            remote(sbuf.at[three(p)], rbuf.at[to], as_.at[part_of(r)], ar.at[part_of(r)], dev).start()
    rbuf[three(8 * order.index(0) + m)] = sbuf[three(e)]

    recut_down((2,))

    for cp in ld_ffn:
        cp.wait()
    gain = fg[...].astype(F32)
    own_gain = []
    for j in range(4):
        row = gain[j : j + 1, :]
        for i in range(1, NT):
            row = jnp.where(t == i, gain[4 * i + j : 4 * i + j + 1, :], row)
        own_gain.append(row)
    own_gain = jnp.concatenate(own_gain, axis=1)

    gs, gr, hs = (gs0, gs1, gs2), (gr0, gr1, gr2), (hs0, hs1, hs2)

    def start_part(k):
        n, at = part_rows[k], first_row[k]
        pick = pick48 if n == 48 else pick72
        remote_rows = n if k < 2 else n - 3
        both = remote(
            sbuf.at[pl.ds(0, remote_rows)], rbuf.at[pl.ds(0, remote_rows)], as_.at[k], ar.at[k],
            (z, x, 1 - c, t),
        )
        both.wait_recv()
        came = dot(pick[...].astype(BF16), rbuf[at : at + n].reshape(4 * n, HD))
        raw = jnp.concatenate([came[n * j : n * j + n] for j in range(4)], axis=1)
        rows_of = (raw * own_gain).astype(BF16)
        for d in (2, 1, 3):
            gs[k][d] = dot(rows_of, wgu[td[d]]).astype(BF16)
        for d in (2, 1, 3):
            send(gs[k].at[d], gr[k].at[d], gss.at[k, d], gsr.at[k, d], (z, x, c, td[d]))
        gate_up = dot(rows_of, wgu[t])
        square = jnp.sum(raw * raw, axis=-1, keepdims=True)
        square = jnp.concatenate([square, jnp.zeros((HD - n, 1), F32)], axis=0)
        fs[k, 0] = jnp.broadcast_to(square, (HD, HD)).T[0:8, :]
        for d in (2, 1, 3):
            send(fs.at[k, 0], fs.at[k, d], fss.at[k, d], fsr.at[k, d], (z, x, c, td[d]))
        return gate_up, both

    def middle_part(k, gate_up):
        for d in (2, 1, 3):
            arrived(gr[k].at[d], gss.at[k, d], gsr.at[k, d])
            gate_up = gate_up + gr[k][d].astype(F32)
            arrived(fs.at[k, d], fss.at[k, d], fsr.at[k, d])
        square = fs[k, 0] + fs[k, 1] + fs[k, 2] + fs[k, 3]
        square = jnp.broadcast_to(square[0:1, :], (HD, HD)).T[0 : part_rows[k], 0:1]
        gate_up = gate_up * lax.rsqrt(square / 2048.0 + EPS)
        gate = gate_up[:, 0:HD]
        hidden = gate / (1.0 + jnp.exp(-gate)) * gate_up[:, HD : 2 * HD]
        hs[k][t] = hidden.astype(BF16)
        own = hs[k].at[t]
        for d in (2, 1, 3):
            send(own, own, hss.at[k, d], hsr.at[k, d], (z, x, c, td[d]))

    def end_part(k):
        n, at = part_rows[k], first_row[k]
        back = back48 if n == 48 else back72
        for d in (2, 1, 3):
            arrived(hs[k].at[td[NT - d]], hss.at[k, d], hsr.at[k, d])
        out = dot(hs[k][0], wd[0])
        for i in range(1, NT):
            out = out + dot(hs[k][i], wd[i])
        out = jnp.concatenate([out[:, HD * j : HD * j + HD] for j in range(4)], axis=0)
        obuf[at : at + n] = dot(back[...], out.astype(BF16)).astype(BF16).reshape(n, 4, HD)
        for r in ((4, 5, 3), (6, 2), (7, 1, 0))[k]:
            for dx, dc in around(r):
                p = 8 * order.index(r) + xd[dx] * NC + cd[dc]
                dev = (zd[r], xd[dx], cd[dc], t)
                remote(obuf.at[three(p)], cbuf.at[three(e)], rs_, rr, dev).start()

    for cp in ld_ex:
        cp.wait()
    for d in (1, 3, 2):
        src = td[NT - d]
        for k in range(2):
            arrived(wgu.at[src, :, pl.ds(128 * k, 128)], ys.at[k, d], yr.at[k, d])
    gate_up2, sent2 = start_part(2)

    for d in (1, 3, 2):
        arrived(res.at[td[NT - d]], as2.at[d], ar2.at[d])
    data = jnp.concatenate([res[i] for i in range(NT)], axis=1).astype(F32)
    factor = lax.rsqrt(jnp.mean(data * data, axis=-1, keepdims=True) + EPS)
    pieces = [data[:, HD * i : HD * i + HD] * factor * gain[i : i + 1, :] for i in range(16)]
    normed_ffn = jnp.concatenate(pieces, axis=1).astype(BF16)
    for cp in ld_sh:
        cp.wait()
    both = dot(normed_ffn, sgu[...])
    gate = both[:, 0:HD]
    shared_hidden = (gate / (1.0 + jnp.exp(-gate)) * both[:, HD : 2 * HD]).astype(BF16)
    shared_part = dot(shared_hidden, sd[...]).astype(BF16)
    for i in range(NT):
        ssb[i] = shared_part[:, 512 * i : 512 * i + 512]
    for d in (2, 1, 3):
        p = td[d]
        send(ssb.at[p], ssr.at[t], sss.at[d], ssrr.at[d], (z, x, c, p))
    ssr[t] = ssb[t]
    logit = dot_nt(normed_ffn, rt[...])
    prob = 1.0 / (1.0 + jnp.exp(-logit))
    picked = jnp.where(code > 0.5, prob, 0.0)
    weight = SCALE * picked / jnp.sum(picked, axis=-1, keepdims=True)
    weight4 = jnp.concatenate([weight] * 4, axis=0)
    w_hi = weight4.astype(BF16)
    w_lo = (weight4 - w_hi.astype(F32)).astype(BF16)
    code4 = jnp.concatenate([code] * 4, axis=0).astype(BF16)
    q1 = iota((64, rows), 1) >> 2
    j1 = iota((64, rows), 1) & 3
    e1 = (q1 * 171) >> 9
    c1 = iota((64, rows), 0)
    spread_t = ones_where(e1 == c1)
    slot_to = dot(code4, spread_t)
    fits = (slot_to == (q1 - 3 * e1 + 1).astype(F32)) & (j1 == (c1 >> 4))
    comb_hi = jnp.where(fits, dot(w_hi, spread_t), 0.0).astype(BF16)
    comb_lo = jnp.where(fits, dot(w_lo, spread_t), 0.0).astype(BF16)

    for d in near_first:
        arrived(kvb.at[lax.rem(z + NZ - d, NZ)], kzs.at[d], kzr.at[d])
    kvpart[...] = dot(rows_in, kvb[...].reshape(256, 256)).astype(BF16).reshape(8, SEQ, 256)
    for dx, dc in mates:
        g = xd[dx] * NC + cd[dc]
        send(kvpart.at[g], kvp.at[m], kps.at[dx, dc], kpr.at[dx, dc], (z, xd[dx], cd[dc], t))
    kvp[m] = kvpart[m]
    gate_up0, sent0 = start_part(0)
    gate_up1, sent1 = start_part(1)
    middle_part(2, gate_up2)
    middle_part(0, gate_up0)
    middle_part(1, gate_up1)
    for d in (1, 3, 2):
        arrived(wd.at[td[NT - d]], ys.at[2, d], yr.at[2, d])
    end_part(0)
    end_part(2)
    end_part(1)
    cbuf[three(e)] = obuf[three(8 * order.index(0) + m)]
    shared_total = jnp.zeros((SEQ, 512), F32)
    for d in (2, 1, 3):
        arrived(ssr.at[td[NT - d]], sss.at[d], ssrr.at[d])
    for i in range(NT):
        shared_total = shared_total + ssr[i].astype(F32)
    base = res[t].astype(F32) + shared_total
    for dx, dc in mates:
        src = kvp.at[lax.rem(x + NX - dx, NX) * NC + cd[dc]]
        arrived(src, kps.at[dx, dc], kpr.at[dx, dc])
    new = kvp[0].astype(F32)
    for i in range(1, 8):
        new = new + kvp[i].astype(F32)
    fk_o[...] = new[:, 0:HD].astype(BF16)
    fv_o[...] = new[:, HD : 2 * HD].astype(BF16)
    back = remote(
        obuf.at[pl.ds(0, 3 * NE - 3)], cbuf.at[pl.ds(0, 3 * NE - 3)], rs_, rr, (z, x, 1 - c, t)
    )
    back.wait_recv()
    came = cbuf[...].reshape(rows, HD)
    routed = dot(comb_hi, came) + dot(comb_lo, came)
    for j in range(4):
        mixed_o[:, HD * j : HD * j + HD] = (
            base[:, HD * j : HD * j + HD] + routed[SEQ * j : SEQ * j + SEQ]
        ).astype(BF16)
    for cp in [*pending, sent0, sent1, sent2, back]:
        cp.wait_send()


def hand_over(a, b, c, a_o, b_o, c_o, sem):
    moves = []
    for i, (src, dst) in enumerate(((a, a_o), (b, b_o), (c, c_o))):
        moves.append(pltpu.make_async_copy(src, dst, sem.at[i]))
        moves[i].start()
    for cp in moves:
        cp.wait()


def body(
    tokens, attn_gain, query_weight, key_weight, value_weight, out_weight, head_gain,
    past_keys, past_values, break_offset, cache_lengths, ffn_gain, router_weight,
    expert_routes, expert_gate, expert_up, expert_down, shared_gate, shared_up, shared_down,
):
    hbm = pl.BlockSpec(memory_space=pl.ANY)
    v, dma = pltpu.VMEM, pltpu.SemaphoreType.DMA
    outs = pl.pallas_call(
        kernel,
        out_shape=(v((SEQ, 512), BF16), v((SEQ, HD), BF16), v((SEQ, HD), BF16)),
        in_specs=[hbm] * 20,
        out_specs=(pl.BlockSpec(memory_space=pltpu.VMEM),) * 3,
        scratch_shapes=[
            v((SEQ, 2048), BF16), v((16, HD), BF16), v((2, HD), BF16), v((16, HD), BF16),
            v((64, 2048), BF16), v((6, SEQ), jnp.int32), v((SEQ, 2, POS), F32),
            v((SEQ, POS, HD), BF16), v((SEQ, HD, POS), BF16), v((SEQ, POS, HD), BF16),
            v((NZ, 32, 256), BF16), v((NZ, 32, 256), BF16), v((NZ, NX, NC, 32, 256), BF16),
            v((NT, 512, 256), BF16), v((NT, 128, 512), BF16),
            v((2048, 256), BF16), v((128, 2048), BF16),
            v((8, SEQ, 256), BF16), v((8, SEQ, 256), BF16),
            v((8, SEQ, 256), F32), v((8, SEQ, 256), F32),
            v((8, SEQ, 256), BF16), v((8, SEQ, 256), BF16),
            v((2 * SEQ, HD), F32), v((2 * SEQ, POS), F32), v((2 * SEQ, HD), jnp.int32),
            v((SEQ, 256), F32), v((NT, SEQ, 512), BF16), v((NT, SEQ, 512), BF16),
            v((NT, SEQ, HD), F32), v((3, NT, 8, HD), F32), v((NT, SEQ, 512), BF16),
            v((3 * NE, 4, HD), BF16), v((3 * NE, 4, HD), BF16),
            *[v((NT, n, 256), BF16) for _ in range(2) for n in (72, 48, 72)],
            *[v((NT, n, HD), BF16) for n in (72, 48, 72)],
            v((288, 288), F32), v((288, 288), BF16), v((192, 192), F32), v((192, 192), BF16),

            v((3 * NE, 4, HD), BF16), v((3 * NE, 4, HD), BF16),
            v((NT, SEQ, 512), BF16), v((NT, SEQ, 512), BF16),
            pltpu.SMEM((SEQ,), jnp.int32), v((SEQ, 512), BF16), dma((32,)), dma((8,)),
            *[dma((NZ,)) for _ in range(6)],
            dma((NZ, NX)), dma((NZ, NX)), dma((NZ,)), dma((NZ,)),
            *[dma((NX, NC)) for _ in range(6)],
            dma((3, 4)), dma((3, 4)), dma((2, 4)), dma((2, 4)), dma((3,)), dma((3,)),
            dma((3, 4)), dma((3, 4)), dma((3, 4)), dma((3, 4)), dma, dma, dma((4,)), dma((4,)),
            dma((4,)), dma((4,)), dma((3, 4)), dma((3, 4)),
        ],
        compiler_params=pltpu.CompilerParams(
            collective_id=0, has_side_effects=True, vmem_limit_bytes=60 * 1024 * 1024
        ),
    )(
        tokens, attn_gain.reshape(16, HD), query_weight, key_weight, value_weight, out_weight,
        head_gain.reshape(2, HD), past_keys.reshape(SEQ, POS, HD),
        past_values.reshape(SEQ, POS, HD), break_offset, cache_lengths,
        ffn_gain.reshape(16, HD), router_weight.T, expert_routes.T, expert_gate, expert_up,
        expert_down, shared_gate, shared_up, shared_down,
    )
    return pl.pallas_call(
        hand_over,
        out_shape=tuple(jax.ShapeDtypeStruct(o.shape, o.dtype) for o in outs),
        in_specs=[pl.BlockSpec(memory_space=pltpu.VMEM)] * 3,
        out_specs=(hbm,) * 3,
        scratch_shapes=[dma((3,))],
    )(*[pltpu.with_memory_space_constraint(o, pltpu.VMEM) for o in outs])


def solution(mesh):
    torus = Mesh(mesh.devices.reshape(NZ, NX, NC, NT), (*EP, "tp"))
    return jax.shard_map(
        body,
        mesh=torus,
        in_specs=(
            P(EP, None),
            P(),
            P(EP, "tp"),
            P(EP, "tp"),
            P(EP, "tp"),
            P(EP, "tp"),
            P("tp"),
            P(EP, None, "tp", None),
            P(EP, None, "tp", None),
            P(EP, "tp", None),
            P(EP),
            P(),
            P(),
            P(EP, None),
            P(EP, None, "tp"),
            P(EP, None, "tp"),
            P(EP, "tp", None),
            P(None, "tp"),
            P(None, "tp"),
            P("tp", None),
        ),
        out_specs=(P(EP, "tp"), P(EP, "tp"), P(EP, "tp")),
        check_vma=False,
    )
```

```python
import jax
import jax.numpy as jnp
from jax import lax
from jax.experimental import pallas as pl
from jax.experimental.pallas import tpu as pltpu
from jax.sharding import Mesh
from jax.sharding import PartitionSpec as P

MESH = pl.DeviceIdType.MESH
EP = ("ep_0", "ep_1", "ep_2")
NZ, NX, NC, NT = 8, 4, 2, 4
NE = NZ * NX * NC
SEQ = 16
POS = 1024
HD = 128
EPS = 1e-06
SCALE = 2.5
F32 = jnp.float32
BF16 = jnp.bfloat16


def dot(a, b):
    return jnp.dot(a, b, preferred_element_type=F32)


def dot_nt(a, b):
    return lax.dot_general(a, b, (((1,), (1,)), ((), ())), preferred_element_type=F32)


def iota(shape, dim):
    return lax.broadcasted_iota(jnp.int32, shape, dim)


def ones_where(cond):
    return jnp.where(cond, 1.0, 0.0).astype(BF16)


def kernel(
    tok_h, ag_h, wq_h, wk_h, wv_h, wo_h, hg_h, pk_h, pv_h, off_h, lens_h, fg_h, rt_h, er_h,
    eg_h, eu_h, ed_h, sg_h, su_h, sd_h,
    mixed_o, fk_o, fv_o,
    tok, ag, hg, fg, rt, er, off, kb, kt, vb, qb, kvb, ob, wgu, wd, sgu, sd,
    tkb, tk, part, qp, kvpart, kvp,
    qs, lg, lenb, ho, pcs, pc, sq, fs, res, sbuf, rbuf, gs0, gs1, gs2, gr0, gr1, gr2, hs0, hs1, hs2,
    pick72, back72, pick48, back48, obuf, cbuf, ssb, ssr,
    lens, tokb, lsem, kvsem,
    qzs, qzr, kzs, kzr, ozs, ozr, oxs, oxr, ods, odr, tks, tkr, qps, qpr, kps, kpr,
    ys, yr, cs, cr, as_, ar, gss, gsr, hss, hsr, rs_, rr, sss, ssrr, as2, ar2, fss, fsr,
):
    z = lax.axis_index("ep_0")
    x = lax.axis_index("ep_1")
    c = lax.axis_index("ep_2")
    t = lax.axis_index("tp")
    e = (z * NX + x) * NC + c
    m = x * NC + c
    zd = [lax.rem(z + d, NZ) for d in range(NZ)]
    xd = [lax.rem(x + d, NX) for d in range(NX)]
    td = [lax.rem(t + d, NT) for d in range(NT)]
    cd = [c, 1 - c]
    mates = [(2, 0), (2, 1), (1, 0), (3, 0), (1, 1), (3, 1), (0, 1)]
    far_first = [4, 3, 5, 2, 6, 1, 7]
    near_first = far_first[::-1]

    def remote(src, dst, ssem, rsem, dev):
        return pltpu.make_async_remote_copy(
            src_ref=src, dst_ref=dst, send_sem=ssem, recv_sem=rsem,
            device_id=dev, device_id_type=MESH,
        )

    pending = []

    def send(src, dst, ssem, rsem, dev):
        cp = remote(src, dst, ssem, rsem, dev)
        cp.start()
        pending.append(cp)

    def arrived(dst, ssem, rsem):
        remote(dst, dst, ssem, rsem, (z, x, 1 - c, t)).wait_recv()

    loads = []

    def load(src, dst):
        cp = pltpu.make_async_copy(src, dst, lsem.at[len(loads)])
        cp.start()
        loads.append(cp)
        return cp

    ld_q = load(wq_h, qb.at[z])
    ld_tok = [load(tok_h, tok), load(ag_h, ag)]
    ld_o = load(wo_h, ob.at[z, x, c])
    ld_kv = [
        load(wk_h, kvb.at[z, :, pl.ds(0, 128)]),
        load(wv_h, kvb.at[z, :, pl.ds(128, 128)]),
    ]
    barrier = pltpu.get_barrier_semaphore()
    first = [(zd[d], x, c, t) for d in range(1, NZ)]
    first += [(z, xd[dx], cd[dc], t) for dx, dc in mates]
    first += [(z, x, c, td[d]) for d in range(1, NT)]
    for dev in first:
        pl.semaphore_signal(barrier, inc=1, device_id=dev, device_id_type=MESH)

    pl.semaphore_wait(barrier, len(first))

    mine_o = ob.at[z, x, c]

    def q_around(*steps):
        for d in steps:
            send(qb.at[z], qb.at[z], qzs.at[d], qzr.at[d], (zd[d], x, c, t))

    def o_around(*steps):
        for d in steps:
            send(mine_o, mine_o, ozs.at[d], ozr.at[d], (zd[d], x, c, t))

    ld_o.wait()
    o_around(*(1, 7, 2, 6))
    ld_q.wait()
    q_around(*far_first)

    for cp in ld_tok:
        cp.wait()
    data = tok[...].astype(F32)
    factor = lax.rsqrt(jnp.mean(data * data, axis=-1, keepdims=True) + EPS)
    gain = ag[...].astype(F32)
    blocks = []
    for i in range(NZ):
        halves = []
        for k in (2 * i, 2 * i + 1):
            halves.append(data[:, HD * k : HD * k + HD] * factor * gain[k : k + 1, :])
        blocks.append(jnp.concatenate(halves, axis=1).astype(BF16).astype(F32))
    chunk = iota((SEQ, 256), 1) >> 5
    for g in range(8):
        own = blocks[g]
        for k in range(1, 8):
            j = (g + k) % 8
            own = jnp.where(chunk == j, pltpu.roll(blocks[j], 32 * k, 1), own)
        tkb[g] = own.astype(BF16)
    for dx, dc in mates:
        g = xd[dx] * NC + cd[dc]
        send(tkb.at[g], tk.at[m], tks.at[dx, dc], tkr.at[dx, dc], (z, xd[dx], cd[dc], t))
    tk[m] = tkb[m]

    def o_along(r):
        src = ob.at[zd[r], x, c]
        for i in (1, 3, 2):
            send(src, src, oxs.at[r, i], oxr.at[r, i], (z, xd[i], c, t))

    def o_forward(r):
        src = ob.at[zd[r], x, c]
        arrived(src, ozs.at[NZ - r], ozr.at[NZ - r])
        o_along(r)

    def o_across(r):
        for i in (1, 3, 2):
            arrived(ob.at[zd[r], xd[i], c], oxs.at[r, NX - i], oxr.at[r, NX - i])
        src = ob.at[zd[r], :, c]
        send(src, src, ods.at[r], odr.at[r], (z, x, 1 - c, t))

    def o_last():
        for r in range(NZ):
            arrived(ob.at[zd[r], :, 1 - c], ods.at[r], odr.at[r])

    o_along(0)
    ld_er = load(er_h, er)
    ld_att = [load(off_h, off), load(hg_h, hg), load(lens_h, lens)]
    kv_loads = []
    for i in range(4):
        ds = pl.ds(4 * i, 4)
        kv_loads.append(pltpu.make_async_copy(pk_h.at[ds], kb.at[ds], kvsem.at[i]))
        kv_loads.append(pltpu.make_async_copy(pv_h.at[ds], vb.at[ds], kvsem.at[4 + i]))
    for cp in kv_loads:
        cp.start()
    ld_ffn = [load(fg_h, fg), load(rt_h, rt)]
    ld_sh = [
        load(sg_h, sgu.at[:, pl.ds(0, 128)]),
        load(su_h, sgu.at[:, pl.ds(128, 128)]),
        load(sd_h, sd),
    ]
    mine = pl.ds(pl.multiple_of(t * 512, 512), 512)
    ld_own = load(tok_h.at[:, mine], tokb)
    ld_ex = [
        load(eg_h.at[0, mine, :], wgu.at[t, :, pl.ds(0, 128)]),
        load(eu_h.at[0, mine, :], wgu.at[t, :, pl.ds(128, 128)]),
        load(ed_h.at[0, :, mine], wd.at[t]),
    ]

    def recut_down(peers):
        for d in peers:
            theirs = pl.ds(pl.multiple_of(td[d] * 512, 512), 512)
            send(ed_h.at[0, :, theirs], wd.at[t], ys.at[2, d], yr.at[2, d], (z, x, c, td[d]))

    for d in (1, 3, 2):
        p = td[d]
        dev = (z, x, c, p)
        theirs = pl.ds(pl.multiple_of(p * 512, 512), 512)
        for k, src in enumerate((eg_h, eu_h)):
            half = pl.ds(128 * k, 128)
            send(src.at[0, theirs, :], wgu.at[t, :, half], ys.at[k, d], yr.at[k, d], dev)
    recut_down((1, 3))

    ld_er.wait()
    rows = NE * 12
    chosen = iota((NE, SEQ), 0) == er[0:1, :]
    for k in range(1, 6):
        chosen = chosen | (iota((NE, SEQ), 0) == er[k : k + 1, :])
    hot_t = ones_where(chosen)
    before = ones_where(iota((SEQ, SEQ), 0) < iota((SEQ, SEQ), 1))
    code_t = jnp.where(chosen, dot(hot_t, before) + 1.0, 0.0).astype(BF16)
    repeat = ones_where((iota((SEQ, 64), 1) & 15) == iota((SEQ, 64), 0))
    eye = ones_where(iota((SEQ, SEQ), 0) == iota((SEQ, SEQ), 1))
    code4_t = dot(code_t, repeat).astype(BF16)
    code = dot_nt(eye, code_t)
    q0 = iota((rows, 64), 0) >> 2
    j0 = iota((rows, 64), 0) & 3
    e0 = (q0 * 171) >> 9
    c0 = iota((rows, 64), 1)
    spread = ones_where(e0 == c0)
    slot_of = dot(spread, code4_t)
    want = (q0 - 3 * e0 + 1).astype(F32)
    dispatch = ones_where((slot_of == want) & (j0 == (c0 >> 4)))

    o_around(*(4, 3, 5))
    for n, pick, back in ((72, pick72, back72), (48, pick48, back48)):
        for j in range(4):
            p, q = iota((n, 4 * n), 0), iota((n, 4 * n), 1)
            pick[n * j : n * j + n, :] = jnp.where(q == 4 * p + j, 1.0, 0.0)
        p, q = iota((4 * n, 4 * n), 1), iota((4 * n, 4 * n), 0)
        j = (p >= n).astype(jnp.int32) + (p >= 2 * n) + (p >= 3 * n)
        back[...] = ones_where(q == 4 * (p - n * j) + j)
    for b in range(SEQ):
        if b % 4 == 0:
            kv_loads[2 * (b // 4)].wait()
        kt[b] = kb[b].T
    o_forward(7)
    o_forward(1)
    o_forward(6)
    o_forward(2)

    for dx, dc in mates:
        src = tk.at[lax.rem(x + NX - dx, NX) * NC + cd[dc]]
        arrived(src, tks.at[dx, dc], tkr.at[dx, dc])
    for d in near_first:
        arrived(qb.at[lax.rem(z + NZ - d, NZ)], qzs.at[d], qzr.at[d])
    rows_in = tk[...].reshape(8 * SEQ, 256)
    part[...] = dot(rows_in, qb[...].reshape(256, 256)).reshape(8, SEQ, 256)
    for dx, dc in mates:
        g = xd[dx] * NC + cd[dc]
        send(part.at[g], qp.at[m], qps.at[dx, dc], qpr.at[dx, dc], (z, xd[dx], cd[dc], t))
    qp[m] = part[m]
    for r in (5, 3, 4):
        o_forward(r)
    for dx, dc in mates:
        src = qp.at[lax.rem(x + NX - dx, NX) * NC + cd[dc]]
        arrived(src, qps.at[dx, dc], qpr.at[dx, dc])
    total = qp[0]
    for i in range(1, 8):
        total = total + qp[i]
    queries = total.astype(BF16).astype(F32)

    for h in range(2):
        qs[pl.ds(h, SEQ, stride=2), :] = queries[:, HD * h : HD * h + HD]
    for cp in ld_att:
        cp.wait()
    for b in range(SEQ):
        q = qs[2 * b : 2 * b + 2, :].astype(BF16)
        lg[2 * b : 2 * b + 2, :] = dot(q, kt[b]) * HD ** (-0.5) + off[b]
        lenb[2 * b : 2 * b + 2, :] = jnp.full((2, HD), lens[b], jnp.int32)
    for cp in ld_kv:
        cp.wait()
    for d in far_first:
        send(kvb.at[z], kvb.at[z], kzs.at[d], kzr.at[d], (zd[d], x, c, t))
    for r in (0, 7, 1, 6, 2):
        o_across(r)
    logits = lg[...]
    length = lenb[:, 0:1]
    usable = iota((2 * SEQ, POS), 1) < length
    tail = jnp.log(1.0 + jnp.exp(-jnp.abs(logits)))
    keep = jnp.where(usable, jnp.minimum(-logits, 0.0) - tail, 0.0)
    nb = POS // HD
    stacked = jnp.concatenate([keep[:, HD * i : HD * i + HD] for i in range(nb)], axis=0)
    k1 = stacked.astype(BF16)
    left = stacked - k1.astype(F32)
    k2 = left.astype(BF16)
    k3 = (left - k2.astype(F32)).astype(BF16)
    later = ones_where(iota((HD, HD), 0) > iota((HD, HD), 1))
    inner = dot(k1, later) + dot(k2, later) + dot(k3, later)
    carry = jnp.zeros((2 * SEQ, 1), F32)
    after = [None] * nb
    n2 = 2 * SEQ
    for i in range(nb - 1, -1, -1):
        after[i] = inner[n2 * i : n2 * i + n2] + carry
        carry = carry + jnp.sum(stacked[n2 * i : n2 * i + n2], axis=-1, keepdims=True)
    after = jnp.concatenate(after, axis=1)
    sticks = jnp.where(usable, jnp.exp(jnp.minimum(logits, 0.0) - tail + after), 0.0)
    lg[...] = sticks
    for r in (5, 3, 4):
        o_across(r)
    for b in range(SEQ):
        if b % 4 == 0:
            kv_loads[2 * (b // 4) + 1].wait()
        got = dot(lg[2 * b : 2 * b + 2, :].astype(BF16), vb[b])
        ho[b : b + 1, 0:HD] = got[0:1, :]
        ho[b : b + 1, HD : 2 * HD] = got[1:2, :]
    heads_out = ho[...]
    scaled = jnp.concatenate(
        [heads_out[:, HD * i : HD * i + HD] * hg[i : i + 1, :].astype(F32) for i in range(2)],
        axis=1,
    ).astype(BF16)
    sq[t] = jnp.broadcast_to(jnp.sum(heads_out * heads_out, axis=-1, keepdims=True), (SEQ, HD))
    o_last()
    for i in range(NT):
        halves = [dot_nt(scaled, ob[zi].reshape(256, 256)) for zi in (2 * i, 2 * i + 1)]
        pcs[i] = jnp.concatenate(halves, axis=1).astype(BF16)

    for d in (2, 1, 3):
        dev = (z, x, c, td[d])
        send(sq.at[t], sq.at[t], cs.at[0, d], cr.at[0, d], dev)
        send(pcs.at[td[d]], pc.at[t], cs.at[1, d], cr.at[1, d], dev)
    pc[t] = pcs[t]
    for d in (1, 3, 2):
        src = td[NT - d]
        for k, buf in enumerate((sq, pc)):
            arrived(buf.at[src], cs.at[k, d], cr.at[k, d])
    head_total = pc[0].astype(F32)
    square = sq[0]
    for i in range(1, NT):
        head_total = head_total + pc[i].astype(F32)
        square = square + sq[i]
    attention = head_total * lax.rsqrt(square[:, 0:1] / 1024.0 + EPS)
    ld_own.wait()
    residual = (tokb[...].astype(F32) + attention).astype(BF16)
    res[t] = residual
    for d in (2, 1, 3):
        send(res.at[t], res.at[t], as2.at[d], ar2.at[d], (z, x, c, td[d]))

    block = jnp.concatenate([residual[:, HD * j : HD * j + HD] for j in range(4)], axis=0)
    sbuf[...] = dot(dispatch, block).astype(BF16).reshape(3 * NE, 4, HD)
    order = (3, 4, 5, 2, 6, 7, 0, 1)
    part_rows = (72, 48, 72)
    first_row = (0, 72, 120)

    def three(i):
        return pl.ds(3 * i, 3)

    def part_of(r):
        return (0, 0, 0, 1, 1, 2, 2, 2)[order.index(r)]

    def around(r):
        return [(0, 0), *mates] if r else mates

    for r in (4, 7, 1, 0, 5, 3, 6, 2):
        d = (NZ - r) % NZ
        to = three(8 * order.index(r) + m)
        for dx, dc in around(r):
            p = (zd[d] * NX + xd[dx]) * NC + cd[dc]
            dev = (zd[d], xd[dx], cd[dc], t)
            remote(sbuf.at[three(p)], rbuf.at[to], as_.at[part_of(r)], ar.at[part_of(r)], dev).start()
    rbuf[three(8 * order.index(0) + m)] = sbuf[three(e)]

    recut_down((2,))

    for cp in ld_ffn:
        cp.wait()
    gain = fg[...].astype(F32)
    own_gain = []
    for j in range(4):
        row = gain[j : j + 1, :]
        for i in range(1, NT):
            row = jnp.where(t == i, gain[4 * i + j : 4 * i + j + 1, :], row)
        own_gain.append(row)
    own_gain = jnp.concatenate(own_gain, axis=1)

    gs, gr, hs = (gs0, gs1, gs2), (gr0, gr1, gr2), (hs0, hs1, hs2)

    def start_part(k):
        n, at = part_rows[k], first_row[k]
        pick = pick48 if n == 48 else pick72
        remote_rows = n if k < 2 else n - 3
        both = remote(
            sbuf.at[pl.ds(0, remote_rows)], rbuf.at[pl.ds(0, remote_rows)], as_.at[k], ar.at[k],
            (z, x, 1 - c, t),
        )
        both.wait_recv()
        came = dot(pick[...].astype(BF16), rbuf[at : at + n].reshape(4 * n, HD))
        raw = jnp.concatenate([came[n * j : n * j + n] for j in range(4)], axis=1)
        rows_of = (raw * own_gain).astype(BF16)
        for d in (2, 1, 3):
            gs[k][d] = dot(rows_of, wgu[td[d]]).astype(BF16)
        for d in (2, 1, 3):
            send(gs[k].at[d], gr[k].at[d], gss.at[k, d], gsr.at[k, d], (z, x, c, td[d]))
        gate_up = dot(rows_of, wgu[t])
        square = jnp.sum(raw * raw, axis=-1, keepdims=True)
        square = jnp.concatenate([square, jnp.zeros((HD - n, 1), F32)], axis=0)
        fs[k, 0] = jnp.broadcast_to(square, (HD, HD)).T[0:8, :]
        for d in (2, 1, 3):
            send(fs.at[k, 0], fs.at[k, d], fss.at[k, d], fsr.at[k, d], (z, x, c, td[d]))
        return gate_up, both

    def middle_part(k, gate_up):
        for d in (2, 1, 3):
            arrived(gr[k].at[d], gss.at[k, d], gsr.at[k, d])
            gate_up = gate_up + gr[k][d].astype(F32)
            arrived(fs.at[k, d], fss.at[k, d], fsr.at[k, d])
        square = fs[k, 0] + fs[k, 1] + fs[k, 2] + fs[k, 3]
        square = jnp.broadcast_to(square[0:1, :], (HD, HD)).T[0 : part_rows[k], 0:1]
        gate_up = gate_up * lax.rsqrt(square / 2048.0 + EPS)
        gate = gate_up[:, 0:HD]
        hidden = gate / (1.0 + jnp.exp(-gate)) * gate_up[:, HD : 2 * HD]
        hs[k][t] = hidden.astype(BF16)
        own = hs[k].at[t]
        for d in (2, 1, 3):
            send(own, own, hss.at[k, d], hsr.at[k, d], (z, x, c, td[d]))

    def end_part(k):
        n, at = part_rows[k], first_row[k]
        back = back48 if n == 48 else back72
        for d in (2, 1, 3):
            arrived(hs[k].at[td[NT - d]], hss.at[k, d], hsr.at[k, d])
        out = dot(hs[k][0], wd[0])
        for i in range(1, NT):
            out = out + dot(hs[k][i], wd[i])
        out = jnp.concatenate([out[:, HD * j : HD * j + HD] for j in range(4)], axis=0)
        obuf[at : at + n] = dot(back[...], out.astype(BF16)).astype(BF16).reshape(n, 4, HD)
        for r in ((4, 5, 3), (6, 2), (7, 1, 0))[k]:
            for dx, dc in around(r):
                p = 8 * order.index(r) + xd[dx] * NC + cd[dc]
                dev = (zd[r], xd[dx], cd[dc], t)
                remote(obuf.at[three(p)], cbuf.at[three(e)], rs_, rr, dev).start()

    for cp in ld_ex:
        cp.wait()
    for d in (1, 3, 2):
        src = td[NT - d]
        for k in range(2):
            arrived(wgu.at[src, :, pl.ds(128 * k, 128)], ys.at[k, d], yr.at[k, d])
    gate_up2, sent2 = start_part(2)

    for d in (1, 3, 2):
        arrived(res.at[td[NT - d]], as2.at[d], ar2.at[d])
    data = jnp.concatenate([res[i] for i in range(NT)], axis=1).astype(F32)
    factor = lax.rsqrt(jnp.mean(data * data, axis=-1, keepdims=True) + EPS)
    pieces = [data[:, HD * i : HD * i + HD] * factor * gain[i : i + 1, :] for i in range(16)]
    normed_ffn = jnp.concatenate(pieces, axis=1).astype(BF16)
    for cp in ld_sh:
        cp.wait()
    both = dot(normed_ffn, sgu[...])
    gate = both[:, 0:HD]
    shared_hidden = (gate / (1.0 + jnp.exp(-gate)) * both[:, HD : 2 * HD]).astype(BF16)
    shared_part = dot(shared_hidden, sd[...]).astype(BF16)
    for i in range(NT):
        ssb[i] = shared_part[:, 512 * i : 512 * i + 512]
    for d in (2, 1, 3):
        p = td[d]
        send(ssb.at[p], ssr.at[t], sss.at[d], ssrr.at[d], (z, x, c, p))
    ssr[t] = ssb[t]
    logit = dot_nt(normed_ffn, rt[...])
    prob = 1.0 / (1.0 + jnp.exp(-logit))
    picked = jnp.where(code > 0.5, prob, 0.0)
    weight = SCALE * picked / jnp.sum(picked, axis=-1, keepdims=True)
    weight4 = jnp.concatenate([weight] * 4, axis=0)
    w_hi = weight4.astype(BF16)
    w_lo = (weight4 - w_hi.astype(F32)).astype(BF16)
    code4 = jnp.concatenate([code] * 4, axis=0).astype(BF16)
    q1 = iota((64, rows), 1) >> 2
    j1 = iota((64, rows), 1) & 3
    e1 = (q1 * 171) >> 9
    c1 = iota((64, rows), 0)
    spread_t = ones_where(e1 == c1)
    slot_to = dot(code4, spread_t)
    fits = (slot_to == (q1 - 3 * e1 + 1).astype(F32)) & (j1 == (c1 >> 4))
    comb_hi = jnp.where(fits, dot(w_hi, spread_t), 0.0).astype(BF16)
    comb_lo = jnp.where(fits, dot(w_lo, spread_t), 0.0).astype(BF16)

    for d in near_first:
        arrived(kvb.at[lax.rem(z + NZ - d, NZ)], kzs.at[d], kzr.at[d])
    kvpart[...] = dot(rows_in, kvb[...].reshape(256, 256)).astype(BF16).reshape(8, SEQ, 256)
    for dx, dc in mates:
        g = xd[dx] * NC + cd[dc]
        send(kvpart.at[g], kvp.at[m], kps.at[dx, dc], kpr.at[dx, dc], (z, xd[dx], cd[dc], t))
    kvp[m] = kvpart[m]
    gate_up0, sent0 = start_part(0)
    gate_up1, sent1 = start_part(1)
    middle_part(2, gate_up2)
    middle_part(0, gate_up0)
    middle_part(1, gate_up1)
    for d in (1, 3, 2):
        arrived(wd.at[td[NT - d]], ys.at[2, d], yr.at[2, d])
    end_part(0)
    end_part(2)
    end_part(1)
    cbuf[three(e)] = obuf[three(8 * order.index(0) + m)]
    shared_total = jnp.zeros((SEQ, 512), F32)
    for d in (2, 1, 3):
        arrived(ssr.at[td[NT - d]], sss.at[d], ssrr.at[d])
    for i in range(NT):
        shared_total = shared_total + ssr[i].astype(F32)
    base = res[t].astype(F32) + shared_total
    for dx, dc in mates:
        src = kvp.at[lax.rem(x + NX - dx, NX) * NC + cd[dc]]
        arrived(src, kps.at[dx, dc], kpr.at[dx, dc])
    new = kvp[0].astype(F32)
    for i in range(1, 8):
        new = new + kvp[i].astype(F32)
    fk_o[...] = new[:, 0:HD].astype(BF16)
    fv_o[...] = new[:, HD : 2 * HD].astype(BF16)
    back = remote(
        obuf.at[pl.ds(0, 3 * NE - 3)], cbuf.at[pl.ds(0, 3 * NE - 3)], rs_, rr, (z, x, 1 - c, t)
    )
    back.wait_recv()
    came = cbuf[...].reshape(rows, HD)
    routed = dot(comb_hi, came) + dot(comb_lo, came)
    for j in range(4):
        mixed_o[:, HD * j : HD * j + HD] = (
            base[:, HD * j : HD * j + HD] + routed[SEQ * j : SEQ * j + SEQ]
        ).astype(BF16)
    for cp in [*pending, sent0, sent1, sent2, back]:
        cp.wait_send()


def hand_over(a, b, c, a_o, b_o, c_o, sem):
    moves = []
    for i, (src, dst) in enumerate(((a, a_o), (b, b_o), (c, c_o))):
        moves.append(pltpu.make_async_copy(src, dst, sem.at[i]))
        moves[i].start()
    for cp in moves:
        cp.wait()


def body(
    tokens, attn_gain, query_weight, key_weight, value_weight, out_weight, head_gain,
    past_keys, past_values, break_offset, cache_lengths, ffn_gain, router_weight,
    expert_routes, expert_gate, expert_up, expert_down, shared_gate, shared_up, shared_down,
):
    hbm = pl.BlockSpec(memory_space=pl.ANY)
    v, dma = pltpu.VMEM, pltpu.SemaphoreType.DMA
    outs = pl.pallas_call(
        kernel,
        out_shape=(v((SEQ, 512), BF16), v((SEQ, HD), BF16), v((SEQ, HD), BF16)),
        in_specs=[hbm] * 20,
        out_specs=(pl.BlockSpec(memory_space=pltpu.VMEM),) * 3,
        scratch_shapes=[
            v((SEQ, 2048), BF16), v((16, HD), BF16), v((2, HD), BF16), v((16, HD), BF16),
            v((64, 2048), BF16), v((6, SEQ), jnp.int32), v((SEQ, 2, POS), F32),
            v((SEQ, POS, HD), BF16), v((SEQ, HD, POS), BF16), v((SEQ, POS, HD), BF16),
            v((NZ, 32, 256), BF16), v((NZ, 32, 256), BF16), v((NZ, NX, NC, 32, 256), BF16),
            v((NT, 512, 256), BF16), v((NT, 128, 512), BF16),
            v((2048, 256), BF16), v((128, 2048), BF16),
            v((8, SEQ, 256), BF16), v((8, SEQ, 256), BF16),
            v((8, SEQ, 256), F32), v((8, SEQ, 256), F32),
            v((8, SEQ, 256), BF16), v((8, SEQ, 256), BF16),
            v((2 * SEQ, HD), F32), v((2 * SEQ, POS), F32), v((2 * SEQ, HD), jnp.int32),
            v((SEQ, 256), F32), v((NT, SEQ, 512), BF16), v((NT, SEQ, 512), BF16),
            v((NT, SEQ, HD), F32), v((3, NT, 8, HD), F32), v((NT, SEQ, 512), BF16),
            v((3 * NE, 4, HD), BF16), v((3 * NE, 4, HD), BF16),
            *[v((NT, n, 256), BF16) for _ in range(2) for n in (72, 48, 72)],
            *[v((NT, n, HD), BF16) for n in (72, 48, 72)],
            v((288, 288), F32), v((288, 288), BF16), v((192, 192), F32), v((192, 192), BF16),

            v((3 * NE, 4, HD), BF16), v((3 * NE, 4, HD), BF16),
            v((NT, SEQ, 512), BF16), v((NT, SEQ, 512), BF16),
            pltpu.SMEM((SEQ,), jnp.int32), v((SEQ, 512), BF16), dma((32,)), dma((8,)),
            *[dma((NZ,)) for _ in range(6)],
            dma((NZ, NX)), dma((NZ, NX)), dma((NZ,)), dma((NZ,)),
            *[dma((NX, NC)) for _ in range(6)],
            dma((3, 4)), dma((3, 4)), dma((2, 4)), dma((2, 4)), dma((3,)), dma((3,)),
            dma((3, 4)), dma((3, 4)), dma((3, 4)), dma((3, 4)), dma, dma, dma((4,)), dma((4,)),
            dma((4,)), dma((4,)), dma((3, 4)), dma((3, 4)),
        ],
        compiler_params=pltpu.CompilerParams(
            collective_id=0, has_side_effects=True, vmem_limit_bytes=60 * 1024 * 1024
        ),
    )(
        tokens, attn_gain.reshape(16, HD), query_weight, key_weight, value_weight, out_weight,
        head_gain.reshape(2, HD), past_keys.reshape(SEQ, POS, HD),
        past_values.reshape(SEQ, POS, HD), break_offset, cache_lengths,
        ffn_gain.reshape(16, HD), router_weight.T, expert_routes.T, expert_gate, expert_up,
        expert_down, shared_gate, shared_up, shared_down,
    )
    return pl.pallas_call(
        hand_over,
        out_shape=tuple(jax.ShapeDtypeStruct(o.shape, o.dtype) for o in outs),
        in_specs=[pl.BlockSpec(memory_space=pltpu.VMEM)] * 3,
        out_specs=(hbm,) * 3,
        scratch_shapes=[dma((3,))],
    )(*[pltpu.with_memory_space_constraint(o, pltpu.VMEM) for o in outs])


def solution(mesh):
    torus = Mesh(mesh.devices.reshape(NZ, NX, NC, NT), (*EP, "tp"))
    return jax.shard_map(
        body,
        mesh=torus,
        in_specs=(
            P(EP, None),
            P(),
            P(EP, "tp"),
            P(EP, "tp"),
            P(EP, "tp"),
            P(EP, "tp"),
            P("tp"),
            P(EP, None, "tp", None),
            P(EP, None, "tp", None),
            P(EP, "tp", None),
            P(EP),
            P(),
            P(),
            P(EP, None),
            P(EP, None, "tp"),
            P(EP, None, "tp"),
            P(EP, "tp", None),
            P(None, "tp"),
            P(None, "tp"),
            P("tp", None),
        ),
        out_specs=(P(EP, "tp"), P(EP, "tp"), P(EP, "tp")),
        check_vma=False,
    )
```

```python
import jax
import jax.numpy as jnp
from jax import lax
from jax.experimental import pallas as pl
from jax.experimental.pallas import tpu as pltpu
from jax.sharding import Mesh
from jax.sharding import PartitionSpec as P

MESH = pl.DeviceIdType.MESH
EP = ("ep_0", "ep_1", "ep_2")
NZ, NX, NC, NT = 8, 4, 2, 4
NE = NZ * NX * NC
SEQ = 16
POS = 1024
HD = 128
EPS = 1e-06
SCALE = 2.5
F32 = jnp.float32
BF16 = jnp.bfloat16


def dot(a, b):
    return jnp.dot(a, b, preferred_element_type=F32)


def dot_nt(a, b):
    return lax.dot_general(a, b, (((1,), (1,)), ((), ())), preferred_element_type=F32)


def iota(shape, dim):
    return lax.broadcasted_iota(jnp.int32, shape, dim)


def ones_where(cond):
    return jnp.where(cond, 1.0, 0.0).astype(BF16)


def kernel(
    tok_h, ag_h, wq_h, wk_h, wv_h, wo_h, hg_h, pk_h, pv_h, off_h, lens_h, fg_h, rt_h, er_h,
    eg_h, eu_h, ed_h, sg_h, su_h, sd_h,
    mixed_o, fk_o, fv_o,
    tok, ag, hg, fg, rt, er, off, kb, kt, vb, qb, kvb, ob, wgu, wd, sgu, sd,
    tkb, tk, part, qp, kvpart, kvp,
    qs, lg, lenb, ho, pcs, pc, sq, fs, res, sbuf, rbuf, gs0, gs1, gs2, gr0, gr1, gr2, hs0, hs1, hs2,
    pick72, back72, pick48, back48, obuf, cbuf, ssb, ssr,
    lens, tokb, lsem, kvsem,
    qzs, qzr, kzs, kzr, ozs, ozr, oxs, oxr, ods, odr, tks, tkr, qps, qpr, kps, kpr,
    ys, yr, cs, cr, as_, ar, gss, gsr, hss, hsr, rs_, rr, sss, ssrr, as2, ar2, fss, fsr,
):
    z = lax.axis_index("ep_0")
    x = lax.axis_index("ep_1")
    c = lax.axis_index("ep_2")
    t = lax.axis_index("tp")
    e = (z * NX + x) * NC + c
    m = x * NC + c
    zd = [lax.rem(z + d, NZ) for d in range(NZ)]
    xd = [lax.rem(x + d, NX) for d in range(NX)]
    td = [lax.rem(t + d, NT) for d in range(NT)]
    cd = [c, 1 - c]
    mates = [(2, 0), (2, 1), (1, 0), (3, 0), (1, 1), (3, 1), (0, 1)]
    far_first = [4, 3, 5, 2, 6, 1, 7]
    near_first = far_first[::-1]

    def remote(src, dst, ssem, rsem, dev):
        return pltpu.make_async_remote_copy(
            src_ref=src, dst_ref=dst, send_sem=ssem, recv_sem=rsem,
            device_id=dev, device_id_type=MESH,
        )

    pending = []

    def send(src, dst, ssem, rsem, dev):
        cp = remote(src, dst, ssem, rsem, dev)
        cp.start()
        pending.append(cp)

    def arrived(dst, ssem, rsem):
        remote(dst, dst, ssem, rsem, (z, x, 1 - c, t)).wait_recv()

    loads = []

    def load(src, dst):
        cp = pltpu.make_async_copy(src, dst, lsem.at[len(loads)])
        cp.start()
        loads.append(cp)
        return cp

    ld_q = load(wq_h, qb.at[z])
    ld_tok = [load(tok_h, tok), load(ag_h, ag)]
    ld_o = load(wo_h, ob.at[z, x, c])
    ld_kv = [
        load(wk_h, kvb.at[z, :, pl.ds(0, 128)]),
        load(wv_h, kvb.at[z, :, pl.ds(128, 128)]),
    ]
    barrier = pltpu.get_barrier_semaphore()
    first = [(zd[d], x, c, t) for d in range(1, NZ)]
    first += [(z, xd[dx], cd[dc], t) for dx, dc in mates]
    first += [(z, x, c, td[d]) for d in range(1, NT)]
    for dev in first:
        pl.semaphore_signal(barrier, inc=1, device_id=dev, device_id_type=MESH)

    pl.semaphore_wait(barrier, len(first))

    mine_o = ob.at[z, x, c]

    def q_around(*steps):
        for d in steps:
            send(qb.at[z], qb.at[z], qzs.at[d], qzr.at[d], (zd[d], x, c, t))

    def o_around(*steps):
        for d in steps:
            send(mine_o, mine_o, ozs.at[d], ozr.at[d], (zd[d], x, c, t))

    ld_o.wait()
    o_around(*(1, 7, 2, 6))
    ld_q.wait()
    q_around(*far_first)

    for cp in ld_tok:
        cp.wait()
    data = tok[...].astype(F32)
    factor = lax.rsqrt(jnp.mean(data * data, axis=-1, keepdims=True) + EPS)
    gain = ag[...].astype(F32)
    blocks = []
    for i in range(NZ):
        halves = []
        for k in (2 * i, 2 * i + 1):
            halves.append(data[:, HD * k : HD * k + HD] * factor * gain[k : k + 1, :])
        blocks.append(jnp.concatenate(halves, axis=1).astype(BF16).astype(F32))
    chunk = iota((SEQ, 256), 1) >> 5
    for g in range(8):
        own = blocks[g]
        for k in range(1, 8):
            j = (g + k) % 8
            own = jnp.where(chunk == j, pltpu.roll(blocks[j], 32 * k, 1), own)
        tkb[g] = own.astype(BF16)
    for dx, dc in mates:
        g = xd[dx] * NC + cd[dc]
        send(tkb.at[g], tk.at[m], tks.at[dx, dc], tkr.at[dx, dc], (z, xd[dx], cd[dc], t))
    tk[m] = tkb[m]

    o_around(4, 3, 5)

    def o_along(r):
        src = ob.at[zd[r], x, c]
        for i in (1, 3, 2):
            send(src, src, oxs.at[r, i], oxr.at[r, i], (z, xd[i], c, t))

    def o_forward(r):
        src = ob.at[zd[r], x, c]
        arrived(src, ozs.at[NZ - r], ozr.at[NZ - r])
        o_along(r)

    def o_across(r):
        for i in (1, 3, 2):
            arrived(ob.at[zd[r], xd[i], c], oxs.at[r, NX - i], oxr.at[r, NX - i])
        src = ob.at[zd[r], :, c]
        send(src, src, ods.at[r], odr.at[r], (z, x, 1 - c, t))

    def o_last():
        for r in range(NZ):
            arrived(ob.at[zd[r], :, 1 - c], ods.at[r], odr.at[r])

    o_along(0)
    ld_er = load(er_h, er)
    ld_att = [load(off_h, off), load(hg_h, hg), load(lens_h, lens)]
    kv_loads = []
    for i in range(4):
        ds = pl.ds(4 * i, 4)
        kv_loads.append(pltpu.make_async_copy(pk_h.at[ds], kb.at[ds], kvsem.at[i]))
        kv_loads.append(pltpu.make_async_copy(pv_h.at[ds], vb.at[ds], kvsem.at[4 + i]))
    for cp in kv_loads:
        cp.start()
    ld_ffn = [load(fg_h, fg), load(rt_h, rt)]
    ld_sh = [
        load(sg_h, sgu.at[:, pl.ds(0, 128)]),
        load(su_h, sgu.at[:, pl.ds(128, 128)]),
        load(sd_h, sd),
    ]
    mine = pl.ds(pl.multiple_of(t * 512, 512), 512)
    ld_own = load(tok_h.at[:, mine], tokb)
    ld_ex = [
        load(eg_h.at[0, mine, :], wgu.at[t, :, pl.ds(0, 128)]),
        load(eu_h.at[0, mine, :], wgu.at[t, :, pl.ds(128, 128)]),
        load(ed_h.at[0, :, mine], wd.at[t]),
    ]

    def recut_down(peers):
        for d in peers:
            theirs = pl.ds(pl.multiple_of(td[d] * 512, 512), 512)
            send(ed_h.at[0, :, theirs], wd.at[t], ys.at[2, d], yr.at[2, d], (z, x, c, td[d]))

    for d in (1, 3, 2):
        p = td[d]
        dev = (z, x, c, p)
        theirs = pl.ds(pl.multiple_of(p * 512, 512), 512)
        for k, src in enumerate((eg_h, eu_h)):
            half = pl.ds(128 * k, 128)
            send(src.at[0, theirs, :], wgu.at[t, :, half], ys.at[k, d], yr.at[k, d], dev)
    recut_down((1, 3))

    ld_er.wait()
    rows = NE * 12
    chosen = iota((NE, SEQ), 0) == er[0:1, :]
    for k in range(1, 6):
        chosen = chosen | (iota((NE, SEQ), 0) == er[k : k + 1, :])
    hot_t = ones_where(chosen)
    before = ones_where(iota((SEQ, SEQ), 0) < iota((SEQ, SEQ), 1))
    code_t = jnp.where(chosen, dot(hot_t, before) + 1.0, 0.0).astype(BF16)
    repeat = ones_where((iota((SEQ, 64), 1) & 15) == iota((SEQ, 64), 0))
    eye = ones_where(iota((SEQ, SEQ), 0) == iota((SEQ, SEQ), 1))
    code4_t = dot(code_t, repeat).astype(BF16)
    code = dot_nt(eye, code_t)
    q0 = iota((rows, 64), 0) >> 2
    j0 = iota((rows, 64), 0) & 3
    e0 = (q0 * 171) >> 9
    c0 = iota((rows, 64), 1)
    spread = ones_where(e0 == c0)
    slot_of = dot(spread, code4_t)
    want = (q0 - 3 * e0 + 1).astype(F32)
    dispatch = ones_where((slot_of == want) & (j0 == (c0 >> 4)))

    for n, pick, back in ((72, pick72, back72), (48, pick48, back48)):
        for j in range(4):
            p, q = iota((n, 4 * n), 0), iota((n, 4 * n), 1)
            pick[n * j : n * j + n, :] = jnp.where(q == 4 * p + j, 1.0, 0.0)
        p, q = iota((4 * n, 4 * n), 1), iota((4 * n, 4 * n), 0)
        j = (p >= n).astype(jnp.int32) + (p >= 2 * n) + (p >= 3 * n)
        back[...] = ones_where(q == 4 * (p - n * j) + j)
    for b in range(SEQ):
        if b % 4 == 0:
            kv_loads[2 * (b // 4)].wait()
        kt[b] = kb[b].T
    o_forward(7)
    o_forward(1)
    o_forward(6)
    o_forward(2)

    for dx, dc in mates:
        src = tk.at[lax.rem(x + NX - dx, NX) * NC + cd[dc]]
        arrived(src, tks.at[dx, dc], tkr.at[dx, dc])
    for d in near_first:
        arrived(qb.at[lax.rem(z + NZ - d, NZ)], qzs.at[d], qzr.at[d])
    rows_in = tk[...].reshape(8 * SEQ, 256)
    part[...] = dot(rows_in, qb[...].reshape(256, 256)).reshape(8, SEQ, 256)
    for dx, dc in mates:
        g = xd[dx] * NC + cd[dc]
        send(part.at[g], qp.at[m], qps.at[dx, dc], qpr.at[dx, dc], (z, xd[dx], cd[dc], t))
    qp[m] = part[m]
    for r in (5, 3, 4):
        o_forward(r)
    for dx, dc in mates:
        src = qp.at[lax.rem(x + NX - dx, NX) * NC + cd[dc]]
        arrived(src, qps.at[dx, dc], qpr.at[dx, dc])
    total = qp[0]
    for i in range(1, 8):
        total = total + qp[i]
    queries = total.astype(BF16).astype(F32)

    for h in range(2):
        qs[pl.ds(h, SEQ, stride=2), :] = queries[:, HD * h : HD * h + HD]
    for cp in ld_att:
        cp.wait()
    for b in range(SEQ):
        q = qs[2 * b : 2 * b + 2, :].astype(BF16)
        lg[2 * b : 2 * b + 2, :] = dot(q, kt[b]) * HD ** (-0.5) + off[b]
        lenb[2 * b : 2 * b + 2, :] = jnp.full((2, HD), lens[b], jnp.int32)
    for cp in ld_kv:
        cp.wait()
    for d in far_first:
        send(kvb.at[z], kvb.at[z], kzs.at[d], kzr.at[d], (zd[d], x, c, t))
    for r in (0, 7, 1, 6, 2):
        o_across(r)
    logits = lg[...]
    length = lenb[:, 0:1]
    usable = iota((2 * SEQ, POS), 1) < length
    tail = jnp.log(1.0 + jnp.exp(-jnp.abs(logits)))
    keep = jnp.where(usable, jnp.minimum(-logits, 0.0) - tail, 0.0)
    nb = POS // HD
    stacked = jnp.concatenate([keep[:, HD * i : HD * i + HD] for i in range(nb)], axis=0)
    k1 = stacked.astype(BF16)
    left = stacked - k1.astype(F32)
    k2 = left.astype(BF16)
    k3 = (left - k2.astype(F32)).astype(BF16)
    later = ones_where(iota((HD, HD), 0) > iota((HD, HD), 1))
    inner = dot(k1, later) + dot(k2, later) + dot(k3, later)
    carry = jnp.zeros((2 * SEQ, 1), F32)
    after = [None] * nb
    n2 = 2 * SEQ
    for i in range(nb - 1, -1, -1):
        after[i] = inner[n2 * i : n2 * i + n2] + carry
        carry = carry + jnp.sum(stacked[n2 * i : n2 * i + n2], axis=-1, keepdims=True)
    after = jnp.concatenate(after, axis=1)
    sticks = jnp.where(usable, jnp.exp(jnp.minimum(logits, 0.0) - tail + after), 0.0)
    lg[...] = sticks
    for r in (5, 3, 4):
        o_across(r)
    for b in range(SEQ):
        if b % 4 == 0:
            kv_loads[2 * (b // 4) + 1].wait()
        got = dot(lg[2 * b : 2 * b + 2, :].astype(BF16), vb[b])
        ho[b : b + 1, 0:HD] = got[0:1, :]
        ho[b : b + 1, HD : 2 * HD] = got[1:2, :]
    heads_out = ho[...]
    scaled = jnp.concatenate(
        [heads_out[:, HD * i : HD * i + HD] * hg[i : i + 1, :].astype(F32) for i in range(2)],
        axis=1,
    ).astype(BF16)
    sq[t] = jnp.broadcast_to(jnp.sum(heads_out * heads_out, axis=-1, keepdims=True), (SEQ, HD))
    o_last()
    for i in range(NT):
        halves = [dot_nt(scaled, ob[zi].reshape(256, 256)) for zi in (2 * i, 2 * i + 1)]
        pcs[i] = jnp.concatenate(halves, axis=1).astype(BF16)

    for d in (2, 1, 3):
        dev = (z, x, c, td[d])
        send(sq.at[t], sq.at[t], cs.at[0, d], cr.at[0, d], dev)
        send(pcs.at[td[d]], pc.at[t], cs.at[1, d], cr.at[1, d], dev)
    pc[t] = pcs[t]
    for d in (1, 3, 2):
        src = td[NT - d]
        for k, buf in enumerate((sq, pc)):
            arrived(buf.at[src], cs.at[k, d], cr.at[k, d])
    head_total = pc[0].astype(F32)
    square = sq[0]
    for i in range(1, NT):
        head_total = head_total + pc[i].astype(F32)
        square = square + sq[i]
    attention = head_total * lax.rsqrt(square[:, 0:1] / 1024.0 + EPS)
    ld_own.wait()
    residual = (tokb[...].astype(F32) + attention).astype(BF16)
    res[t] = residual
    for d in (2, 1, 3):
        send(res.at[t], res.at[t], as2.at[d], ar2.at[d], (z, x, c, td[d]))

    block = jnp.concatenate([residual[:, HD * j : HD * j + HD] for j in range(4)], axis=0)
    sbuf[...] = dot(dispatch, block).astype(BF16).reshape(3 * NE, 4, HD)
    order = (3, 4, 5, 2, 6, 7, 0, 1)
    part_rows = (72, 48, 72)
    first_row = (0, 72, 120)

    def three(i):
        return pl.ds(3 * i, 3)

    def part_of(r):
        return (0, 0, 0, 1, 1, 2, 2, 2)[order.index(r)]

    def around(r):
        return [(0, 0), *mates] if r else mates

    for r in (4, 7, 1, 0, 5, 3, 6, 2):
        d = (NZ - r) % NZ
        to = three(8 * order.index(r) + m)
        for dx, dc in around(r):
            p = (zd[d] * NX + xd[dx]) * NC + cd[dc]
            dev = (zd[d], xd[dx], cd[dc], t)
            remote(sbuf.at[three(p)], rbuf.at[to], as_.at[part_of(r)], ar.at[part_of(r)], dev).start()
    rbuf[three(8 * order.index(0) + m)] = sbuf[three(e)]

    recut_down((2,))

    for cp in ld_ffn:
        cp.wait()
    gain = fg[...].astype(F32)
    own_gain = []
    for j in range(4):
        row = gain[j : j + 1, :]
        for i in range(1, NT):
            row = jnp.where(t == i, gain[4 * i + j : 4 * i + j + 1, :], row)
        own_gain.append(row)
    own_gain = jnp.concatenate(own_gain, axis=1)

    gs, gr, hs = (gs0, gs1, gs2), (gr0, gr1, gr2), (hs0, hs1, hs2)

    def start_part(k):
        n, at = part_rows[k], first_row[k]
        pick = pick48 if n == 48 else pick72
        remote_rows = n if k < 2 else n - 3
        both = remote(
            sbuf.at[pl.ds(0, remote_rows)], rbuf.at[pl.ds(0, remote_rows)], as_.at[k], ar.at[k],
            (z, x, 1 - c, t),
        )
        both.wait_recv()
        came = dot(pick[...].astype(BF16), rbuf[at : at + n].reshape(4 * n, HD))
        raw = jnp.concatenate([came[n * j : n * j + n] for j in range(4)], axis=1)
        rows_of = (raw * own_gain).astype(BF16)
        for d in (2, 1, 3):
            gs[k][d] = dot(rows_of, wgu[td[d]]).astype(BF16)
        for d in (2, 1, 3):
            send(gs[k].at[d], gr[k].at[d], gss.at[k, d], gsr.at[k, d], (z, x, c, td[d]))
        gate_up = dot(rows_of, wgu[t])
        square = jnp.sum(raw * raw, axis=-1, keepdims=True)
        square = jnp.concatenate([square, jnp.zeros((HD - n, 1), F32)], axis=0)
        fs[k, 0] = jnp.broadcast_to(square, (HD, HD)).T[0:8, :]
        for d in (2, 1, 3):
            send(fs.at[k, 0], fs.at[k, d], fss.at[k, d], fsr.at[k, d], (z, x, c, td[d]))
        return gate_up, both

    def middle_part(k, gate_up):
        for d in (2, 1, 3):
            arrived(gr[k].at[d], gss.at[k, d], gsr.at[k, d])
            gate_up = gate_up + gr[k][d].astype(F32)
            arrived(fs.at[k, d], fss.at[k, d], fsr.at[k, d])
        square = fs[k, 0] + fs[k, 1] + fs[k, 2] + fs[k, 3]
        square = jnp.broadcast_to(square[0:1, :], (HD, HD)).T[0 : part_rows[k], 0:1]
        gate_up = gate_up * lax.rsqrt(square / 2048.0 + EPS)
        gate = gate_up[:, 0:HD]
        hidden = gate / (1.0 + jnp.exp(-gate)) * gate_up[:, HD : 2 * HD]
        hs[k][t] = hidden.astype(BF16)
        own = hs[k].at[t]
        for d in (2, 1, 3):
            send(own, own, hss.at[k, d], hsr.at[k, d], (z, x, c, td[d]))

    def end_part(k):
        n, at = part_rows[k], first_row[k]
        back = back48 if n == 48 else back72
        for d in (2, 1, 3):
            arrived(hs[k].at[td[NT - d]], hss.at[k, d], hsr.at[k, d])
        out = dot(hs[k][0], wd[0])
        for i in range(1, NT):
            out = out + dot(hs[k][i], wd[i])
        out = jnp.concatenate([out[:, HD * j : HD * j + HD] for j in range(4)], axis=0)
        obuf[at : at + n] = dot(back[...], out.astype(BF16)).astype(BF16).reshape(n, 4, HD)
        for r in ((4, 5, 3), (6, 2), (7, 1, 0))[k]:
            for dx, dc in around(r):
                p = 8 * order.index(r) + xd[dx] * NC + cd[dc]
                dev = (zd[r], xd[dx], cd[dc], t)
                remote(obuf.at[three(p)], cbuf.at[three(e)], rs_, rr, dev).start()

    for cp in ld_ex:
        cp.wait()
    for d in (1, 3, 2):
        src = td[NT - d]
        for k in range(2):
            arrived(wgu.at[src, :, pl.ds(128 * k, 128)], ys.at[k, d], yr.at[k, d])
    gate_up2, sent2 = start_part(2)

    for d in (1, 3, 2):
        arrived(res.at[td[NT - d]], as2.at[d], ar2.at[d])
    data = jnp.concatenate([res[i] for i in range(NT)], axis=1).astype(F32)
    factor = lax.rsqrt(jnp.mean(data * data, axis=-1, keepdims=True) + EPS)
    pieces = [data[:, HD * i : HD * i + HD] * factor * gain[i : i + 1, :] for i in range(16)]
    normed_ffn = jnp.concatenate(pieces, axis=1).astype(BF16)
    for cp in ld_sh:
        cp.wait()
    both = dot(normed_ffn, sgu[...])
    gate = both[:, 0:HD]
    shared_hidden = (gate / (1.0 + jnp.exp(-gate)) * both[:, HD : 2 * HD]).astype(BF16)
    shared_part = dot(shared_hidden, sd[...]).astype(BF16)
    for i in range(NT):
        ssb[i] = shared_part[:, 512 * i : 512 * i + 512]
    for d in (2, 1, 3):
        p = td[d]
        send(ssb.at[p], ssr.at[t], sss.at[d], ssrr.at[d], (z, x, c, p))
    ssr[t] = ssb[t]
    logit = dot_nt(normed_ffn, rt[...])
    prob = 1.0 / (1.0 + jnp.exp(-logit))
    picked = jnp.where(code > 0.5, prob, 0.0)
    weight = SCALE * picked / jnp.sum(picked, axis=-1, keepdims=True)
    weight4 = jnp.concatenate([weight] * 4, axis=0)
    w_hi = weight4.astype(BF16)
    w_lo = (weight4 - w_hi.astype(F32)).astype(BF16)
    code4 = jnp.concatenate([code] * 4, axis=0).astype(BF16)
    q1 = iota((64, rows), 1) >> 2
    j1 = iota((64, rows), 1) & 3
    e1 = (q1 * 171) >> 9
    c1 = iota((64, rows), 0)
    spread_t = ones_where(e1 == c1)
    slot_to = dot(code4, spread_t)
    fits = (slot_to == (q1 - 3 * e1 + 1).astype(F32)) & (j1 == (c1 >> 4))
    comb_hi = jnp.where(fits, dot(w_hi, spread_t), 0.0).astype(BF16)
    comb_lo = jnp.where(fits, dot(w_lo, spread_t), 0.0).astype(BF16)

    for d in near_first:
        arrived(kvb.at[lax.rem(z + NZ - d, NZ)], kzs.at[d], kzr.at[d])
    kvpart[...] = dot(rows_in, kvb[...].reshape(256, 256)).astype(BF16).reshape(8, SEQ, 256)
    for dx, dc in mates:
        g = xd[dx] * NC + cd[dc]
        send(kvpart.at[g], kvp.at[m], kps.at[dx, dc], kpr.at[dx, dc], (z, xd[dx], cd[dc], t))
    kvp[m] = kvpart[m]
    gate_up0, sent0 = start_part(0)
    gate_up1, sent1 = start_part(1)
    middle_part(2, gate_up2)
    middle_part(0, gate_up0)
    middle_part(1, gate_up1)
    for d in (1, 3, 2):
        arrived(wd.at[td[NT - d]], ys.at[2, d], yr.at[2, d])
    end_part(0)
    end_part(2)
    end_part(1)
    cbuf[three(e)] = obuf[three(8 * order.index(0) + m)]
    shared_total = jnp.zeros((SEQ, 512), F32)
    for d in (2, 1, 3):
        arrived(ssr.at[td[NT - d]], sss.at[d], ssrr.at[d])
    for i in range(NT):
        shared_total = shared_total + ssr[i].astype(F32)
    base = res[t].astype(F32) + shared_total
    for dx, dc in mates:
        src = kvp.at[lax.rem(x + NX - dx, NX) * NC + cd[dc]]
        arrived(src, kps.at[dx, dc], kpr.at[dx, dc])
    new = kvp[0].astype(F32)
    for i in range(1, 8):
        new = new + kvp[i].astype(F32)
    fk_o[...] = new[:, 0:HD].astype(BF16)
    fv_o[...] = new[:, HD : 2 * HD].astype(BF16)
    back = remote(
        obuf.at[pl.ds(0, 3 * NE - 3)], cbuf.at[pl.ds(0, 3 * NE - 3)], rs_, rr, (z, x, 1 - c, t)
    )
    back.wait_recv()
    came = cbuf[...].reshape(rows, HD)
    routed = dot(comb_hi, came) + dot(comb_lo, came)
    for j in range(4):
        mixed_o[:, HD * j : HD * j + HD] = (
            base[:, HD * j : HD * j + HD] + routed[SEQ * j : SEQ * j + SEQ]
        ).astype(BF16)
    for cp in [*pending, sent0, sent1, sent2, back]:
        cp.wait_send()


def hand_over(a, b, c, a_o, b_o, c_o, sem):
    moves = []
    for i, (src, dst) in enumerate(((a, a_o), (b, b_o), (c, c_o))):
        moves.append(pltpu.make_async_copy(src, dst, sem.at[i]))
        moves[i].start()
    for cp in moves:
        cp.wait()


def body(
    tokens, attn_gain, query_weight, key_weight, value_weight, out_weight, head_gain,
    past_keys, past_values, break_offset, cache_lengths, ffn_gain, router_weight,
    expert_routes, expert_gate, expert_up, expert_down, shared_gate, shared_up, shared_down,
):
    hbm = pl.BlockSpec(memory_space=pl.ANY)
    v, dma = pltpu.VMEM, pltpu.SemaphoreType.DMA
    outs = pl.pallas_call(
        kernel,
        out_shape=(v((SEQ, 512), BF16), v((SEQ, HD), BF16), v((SEQ, HD), BF16)),
        in_specs=[hbm] * 20,
        out_specs=(pl.BlockSpec(memory_space=pltpu.VMEM),) * 3,
        scratch_shapes=[
            v((SEQ, 2048), BF16), v((16, HD), BF16), v((2, HD), BF16), v((16, HD), BF16),
            v((64, 2048), BF16), v((6, SEQ), jnp.int32), v((SEQ, 2, POS), F32),
            v((SEQ, POS, HD), BF16), v((SEQ, HD, POS), BF16), v((SEQ, POS, HD), BF16),
            v((NZ, 32, 256), BF16), v((NZ, 32, 256), BF16), v((NZ, NX, NC, 32, 256), BF16),
            v((NT, 512, 256), BF16), v((NT, 128, 512), BF16),
            v((2048, 256), BF16), v((128, 2048), BF16),
            v((8, SEQ, 256), BF16), v((8, SEQ, 256), BF16),
            v((8, SEQ, 256), F32), v((8, SEQ, 256), F32),
            v((8, SEQ, 256), BF16), v((8, SEQ, 256), BF16),
            v((2 * SEQ, HD), F32), v((2 * SEQ, POS), F32), v((2 * SEQ, HD), jnp.int32),
            v((SEQ, 256), F32), v((NT, SEQ, 512), BF16), v((NT, SEQ, 512), BF16),
            v((NT, SEQ, HD), F32), v((3, NT, 8, HD), F32), v((NT, SEQ, 512), BF16),
            v((3 * NE, 4, HD), BF16), v((3 * NE, 4, HD), BF16),
            *[v((NT, n, 256), BF16) for _ in range(2) for n in (72, 48, 72)],
            *[v((NT, n, HD), BF16) for n in (72, 48, 72)],
            v((288, 288), F32), v((288, 288), BF16), v((192, 192), F32), v((192, 192), BF16),

            v((3 * NE, 4, HD), BF16), v((3 * NE, 4, HD), BF16),
            v((NT, SEQ, 512), BF16), v((NT, SEQ, 512), BF16),
            pltpu.SMEM((SEQ,), jnp.int32), v((SEQ, 512), BF16), dma((32,)), dma((8,)),
            *[dma((NZ,)) for _ in range(6)],
            dma((NZ, NX)), dma((NZ, NX)), dma((NZ,)), dma((NZ,)),
            *[dma((NX, NC)) for _ in range(6)],
            dma((3, 4)), dma((3, 4)), dma((2, 4)), dma((2, 4)), dma((3,)), dma((3,)),
            dma((3, 4)), dma((3, 4)), dma((3, 4)), dma((3, 4)), dma, dma, dma((4,)), dma((4,)),
            dma((4,)), dma((4,)), dma((3, 4)), dma((3, 4)),
        ],
        compiler_params=pltpu.CompilerParams(
            collective_id=0, has_side_effects=True, vmem_limit_bytes=60 * 1024 * 1024
        ),
    )(
        tokens, attn_gain.reshape(16, HD), query_weight, key_weight, value_weight, out_weight,
        head_gain.reshape(2, HD), past_keys.reshape(SEQ, POS, HD),
        past_values.reshape(SEQ, POS, HD), break_offset, cache_lengths,
        ffn_gain.reshape(16, HD), router_weight.T, expert_routes.T, expert_gate, expert_up,
        expert_down, shared_gate, shared_up, shared_down,
    )
    return pl.pallas_call(
        hand_over,
        out_shape=tuple(jax.ShapeDtypeStruct(o.shape, o.dtype) for o in outs),
        in_specs=[pl.BlockSpec(memory_space=pltpu.VMEM)] * 3,
        out_specs=(hbm,) * 3,
        scratch_shapes=[dma((3,))],
    )(*[pltpu.with_memory_space_constraint(o, pltpu.VMEM) for o in outs])


def solution(mesh):
    torus = Mesh(mesh.devices.reshape(NZ, NX, NC, NT), (*EP, "tp"))
    return jax.shard_map(
        body,
        mesh=torus,
        in_specs=(
            P(EP, None),
            P(),
            P(EP, "tp"),
            P(EP, "tp"),
            P(EP, "tp"),
            P(EP, "tp"),
            P("tp"),
            P(EP, None, "tp", None),
            P(EP, None, "tp", None),
            P(EP, "tp", None),
            P(EP),
            P(),
            P(),
            P(EP, None),
            P(EP, None, "tp"),
            P(EP, None, "tp"),
            P(EP, "tp", None),
            P(None, "tp"),
            P(None, "tp"),
            P("tp", None),
        ),
        out_specs=(P(EP, "tp"), P(EP, "tp"), P(EP, "tp")),
        check_vma=False,
    )
```
